32 devices in a mesh: sp: 8 (over z, y), dp: 4 (over x, core).
Axes of the slice: x: 2, y: 2, z: 4, core: 2. Of those that a mesh axis runs over, the one named last changes fastest.
Arguments:
- query_nope: bfloat16 [4, 2048, 16, 128], P('dp', 'sp'), may hold values from -6 to 6
- query_rope: bfloat16 [4, 2048, 16, 64], P('dp', 'sp'), may hold values from -160 to 160
- latent: bfloat16 [4, 2048, 256], P('dp', 'sp'), may hold values from -6 to 6
- key_rope: bfloat16 [4, 2048, 64], P('dp', 'sp'), may hold values from -4 to 4
- resid: bfloat16 [4, 2048, 2048], P('dp', 'sp'), may hold values from -6 to 6
- latent_gain: float32 [256], replicated, may hold values from 0.1 to 1.9
- key_up: bfloat16 [256, 2048], P(None, 'sp'), may hold values from -0.375 to 0.375
- value_up: bfloat16 [256, 2048], P(None, 'sp'), may hold values from -0.375 to 0.375
- out_proj: bfloat16 [2048, 2048], P('sp', 'dp'), may hold values from -0.125 to 0.125
- norm_gain: float32 [2048], replicated, may hold values from 0.1 to 1.9
- expert_gate: bfloat16 [8, 2048, 1024], P('sp'), may hold values from -0.125 to 0.125
- expert_up: bfloat16 [8, 2048, 1024], P('sp'), may hold values from -0.125 to 0.125
- expert_down: bfloat16 [8, 1024, 2048], P('sp'), may hold values from -0.1875 to 0.1875
- routes: int32 [4, 2048, 2], P('dp', 'sp'), may hold values from 0 to 7, all different within a row; in each aligned block of 256 rows (0 to 255, 256 to 511, ..., all dimensions but the last counted through in order) at most 128 rows name the same one
- route_weight: float32 [4, 2048, 2], P('dp', 'sp'), may hold values from 0.2 to 1
Outputs:
- mixed: bfloat16 [4, 2048, 2048], P('dp', 'sp')
The draws below stay inside these ranges and needn't reach their ends.
Inputs may be any that keep to these rules, and one draw needn't show every extreme that they name: `routes`: each token names two different experts. Among the tokens of one device no expert is named more than 128 times, and in every draw some expert is named exactly 128 times by some device's tokens.
All inputs are finite; a program needn't handle non-finite values.
Results may differ from the reference program's by a relative error of at most 0.0075.
Values may be sent and summed in bfloat16 or wider, within the bound.
A program may use at most 128 MiB of HBM per device.

```python
import math
import jax
import jax.numpy as jnp
import numpy as np
from jax import lax

D = 2048
HEADS = 16
NOPE = 128
ROPE = 64
VDIM = 128
LATENT = 256
FFE = 1024
TOK_DEV = 256
LENGTH = 2048
SEQS = 4
EXPERTS = 8
CAP = 128
N_SP = 8
N_DP = 4


def rope_pair(key):
    base_key = jax.random.fold_in(key, 911)
    key_draw, query_draw = jax.random.split(base_key, 2)
    keys_raw = jnp.clip(jax.random.normal(key_draw, (SEQS, LENGTH, ROPE), jnp.float32), -4.0, 4.0)
    queries = jnp.clip(jax.random.normal(query_draw, (SEQS, LENGTH, HEADS, ROPE), jnp.float32), -4.0, 4.0)
    return (queries, keys_raw)


def draw_query_rope(key, part):
    return rope_pair(key)[0].astype(jnp.bfloat16)


def draw_key_rope(key, part):
    return rope_pair(key)[1].astype(jnp.bfloat16)


def steps_of(rng, extent, cuts, low, top_value):
    def one(axis_at, parts):
        steps = jax.random.uniform(jax.random.fold_in(jax.random.fold_in(rng, 6), axis_at), (parts,), jnp.float32, low / len(cuts), top_value / len(cuts))
        return jnp.repeat(jnp.exp(steps), extent[axis_at] // parts).reshape((-1,) + (1,) * (len(extent) - axis_at - 1))

    factor_of = one(*cuts[0])
    for cut in cuts[1:]:
        factor_of = factor_of * one(*cut)
    return factor_of


def deal_out(key, own, number, rows, count, top, most, lean):
    order = jax.random.permutation(key, count)
    heavy_load, usual = load_shares(count, rows * top, most, lean, True), load_shares(count, rows * top, most, lean, False)
    places = jnp.arange(count)

    def named(tallies, offset_by):
        used = int((tallies > 0).sum())
        fixed = max(1, used // 4)
        shifted = fixed + (places - fixed + offset_by * (used - fixed)) % max(1, count - fixed)
        return jnp.zeros((count,), jnp.int32).at[order[jnp.where(places < fixed, places, shifted)]].set(jnp.asarray(tallies, jnp.int32))

    tallies = jnp.where(number % 4 == 0, named(heavy_load, number // 4), named(usual, number - number // 4 - 1))
    mixed = jax.random.permutation(jax.random.fold_in(own, 3), count)
    giver, receiver = mixed[0:count // 2 * 2:2], mixed[1:count // 2 * 2:2]
    slack = jnp.minimum(tallies[giver] - 1, most - tallies[receiver]) // 2
    slack = jnp.where((giver == order[0]) | (receiver == order[0]) | (tallies[receiver] == 0), 0, jnp.maximum(slack, 0))
    shifted = jax.random.randint(jax.random.fold_in(own, 4), (count // 2,), 0, 1 << 20) % (slack + 1)
    tallies = tallies.at[giver].add(-shifted).at[receiver].add(shifted)
    items = jnp.searchsorted(jnp.cumsum(tallies), jnp.arange(rows * top), side="right").astype(jnp.int32)
    listing = items.reshape(top, rows).T
    listing = listing[jax.random.permutation(jax.random.fold_in(own, 1), rows)]
    offset_by = jax.random.randint(jax.random.fold_in(own, 2), (rows, 1), 0, top)
    return jnp.take_along_axis(listing, (jnp.arange(top)[None, :] + offset_by) % top, axis=1)


def load_shares(number_of, total, limit, slope, full):
    portions = [(1 << 20) // math.isqrt(standing ** slope) + 1 for standing in range(1, number_of + 1)]
    largest = limit if full else min(limit, max(-(-total // number_of), total * portions[0] // sum(portions)))
    least = 1 if total - largest >= number_of - 1 else 0
    counts, rest = [largest] + [least] * (number_of - 1), total - largest - least * (number_of - 1)
    while rest > 0:
        candidates = [i for i in range(1, number_of) if counts[i] < largest] or [i for i in range(1, number_of) if counts[i] < limit]
        mass, remaining = sum([portions[i] for i in candidates]), rest
        for i in candidates:
            more = min(limit - counts[i], max(1, remaining * portions[i] // mass), rest)
            counts[i] = counts[i] + more
            rest = rest - more
    return np.array(counts)


def centred(key, shape, deviation, reach, cuts=(), held_as=jnp.bfloat16):
    drawn = jax.random.normal(key, shape, jnp.float32) * deviation
    if len(cuts) > 0:
        drawn = steps_of(key, shape, cuts, -0.22, 0.18) * drawn
    return jnp.clip(drawn, min=-reach, max=reach).astype(held_as)


def setup_inputs(seed: int = 0) -> dict:
    keys = jax.random.split(jax.random.key(seed), 16)
    query_nope = centred(keys[0], (SEQS, LENGTH, HEADS, NOPE), 1.0, 6.0, ((0, 4), (1, 8)))
    query_rope = draw_query_rope(jax.random.fold_in(keys[15], 71), 0)
    latent = centred(keys[2], (SEQS, LENGTH, LATENT), 1.0, 6.0, ((0, 4), (1, 8)))
    key_rope = draw_key_rope(jax.random.fold_in(keys[15], 71), 0)
    resid = centred(keys[4], (SEQS, LENGTH, D), 1.0, 6.0, ((0, 4), (1, 8)))
    latent_gain = jnp.clip(1.0 + 0.18 * jax.random.normal(keys[5], (LATENT,), jnp.float32), 0.1, 1.9)
    key_up = centred(keys[6], (LATENT, HEADS * NOPE), LATENT ** -0.5, 0.375, ((1, 8),))
    value_up = centred(keys[7], (LATENT, HEADS * VDIM), LATENT ** -0.5, 0.375, ((1, 8),))
    out_proj = centred(keys[8], (HEADS * VDIM, D), (HEADS * VDIM) ** -0.5, 0.125, ((0, 8), (1, 4)))
    norm_gain = jnp.clip(1.0 + 0.18 * jax.random.normal(keys[9], (D,), jnp.float32), 0.1, 1.9)
    expert_gate = centred(keys[10], (EXPERTS, D, FFE), D ** -0.5, 0.125, ((0, 8),))
    expert_up = centred(keys[11], (EXPERTS, D, FFE), D ** -0.5, 0.125, ((0, 8),))
    expert_down = centred(keys[12], (EXPERTS, FFE, D), FFE ** -0.5, 0.1875, ((0, 8),))
    routes_keys = jax.random.split(jax.random.fold_in(keys[13], 1), SEQS * LENGTH // TOK_DEV)
    routes_turns = jax.random.permutation(jax.random.fold_in(keys[13], 3), SEQS * LENGTH // TOK_DEV)
    routes = jax.vmap(lambda own, number: deal_out(jax.random.fold_in(keys[13], 2), own, number, TOK_DEV, EXPERTS, 2, CAP, 1))(routes_keys, routes_turns).reshape((SEQS, LENGTH, 2))
    route_weight = jnp.clip(0.2 + 0.8 * jax.random.uniform(keys[14], (SEQS, LENGTH, 2), jnp.float32) ** steps_of(keys[14], (SEQS, LENGTH, 2), ((0, 4), (1, 8)), -0.2, 0.2), 0.2, 1.0)
    return dict(query_nope=query_nope, query_rope=query_rope, latent=latent, key_rope=key_rope, resid=resid, latent_gain=latent_gain, key_up=key_up, value_up=value_up, out_proj=out_proj, norm_gain=norm_gain, expert_gate=expert_gate, expert_up=expert_up, expert_down=expert_down, routes=routes, route_weight=route_weight)


epsilon = 1e-06
rope_base = 10000.0
masked_score = -1e+30

def rotate(values, positions):
    half_width = values.shape[-1] // 2
    frequency = rope_base ** (-jnp.arange(half_width, dtype=jnp.float32) / half_width)
    angles = positions.astype(jnp.float32)[:, None] * frequency[None, :]
    cosine = jnp.cos(angles)
    sine_part = jnp.sin(angles)
    if values.ndim == 3:
        cosine = cosine[:, None, :]
        sine_part = sine_part[:, None, :]
    floats = values.astype(jnp.float32)
    first_half = floats[..., :half_width]
    second_half = floats[..., half_width:]
    turned = jnp.concatenate([first_half * cosine - second_half * sine_part, second_half * cosine + first_half * sine_part], axis=-1)
    return turned.astype(jnp.bfloat16)

def rms_scaled(values, gain):
    floats = values.astype(jnp.float32)
    return floats * lax.rsqrt(lax.optimization_barrier(jnp.mean(floats * floats, axis=-1, keepdims=True)) + epsilon) * gain

def assign_slots(route_block, experts_all, capacity):
    flat_routes = route_block.reshape(-1)
    onehot = (flat_routes[:, None] == jnp.arange(experts_all, dtype=jnp.int32)[None, :]).astype(jnp.int32)
    earlier = jnp.cumsum(onehot, axis=0) - onehot
    placed = lax.optimization_barrier(jnp.sum(earlier * onehot, axis=1))
    return (flat_routes * capacity + placed).astype(jnp.int32)

def fill_slots(rows, slot_ids, experts_all, capacity):
    pairs = slot_ids.shape[0]
    matches = jnp.arange(experts_all * capacity, dtype=jnp.int32)[:, None] == slot_ids[None, :]
    source = lax.optimization_barrier(jnp.sum(jnp.where(matches, jnp.arange(pairs, dtype=jnp.int32)[None, :], 0), axis=1)) // 2
    filled = jnp.any(matches, axis=1)
    picked = jnp.take(rows, source.astype(jnp.int32), axis=0)
    chosen = jnp.where(filled[:, None], picked, jnp.zeros_like(picked))
    return chosen.reshape(experts_all, capacity, rows.shape[-1])

def combine_slots(returned, slot_ids, weights):
    flat_back = returned.reshape(-1, returned.shape[-1])
    picked = jnp.take(flat_back, slot_ids, axis=0).astype(jnp.float32).reshape(weights.shape[0], 2, -1)
    return lax.optimization_barrier(jnp.sum(weights[:, :, None] * picked, axis=1))

def expert_rows(rows, gate_weight, up_weight, down_weight):
    gate = jnp.dot(rows, gate_weight, preferred_element_type=jnp.float32)
    upward = jnp.dot(rows, up_weight, preferred_element_type=jnp.float32)
    hidden = (jax.nn.silu(gate) * upward).astype(jnp.bfloat16)
    return jnp.dot(hidden, down_weight, preferred_element_type=jnp.float32).astype(jnp.bfloat16)

def head_attention(query_plain, query_turn, key_plain, key_turn, value_head, block):
    length = key_plain.shape[0]
    blocks = length // block
    scale = (query_plain.shape[-1] + query_turn.shape[-1]) ** (-0.5)
    key_ids = jnp.arange(length, dtype=jnp.int32)

    def one_block(items):
        index, plain_block, turn_block = items
        scores = jnp.dot(plain_block, key_plain.T, preferred_element_type=jnp.float32)
        scores = (scores + jnp.dot(turn_block, key_turn.T, preferred_element_type=jnp.float32)) * scale
        row_ids = index * block + jnp.arange(block, dtype=jnp.int32)
        allowed = key_ids[None, :] <= row_ids[:, None]
        scores = jnp.where(allowed, scores, masked_score)
        largest = lax.optimization_barrier(jnp.max(scores, axis=-1, keepdims=True))
        powers = jnp.exp(scores - largest)
        attend = (powers / lax.optimization_barrier(jnp.sum(powers, axis=-1, keepdims=True))).astype(jnp.bfloat16)
        return jnp.dot(attend, value_head, preferred_element_type=jnp.float32).astype(jnp.bfloat16)
    result = lax.map(one_block, (jnp.arange(blocks, dtype=jnp.int32), query_plain.reshape(blocks, block, -1), query_turn.reshape(blocks, block, -1)))
    return result.reshape(length, -1)

def reference(query_nope, query_rope, latent, key_rope, resid, latent_gain, key_up, value_up, out_proj, norm_gain, expert_gate, expert_up, expert_down, routes, route_weight):
    positions = jnp.arange(LENGTH, dtype=jnp.int32)
    block = min(512, LENGTH)
    key_turned = jax.vmap(lambda item: rotate(item, positions))(key_rope)
    query_turned = jax.vmap(lambda item: rotate(item, positions))(query_rope)
    latent_normed = rms_scaled(latent, latent_gain).astype(jnp.bfloat16)
    flat_latent = latent_normed.reshape(-1, LATENT)
    key_nope = jnp.dot(flat_latent, key_up, preferred_element_type=jnp.float32).astype(jnp.bfloat16).reshape(SEQS, LENGTH, HEADS, NOPE)
    values = jnp.dot(flat_latent, value_up, preferred_element_type=jnp.float32).astype(jnp.bfloat16).reshape(SEQS, LENGTH, HEADS, VDIM)

    def one_sequence(items):
        plain_heads, turn_heads, key_heads, value_heads, key_turn = items
        return lax.map(lambda head: head_attention(head[0], head[1], head[2], key_turn, head[3], block), (plain_heads, turn_heads, key_heads, value_heads))
    heads_out = lax.map(one_sequence, (jnp.transpose(query_nope, (0, 2, 1, 3)), jnp.transpose(query_turned, (0, 2, 1, 3)), jnp.transpose(key_nope, (0, 2, 1, 3)), jnp.transpose(values, (0, 2, 1, 3)), key_turned))
    heads_out = jnp.transpose(heads_out, (0, 2, 1, 3)).reshape(SEQS * LENGTH, HEADS * VDIM)
    projected = jnp.dot(heads_out, out_proj, preferred_element_type=jnp.float32).astype(jnp.bfloat16)
    after_attention = resid.reshape(-1, D).astype(jnp.float32) + projected.astype(jnp.float32)
    normed = rms_scaled(after_attention, norm_gain).astype(jnp.bfloat16)
    normed_blocks = normed.reshape(N_DP, N_SP, TOK_DEV, D)
    route_blocks = routes.reshape(N_DP, N_SP, TOK_DEV, 2)
    slot_ids = jax.vmap(jax.vmap(lambda item: assign_slots(item, EXPERTS, CAP)))(route_blocks)
    buffers = jax.vmap(jax.vmap(lambda rows, ids: fill_slots(rows, ids, EXPERTS, CAP)))(normed_blocks, slot_ids)
    by_expert = jnp.transpose(buffers, (2, 0, 1, 3, 4)).reshape(EXPERTS, N_DP * N_SP * CAP, D)
    outputs = lax.map(lambda item: expert_rows(item[0], item[1], item[2], item[3]), (by_expert, expert_gate, expert_up, expert_down))
    returned = jnp.transpose(outputs.reshape(EXPERTS, N_DP, N_SP, CAP, D), (1, 2, 0, 3, 4))
    routed = jax.vmap(jax.vmap(combine_slots))(returned, slot_ids, route_weight.reshape(N_DP, N_SP, TOK_DEV, 2))
    mixed = after_attention + routed.reshape(-1, D)
    return mixed.astype(jnp.bfloat16).reshape(SEQS, LENGTH, D)
```

```python
import functools
import math

import jax
import jax.numpy as jnp
from jax import lax
from jax.experimental import pallas as pl
from jax.experimental.pallas import tpu as pltpu
from jax.sharding import PartitionSpec as P

epsilon = 1e-06
rope_base = 10000.0
masked_score = -1e30
log2_e = 1.4426950408889634


def rotate(values, positions):
    half_width = values.shape[-1] // 2
    frequency = rope_base ** (-jnp.arange(half_width, dtype=jnp.float32) / half_width)
    angles = positions.astype(jnp.float32)[:, None] * frequency[None, :]
    cosine = jnp.cos(angles)
    sine_part = jnp.sin(angles)
    if values.ndim == 3:
        cosine = cosine[:, None, :]
        sine_part = sine_part[:, None, :]
    floats = values.astype(jnp.float32)
    first_half = floats[..., :half_width]
    second_half = floats[..., half_width:]
    turned = jnp.concatenate(
        [
            first_half * cosine - second_half * sine_part,
            second_half * cosine + first_half * sine_part,
        ],
        axis=-1,
    )
    return turned.astype(jnp.bfloat16)


def rms_scaled(values, gain):
    floats = values.astype(jnp.float32)
    return floats * lax.rsqrt(jnp.mean(floats * floats, axis=-1, keepdims=True) + epsilon) * gain


def attend_kernel(heads_here, nope, channels, scale, me_ref, query_ref, shared_ref, ups_ref, out_ref):
    group = pl.program_id(0)
    columns = heads_here * nope
    me = me_ref[0]
    tokens = shared_ref.shape[1]
    ups = ups_ref[...].reshape(channels, 2 * columns)
    up_keys = ups[:, 0:columns]
    up_values = ups[:, columns : 2 * columns]
    up_values_t = jnp.transpose(up_values.astype(jnp.float32)).astype(jnp.bfloat16)

    def scores_of(chunk):
        latent = shared_ref[chunk, :, 0:channels]
        turned = shared_ref[chunk, :, channels:]
        keys = jnp.dot(latent, up_keys, preferred_element_type=jnp.float32).astype(jnp.bfloat16)
        values_t = lax.dot_general(
            up_values_t, latent, (((1,), (1,)), ((), ())), preferred_element_type=jnp.float32
        ).astype(jnp.bfloat16)
        scores = []
        for head in range(heads_here):
            full = jnp.concatenate([keys[:, head * nope : (head + 1) * nope], turned], axis=1)
            scores.append(
                jnp.dot(full, query_ref[head], preferred_element_type=jnp.float32)
                * (scale * log2_e)
            )
        return scores, [values_t[h * nope : (h + 1) * nope, :] for h in range(heads_here)]

    key_ids = lax.broadcasted_iota(jnp.int32, (tokens, tokens), 0)
    query_ids = lax.broadcasted_iota(jnp.int32, (tokens, tokens), 1)
    allowed = key_ids <= query_ids
    scores, values = scores_of(me)
    state = []
    for score, value in zip(scores, values):
        score = jnp.where(allowed, score, masked_score)
        largest = jnp.max(score, axis=0, keepdims=True)
        powers = jnp.exp2(score - largest)
        state.append(
            (
                largest,
                jnp.sum(powers, axis=0, keepdims=True),
                jnp.dot(value, powers.astype(jnp.bfloat16), preferred_element_type=jnp.float32),
            )
        )

    def step(chunk, state):
        scores, values = scores_of(chunk)
        after = []
        for (largest, total, kept), score, value in zip(state, scores, values):
            now = jnp.maximum(largest, jnp.max(score, axis=0, keepdims=True))
            fade = jnp.exp2(largest - now)
            powers = jnp.exp2(score - now)
            after.append(
                (
                    now,
                    total * fade + jnp.sum(powers, axis=0, keepdims=True),
                    kept * fade
                    + jnp.dot(
                        value, powers.astype(jnp.bfloat16), preferred_element_type=jnp.float32
                    ),
                )
            )
        return tuple(after)

    state = lax.fori_loop(0, me, step, tuple(state))
    for head, (_, total, kept) in enumerate(state):
        out_ref[:, head * nope : (head + 1) * nope] = jnp.transpose(kept / total).astype(
            out_ref.dtype
        )


def attend(me, queries_t, shared, ups, heads_here, nope, channels, scale):
    groups, tokens, width = shared.shape
    columns = heads_here * nope
    depth = queries_t.shape[1]
    return pl.pallas_call(
        functools.partial(attend_kernel, heads_here, nope, channels, scale),
        grid_spec=pltpu.PrefetchScalarGridSpec(
            num_scalar_prefetch=1,
            grid=(groups,),
            in_specs=[
                pl.BlockSpec((heads_here, depth, tokens), lambda g, me: (g, 0, 0)),
                pl.BlockSpec((groups, tokens, width), lambda g, me: (0, 0, 0)),
                pl.BlockSpec((ups.shape[0], 1) + ups.shape[2:], lambda g, me: (0, g, 0, 0)),
            ],
            out_specs=pl.BlockSpec((tokens, columns), lambda g, me: (0, g)),
        ),
        out_shape=jax.ShapeDtypeStruct((tokens, groups * columns), jnp.bfloat16),
        cost_estimate=pl.CostEstimate(
            flops=20 * groups * tokens * groups * tokens * columns,
            bytes_accessed=2 * groups * tokens * width,
            transcendentals=0,
        ),
    )(me, queries_t, shared, ups)


def project_kernel(heads_ref, weight_ref, resid_ref, gain_ref, after_ref, normed_ref, square_ref):
    part = pl.program_id(0)
    rows, width = weight_ref.shape[0] * weight_ref.shape[2], weight_ref.shape[3]
    weight = weight_ref[...].reshape(rows, width)
    projected = (
        jnp.dot(heads_ref[...], weight, preferred_element_type=jnp.float32)
        .astype(jnp.bfloat16)
        .astype(jnp.float32)
    )
    after = resid_ref[...].astype(jnp.float32) + projected
    after_ref[part] = after

    @pl.when(part == 0)
    def _():
        square_ref[...] = jnp.zeros_like(square_ref)

    square_ref[...] += jnp.sum(after * after, axis=1, keepdims=True)

    @pl.when(part == pl.num_programs(0) - 1)
    def _():
        parts = after_ref.shape[0]
        factor = lax.rsqrt(square_ref[...] / (parts * width) + epsilon)
        for at in range(parts):
            cols = slice(at * width, (at + 1) * width)
            normed_ref[at] = (after_ref[at] * factor * gain_ref[:, cols]).astype(normed_ref.dtype)


def project(heads, weights, resid, gain):
    groups, parts, rows, width = weights.shape
    tokens = heads.shape[0]
    return pl.pallas_call(
        project_kernel,
        grid=(parts,),
        in_specs=[
            pl.BlockSpec((tokens, groups * rows), lambda p: (0, 0)),
            pl.BlockSpec((groups, 1, rows, width), lambda p: (0, p, 0, 0)),
            pl.BlockSpec((tokens, width), lambda p: (0, p)),
            pl.BlockSpec((1, parts * width), lambda p: (0, 0)),
        ],
        out_specs=[
            pl.BlockSpec((parts, tokens, width), lambda p: (0, 0, 0)),
            pl.BlockSpec((parts, tokens, width), lambda p: (0, 0, 0)),
        ],
        out_shape=[
            jax.ShapeDtypeStruct((parts, tokens, width), jnp.float32),
            jax.ShapeDtypeStruct((parts, tokens, width), jnp.bfloat16),
        ],
        scratch_shapes=[pltpu.VMEM((tokens, 1), jnp.float32)],
        cost_estimate=pl.CostEstimate(
            flops=2 * tokens * groups * rows * parts * width,
            bytes_accessed=2 * groups * rows * parts * width,
            transcendentals=0,
        ),
    )(heads, weights, resid, gain)


def gather_kernel(
    outer, inner, dp_count, row_ref, piece_ref, rows_ref, pieces_ref,
    own_sems, far_send, far_recv, near_send, near_recv, dp_send, dp_recv,
):
    me = lax.axis_index("sp")
    dp = lax.axis_index("dp")
    far, near = me // inner, lax.rem(me, inner)
    barrier = pltpu.get_barrier_semaphore()
    fars = [lax.rem(far + step, outer) for step in range(1, outer)]
    nears = [lax.rem(near + step, inner) for step in range(1, inner)]
    dps = [lax.rem(dp + step, dp_count) for step in range(1, dp_count)]
    greeted = (
        [{"sp": f * inner + near} for f in fars]
        + [{"sp": far * inner + n} for n in nears]
        + [{"dp": d} for d in dps]
    )
    for peer in greeted:
        pl.semaphore_signal(barrier, inc=1, device_id=peer, device_id_type=pl.DeviceIdType.MESH)
    pl.semaphore_wait(barrier, len(greeted))

    def remote(source, target, send, recv, peer):
        copy = pltpu.make_async_remote_copy(
            src_ref=source, dst_ref=target, send_sem=send, recv_sem=recv,
            device_id=peer, device_id_type=pl.DeviceIdType.MESH,
        )
        copy.start()
        return copy

    def pair(row, piece, block, send, recv, peer):
        return [
            remote(row, rows_ref.at[block], send.at[0], recv.at[0], peer),
            remote(piece, pieces_ref.at[dp, block], send.at[1], recv.at[1], peer),
        ]

    out_far = []
    for at, f in enumerate(fars):
        out_far.append(pair(row_ref, piece_ref, me, far_send.at[at], far_recv.at[at], {"sp": f * inner + near}))
    last = []

    def share(block):
        for at, d in enumerate(dps):
            last.append(
                remote(
                    pieces_ref.at[dp, block], pieces_ref.at[dp, block],
                    dp_send.at[len(last)], dp_recv.at[len(last)], {"dp": d},
                )
            )

    sends = []
    for at, n in enumerate(nears):
        sends.append(pair(row_ref, piece_ref, me, near_send.at[0, at], near_recv.at[0, at], {"sp": far * inner + n}))
    own = [
        pltpu.make_async_copy(row_ref, rows_ref.at[me], own_sems.at[0]),
        pltpu.make_async_copy(piece_ref, pieces_ref.at[dp, me], own_sems.at[1]),
    ]
    for copy in own:
        copy.start()
    for copy in own:
        copy.wait()
    share(me)
    for at in range(outer - 1):
        for copy in out_far[at]:
            copy.wait_recv()
        block = lax.rem(far + outer - 1 - at, outer) * inner + near
        for to, n in enumerate(nears):
            sends.append(
                pair(
                    rows_ref.at[block], pieces_ref.at[dp, block], block,
                    near_send.at[at + 1, to], near_recv.at[at + 1, to], {"sp": far * inner + n},
                )
            )
        share(block)
    for at in range(outer):
        for to in range(inner - 1):
            for copy in sends[at * (inner - 1) + to]:
                copy.wait_recv()
            column = lax.rem(near + inner - 1 - to, inner)
            share(lax.rem(far + outer - at, outer) * inner + column)
    for copies in out_far + sends:
        for copy in copies:
            copy.wait_send()
    for copy in last:
        copy.wait()


def gather_shared(row, piece, sp_count, dp_count, number):
    outer, inner = split_of(sp_count)
    dma = pltpu.SemaphoreType.DMA
    return pl.pallas_call(
        functools.partial(gather_kernel, outer, inner, dp_count),
        out_shape=[
            jax.ShapeDtypeStruct((sp_count,) + row.shape, row.dtype),
            jax.ShapeDtypeStruct((dp_count, sp_count) + piece.shape, piece.dtype),
        ],
        in_specs=[pl.BlockSpec(memory_space=pltpu.VMEM)] * 2,
        out_specs=[pl.BlockSpec(memory_space=pltpu.VMEM)] * 2,
        scratch_shapes=[
            dma((2,)),
            dma((max(outer - 1, 1), 2)),
            dma((max(outer - 1, 1), 2)),
            dma((outer, max(inner - 1, 1), 2)),
            dma((outer, max(inner - 1, 1), 2)),
            dma((max(dp_count - 1, 1) * sp_count,)),
            dma((max(dp_count - 1, 1) * sp_count,)),
        ],
        compiler_params=pltpu.CompilerParams(collective_id=number, has_side_effects=True),
        cost_estimate=pl.CostEstimate(flops=2 * 10**10, bytes_accessed=10**7, transcendentals=0),
    )(row, piece)


def split_of(sp_count):
    inner = max(d for d in range(1, math.isqrt(sp_count) + 1) if sp_count % d == 0)
    return sp_count // inner, inner


def experts_kernel(
    outer, inner, capacity,
    normed_ref, meta_ref, after_ref, gate_hbm, up_hbm, down_hbm, out_ref,
    gate_w, up_w, down_w, blocks, metas, picked, rows, made, back, partial, coming, total, gate_acc, up_acc,
    weight_sems, meta_send, meta_recv, block_send, block_recv, row_send, row_recv,
    back_send, back_recv, sum_send, sum_recv,
):
    me = lax.axis_index("sp")
    z, y = me // inner, lax.rem(me, inner)
    parts, tokens, width = normed_ref.shape
    slots = inner * capacity
    loads = [
        pltpu.make_async_copy(hbm.at[0], ref, weight_sems.at[at])
        for at, (hbm, ref) in enumerate([(gate_hbm, gate_w), (up_hbm, up_w), (down_hbm, down_w)])
    ]
    for load in loads:
        load.start()

    barrier = pltpu.get_barrier_semaphore()
    steps_z = [lax.rem(z + step, outer) for step in range(1, outer)]
    steps_y = [lax.rem(y + step, inner) for step in range(1, inner)]
    greeted = [{"sp": at * inner + y} for at in steps_z] + [{"sp": z * inner + at} for at in steps_y]
    for peer in greeted:
        pl.semaphore_signal(barrier, inc=1, device_id=peer, device_id_type=pl.DeviceIdType.MESH)
    pl.semaphore_wait(barrier, len(greeted))

    def remote(source, target, send, recv, at_z, at_y):
        return pltpu.make_async_remote_copy(
            src_ref=source, dst_ref=target, send_sem=send, recv_sem=recv,
            device_id={"sp": at_z * inner + at_y}, device_id_type=pl.DeviceIdType.MESH,
        )

    def block_copy(source, part, own, way):
        ref = normed_ref.at[part] if own else blocks.at[source, part]
        return remote(
            ref, blocks.at[source, part],
            block_send.at[(way + 1) // 2, source, part], block_recv.at[source, part], z + way, y,
        )

    def meta_copy(step):
        at = lax.rem(z + step, outer)
        return remote(meta_ref.at[at], metas.at[z], meta_send.at[step - 1], meta_recv.at[z], at, y)

    def row_copy(source, step, part):
        at = lax.rem(y + step, inner)
        return remote(
            picked.at[source, at, part], rows.at[source, y, part],
            row_send.at[source, step - 1, part], row_recv.at[source, y, part], z, at,
        )

    def back_copy(source, step, part):
        at = lax.rem(y + step, inner)
        return remote(
            made.at[source, at, part], back.at[source, y, part],
            back_send.at[source, step - 1, part], back_recv.at[source, y, part], z, at,
        )

    def sum_copy(source, part, way):
        slot = source if way < 0 else jnp.where(source == z + 1, outer, source)
        return remote(
            partial.at[source, part], coming.at[slot, part],
            sum_send.at[source, part], sum_recv.at[slot, part], z + way, y,
        )

    def wait_recv(ref, sem):
        remote(ref, ref, block_send.at[0, 0, 0], sem, z, y).wait_recv()

    for step in range(1, outer):
        meta_copy(step).start()
    for part in range(parts):
        for way in (1, -1):

            @pl.when((z + way >= 0) & (z + way < outer))
            def _():
                block_copy(z, part, True, way).start()

    blocks[z] = normed_ref[...]
    metas[z] = meta_ref[z]

    orders = [sorted(range(outer), key=lambda s: (abs(s - at), s)) for at in range(outer)]

    def source_of(turn):
        found = jnp.int32(0)
        for at in range(outer):
            for index in range(outer):
                found = jnp.where((z == at) & (turn == index), orders[at][index], found)
        return found

    def forwards(source):
        return [
            (1, (source < z) & (z < outer - 1)),
            (-1, (source > z) & (z > 0)),
        ]

    def ends(source):
        return [
            (-1, (source < z) & (z == outer - 1)),
            (1, (source > z) & (z == 0)),
        ]

    def turn_body(turn, carry):
        source = source_of(turn)

        @pl.when(turn > 0)
        def _():
            wait_recv(metas.at[source], meta_recv.at[source])

        meta = metas[source]
        slot_ids = lax.broadcasted_iota(jnp.int32, (capacity, tokens), 0).astype(jnp.float32)
        select = jnp.concatenate(
            [
                jnp.where(meta[at : at + 1, :] == slot_ids, 1.0, 0.0).astype(jnp.bfloat16)
                for at in range(inner)
            ],
            axis=0,
        )

        def pick(part, carry):
            @pl.when(turn > 0)
            def _():
                wait_recv(blocks.at[source, part], block_recv.at[source, part])

            for way, needed in forwards(source):

                @pl.when(needed)
                def _():
                    block_copy(source, part, False, way).start()

            found = jnp.dot(
                select, blocks[source, part], preferred_element_type=jnp.float32
            ).astype(jnp.bfloat16)
            for at in range(inner):
                picked[source, at, part] = found[at * capacity : (at + 1) * capacity]
            rows[source, y, part] = picked[source, y, part]
            for step in range(1, inner):
                row_copy(source, step, part).start()
            return carry

        lax.fori_loop(0, parts, pick, 0)

        @pl.when(turn == 0)
        def _():
            for load in loads:
                load.wait()

        gate_acc[...] = jnp.zeros_like(gate_acc)
        up_acc[...] = jnp.zeros_like(up_acc)

        def widen(part, carry):
            for step in range(1, inner):
                at = lax.rem(y + step, inner)
                wait_recv(rows.at[source, at, part], row_recv.at[source, at, part])
            taken = jnp.concatenate([rows[source, at, part] for at in range(inner)], axis=0)
            depth = pl.ds(pl.multiple_of(part * width, width), width)
            gate_acc[...] += jnp.dot(taken, gate_w[depth, :], preferred_element_type=jnp.float32)
            up_acc[...] += jnp.dot(taken, up_w[depth, :], preferred_element_type=jnp.float32)
            return carry

        lax.fori_loop(0, parts, widen, 0)
        gate = gate_acc[...]
        hidden = (gate / (1.0 + jnp.exp(-gate)) * up_acc[...]).astype(jnp.bfloat16)

        for part in range(parts):
            cols = slice(part * width, (part + 1) * width)
            result = jnp.dot(hidden, down_w[:, cols], preferred_element_type=jnp.float32).astype(
                jnp.bfloat16
            )
            for at in range(inner):
                made[source, at, part] = result[at * capacity : (at + 1) * capacity]
            back[source, y, part] = made[source, y, part]
            for step in range(1, inner):
                back_copy(source, step, part).start()

        columns = jnp.transpose(meta)
        slot_lanes = lax.broadcasted_iota(jnp.int32, (tokens, capacity), 1).astype(jnp.float32)
        spread = [
            jnp.where(columns[:, at : at + 1] == slot_lanes, 1.0, 0.0).astype(jnp.bfloat16)
            for at in range(inner)
        ]

        def gather_back(part, carry):
            for step in range(1, inner):
                at = lax.rem(y + step, inner)
                wait_recv(back.at[source, at, part], back_recv.at[source, at, part])
            summed = sum(
                jnp.dot(spread[at], back[source, at, part], preferred_element_type=jnp.float32)
                * columns[:, inner + at : inner + at + 1]
                for at in range(inner)
            )

            @pl.when(turn == 0)
            def _():
                total[part] = after_ref[part] + summed

            @pl.when(turn > 0)
            def _():
                partial[source, part] = summed.astype(jnp.bfloat16)

            for way, needed in ends(source):

                @pl.when(needed)
                def _():
                    sum_copy(source, part, way).start()

            return carry

        lax.fori_loop(0, parts, gather_back, 0)
        return carry

    lax.fori_loop(0, outer, turn_body, 0)

    def relay(tick, carry):
        for way in (-1, 1):
            since = tick - (z if way > 0 else outer - 1 - z)
            part = lax.rem(since + parts * outer, parts)
            steps = (since + parts * outer) // parts - outer
            source = steps if way > 0 else outer - 1 - steps
            passing = (source > z) if way > 0 else (source < z)
            valid = (source >= 0) & (source < outer) & passing & (z - way >= 0) & (z - way < outer)

            @pl.when(valid)
            def _():
                wait_recv(coming.at[source, part], sum_recv.at[source, part])
                partial[source, part] = (
                    partial[source, part].astype(jnp.float32)
                    + coming[source, part].astype(jnp.float32)
                ).astype(jnp.bfloat16)
                sum_copy(source, part, way).start()

        return carry

    lax.fori_loop(0, outer * (parts + 1), relay, 0)

    for part in range(parts):
        for slot, valid in ((z, z < outer - 1), (outer, z > 0)):

            @pl.when(valid)
            def _():
                wait_recv(coming.at[slot, part], sum_recv.at[slot, part])
                total[part] += coming[slot, part].astype(jnp.float32)

        out_ref[:, part * width : (part + 1) * width] = total[part].astype(out_ref.dtype)

    for step in range(1, outer):
        meta_copy(step).wait_send()
    def drain(source, carry):
        for part in range(parts):
            for way in (1, -1):
                onward = (z + way >= 0) & (z + way < outer)
                passing = (source == z) | ((source < z) if way > 0 else (source > z))

                @pl.when(onward & passing)
                def _():
                    block_copy(source, part, False, way).wait_send()

                @pl.when(onward & ((source > z) if way > 0 else (source < z)))
                def _():
                    sum_copy(source, part, way).wait_send()

            for step in range(1, inner):
                row_copy(source, step, part).wait_send()
                back_copy(source, step, part).wait_send()
        return carry

    lax.fori_loop(0, outer, drain, 0)


def run_experts(normed, meta, after, gate, up, down, sp_count, capacity, number):
    outer, inner = split_of(sp_count)
    parts, tokens, width = normed.shape
    model, hidden = gate.shape[1:]
    dma = pltpu.SemaphoreType.DMA
    bf16, f32 = jnp.bfloat16, jnp.float32
    steps_y = max(inner - 1, 1)
    vmem = pl.BlockSpec(memory_space=pltpu.VMEM)
    anywhere = pl.BlockSpec(memory_space=pl.ANY)
    return pl.pallas_call(
        functools.partial(experts_kernel, outer, inner, capacity),
        out_shape=jax.ShapeDtypeStruct((tokens, parts * width), bf16),
        in_specs=[vmem, vmem, vmem, anywhere, anywhere, anywhere],
        out_specs=vmem,
        scratch_shapes=[
            pltpu.VMEM((model, hidden), bf16),
            pltpu.VMEM((model, hidden), bf16),
            pltpu.VMEM((hidden, model), bf16),
            pltpu.VMEM((outer, parts, tokens, width), bf16),
            pltpu.VMEM((outer,) + meta.shape[1:], f32),
            pltpu.VMEM((outer, inner, parts, capacity, width), bf16),
            pltpu.VMEM((outer, inner, parts, capacity, width), bf16),
            pltpu.VMEM((outer, inner, parts, capacity, width), bf16),
            pltpu.VMEM((outer, inner, parts, capacity, width), bf16),
            pltpu.VMEM((outer, parts, tokens, width), bf16),
            pltpu.VMEM((outer + 1, parts, tokens, width), bf16),
            pltpu.VMEM((parts, tokens, width), f32),
            pltpu.VMEM((inner * capacity, hidden), f32),
            pltpu.VMEM((inner * capacity, hidden), f32),
            dma((3,)),
            dma((outer,)),
            dma((outer,)),
            dma((2, outer, parts)),
            dma((outer, parts)),
            dma((outer, steps_y, parts)),
            dma((outer, inner, parts)),
            dma((outer, steps_y, parts)),
            dma((outer, inner, parts)),
            dma((outer, parts)),
            dma((outer + 1, parts)),
        ],
        compiler_params=pltpu.CompilerParams(
            collective_id=number, has_side_effects=True, vmem_limit_bytes=60 * 2**20
        ),
        cost_estimate=pl.CostEstimate(
            flops=6 * sp_count * capacity * model * hidden, bytes_accessed=10**7, transcendentals=0
        ),
    )(normed, meta, after, gate, up, down)


def shards(
    query_nope,
    query_rope,
    latent,
    key_rope,
    resid,
    latent_gain,
    key_up,
    value_up,
    out_proj,
    norm_gain,
    expert_gate,
    expert_up,
    expert_down,
    routes,
    route_weight,
):
    tokens, channels = latent.shape[1:]
    sp_count = lax.axis_size("sp")
    dp_count = lax.axis_size("dp")
    me = lax.axis_index("sp")
    nope, rope = query_nope.shape[-1], query_rope.shape[-1]
    heads_here = key_up.shape[1] // nope
    scale = (nope + rope) ** (-0.5)
    local_pos = me * tokens + jnp.arange(tokens, dtype=jnp.int32)
    latent_normed = rms_scaled(latent[0], latent_gain).astype(jnp.bfloat16)
    key_turned = rotate(key_rope[0], local_pos)
    spare = 128 - rope
    row = jnp.concatenate(
        [latent_normed, key_turned, jnp.zeros((tokens, spare), jnp.bfloat16)], axis=1
    )
    piece = channels // dp_count
    ups = lax.dynamic_slice_in_dim(
        jnp.concatenate([key_up, value_up], axis=1), lax.axis_index("dp") * piece, piece, axis=0
    )
    shared, ups = gather_shared(row, ups, sp_count, dp_count, 0)
    weights = lax.all_gather(out_proj, ("sp", "dp"), axis=0)
    weights = weights.reshape(sp_count, dp_count, *out_proj.shape)
    query_turned = rotate(query_rope[0], local_pos)
    queries = jnp.concatenate(
        [query_nope[0], query_turned, jnp.zeros(query_turned.shape[:2] + (128 - rope,), jnp.bfloat16)],
        axis=-1,
    )
    queries_t = jnp.transpose(queries, (1, 2, 0))
    heads = attend(
        me.astype(jnp.int32)[None], queries_t, shared, ups, heads_here, nope, channels, scale
    )
    after, normed = project(heads, weights, resid[0], norm_gain[None])

    experts_all = sp_count * expert_gate.shape[0]
    capacity = 4 * tokens // experts_all
    ids = jnp.arange(experts_all, dtype=jnp.int32)[:, None, None]
    mine = routes[0][None] == ids
    named = jnp.any(mine, axis=-1)
    weight = jnp.sum(jnp.where(mine, route_weight[0][None], 0.0), axis=-1)
    place = jnp.cumsum(named.astype(jnp.int32), axis=1) - 1
    outer, inner = split_of(sp_count)
    slot = jnp.where(named, place, -1).astype(jnp.float32).reshape(outer, inner, tokens)
    meta = jnp.concatenate([slot, weight.reshape(outer, inner, tokens)], axis=1)
    meta = jnp.pad(meta, ((0, 0), (0, -2 * inner % 8), (0, 0)))
    mixed = run_experts(
        normed, meta, after, expert_gate, expert_up, expert_down, sp_count, capacity, 1
    )
    return mixed[None]


def solution(mesh):
    return jax.shard_map(
        shards,
        mesh=mesh,
        in_specs=(
            P("dp", "sp", None, None),
            P("dp", "sp", None, None),
            P("dp", "sp", None),
            P("dp", "sp", None),
            P("dp", "sp", None),
            P(),
            P(None, "sp"),
            P(None, "sp"),
            P("sp", "dp"),
            P(),
            P("sp", None, None),
            P("sp", None, None),
            P("sp", None, None),
            P("dp", "sp", None),
            P("dp", "sp", None),
        ),
        out_specs=P("dp", "sp", None),
        check_vma=False,
    )
```

```python
import functools
import math

import jax
import jax.numpy as jnp
from jax import lax
from jax.experimental import pallas as pl
from jax.experimental.pallas import tpu as pltpu
from jax.sharding import PartitionSpec as P

epsilon = 1e-06
rope_base = 10000.0
masked_score = -1e30
log2_e = 1.4426950408889634


def rotate(values, positions):
    half_width = values.shape[-1] // 2
    frequency = rope_base ** (-jnp.arange(half_width, dtype=jnp.float32) / half_width)
    angles = positions.astype(jnp.float32)[:, None] * frequency[None, :]
    cosine = jnp.cos(angles)
    sine_part = jnp.sin(angles)
    if values.ndim == 3:
        cosine = cosine[:, None, :]
        sine_part = sine_part[:, None, :]
    floats = values.astype(jnp.float32)
    first_half = floats[..., :half_width]
    second_half = floats[..., half_width:]
    turned = jnp.concatenate(
        [
            first_half * cosine - second_half * sine_part,
            second_half * cosine + first_half * sine_part,
        ],
        axis=-1,
    )
    return turned.astype(jnp.bfloat16)


def rms_scaled(values, gain):
    floats = values.astype(jnp.float32)
    return floats * lax.rsqrt(jnp.mean(floats * floats, axis=-1, keepdims=True) + epsilon) * gain


def attend_kernel(heads_here, nope, channels, scale, me_ref, query_ref, shared_ref, ups_ref, out_ref):
    group = pl.program_id(0)
    columns = heads_here * nope
    me = me_ref[0]
    tokens = shared_ref.shape[1]
    ups = ups_ref[...].reshape(channels, 2 * columns)
    up_keys = ups[:, 0:columns]
    up_values = ups[:, columns : 2 * columns]
    up_values_t = jnp.transpose(up_values.astype(jnp.float32)).astype(jnp.bfloat16)

    def scores_of(chunk):
        latent = shared_ref[chunk, :, 0:channels]
        turned = shared_ref[chunk, :, channels:]
        keys = jnp.dot(latent, up_keys, preferred_element_type=jnp.float32).astype(jnp.bfloat16)
        values_t = lax.dot_general(
            up_values_t, latent, (((1,), (1,)), ((), ())), preferred_element_type=jnp.float32
        ).astype(jnp.bfloat16)
        scores = []
        for head in range(heads_here):
            full = jnp.concatenate([keys[:, head * nope : (head + 1) * nope], turned], axis=1)
            scores.append(
                jnp.dot(full, query_ref[head], preferred_element_type=jnp.float32)
                * (scale * log2_e)
            )
        return scores, [values_t[h * nope : (h + 1) * nope, :] for h in range(heads_here)]

    key_ids = lax.broadcasted_iota(jnp.int32, (tokens, tokens), 0)
    query_ids = lax.broadcasted_iota(jnp.int32, (tokens, tokens), 1)
    allowed = key_ids <= query_ids
    scores, values = scores_of(me)
    state = []
    for score, value in zip(scores, values):
        score = jnp.where(allowed, score, masked_score)
        largest = jnp.max(score, axis=0, keepdims=True)
        powers = jnp.exp2(score - largest)
        state.append(
            (
                largest,
                jnp.sum(powers, axis=0, keepdims=True),
                jnp.dot(value, powers.astype(jnp.bfloat16), preferred_element_type=jnp.float32),
            )
        )

    def step(chunk, state):
        scores, values = scores_of(chunk)
        after = []
        for (largest, total, kept), score, value in zip(state, scores, values):
            now = jnp.maximum(largest, jnp.max(score, axis=0, keepdims=True))
            fade = jnp.exp2(largest - now)
            powers = jnp.exp2(score - now)
            after.append(
                (
                    now,
                    total * fade + jnp.sum(powers, axis=0, keepdims=True),
                    kept * fade
                    + jnp.dot(
                        value, powers.astype(jnp.bfloat16), preferred_element_type=jnp.float32
                    ),
                )
            )
        return tuple(after)

    state = lax.fori_loop(0, me, step, tuple(state))
    for head, (_, total, kept) in enumerate(state):
        out_ref[:, head * nope : (head + 1) * nope] = jnp.transpose(kept / total).astype(
            out_ref.dtype
        )


def attend(me, queries_t, shared, ups, heads_here, nope, channels, scale):
    groups, tokens, width = shared.shape
    columns = heads_here * nope
    depth = queries_t.shape[1]
    return pl.pallas_call(
        functools.partial(attend_kernel, heads_here, nope, channels, scale),
        grid_spec=pltpu.PrefetchScalarGridSpec(
            num_scalar_prefetch=1,
            grid=(groups,),
            in_specs=[
                pl.BlockSpec((heads_here, depth, tokens), lambda g, me: (g, 0, 0)),
                pl.BlockSpec((groups, tokens, width), lambda g, me: (0, 0, 0)),
                pl.BlockSpec((ups.shape[0], 1) + ups.shape[2:], lambda g, me: (0, g, 0, 0)),
            ],
            out_specs=pl.BlockSpec((tokens, columns), lambda g, me: (0, g)),
        ),
        out_shape=jax.ShapeDtypeStruct((tokens, groups * columns), jnp.bfloat16),
        cost_estimate=pl.CostEstimate(
            flops=20 * groups * tokens * groups * tokens * columns,
            bytes_accessed=2 * groups * tokens * width,
            transcendentals=0,
        ),
    )(me, queries_t, shared, ups)


def project_kernel(heads_ref, weight_ref, resid_ref, gain_ref, after_ref, normed_ref, square_ref):
    part = pl.program_id(0)
    rows, width = weight_ref.shape[0] * weight_ref.shape[2], weight_ref.shape[3]
    weight = weight_ref[...].reshape(rows, width)
    projected = (
        jnp.dot(heads_ref[...], weight, preferred_element_type=jnp.float32)
        .astype(jnp.bfloat16)
        .astype(jnp.float32)
    )
    after = resid_ref[...].astype(jnp.float32) + projected
    after_ref[part] = after

    @pl.when(part == 0)
    def _():
        square_ref[...] = jnp.zeros_like(square_ref)

    square_ref[...] += jnp.sum(after * after, axis=1, keepdims=True)

    @pl.when(part == pl.num_programs(0) - 1)
    def _():
        parts = after_ref.shape[0]
        factor = lax.rsqrt(square_ref[...] / (parts * width) + epsilon)
        for at in range(parts):
            cols = slice(at * width, (at + 1) * width)
            normed_ref[at] = (after_ref[at] * factor * gain_ref[:, cols]).astype(normed_ref.dtype)


def project(heads, weights, resid, gain):
    groups, parts, rows, width = weights.shape
    tokens = heads.shape[0]
    return pl.pallas_call(
        project_kernel,
        grid=(parts,),
        in_specs=[
            pl.BlockSpec((tokens, groups * rows), lambda p: (0, 0)),
            pl.BlockSpec((groups, 1, rows, width), lambda p: (0, p, 0, 0)),
            pl.BlockSpec((tokens, width), lambda p: (0, p)),
            pl.BlockSpec((1, parts * width), lambda p: (0, 0)),
        ],
        out_specs=[
            pl.BlockSpec((parts, tokens, width), lambda p: (0, 0, 0)),
            pl.BlockSpec((parts, tokens, width), lambda p: (0, 0, 0)),
        ],
        out_shape=[
            jax.ShapeDtypeStruct((parts, tokens, width), jnp.float32),
            jax.ShapeDtypeStruct((parts, tokens, width), jnp.bfloat16),
        ],
        scratch_shapes=[pltpu.VMEM((tokens, 1), jnp.float32)],
        cost_estimate=pl.CostEstimate(
            flops=2 * tokens * groups * rows * parts * width,
            bytes_accessed=2 * groups * rows * parts * width,
            transcendentals=0,
        ),
    )(heads, weights, resid, gain)


def gather_kernel(
    outer, inner, dp_count, row_ref, piece_ref, rows_ref, pieces_ref,
    own_sems, far_send, far_recv, near_send, near_recv, dp_send, dp_recv,
):
    me = lax.axis_index("sp")
    dp = lax.axis_index("dp")
    far, near = me // inner, lax.rem(me, inner)
    barrier = pltpu.get_barrier_semaphore()
    fars = [lax.rem(far + step, outer) for step in range(1, outer)]
    nears = [lax.rem(near + step, inner) for step in range(1, inner)]
    dps = [lax.rem(dp + step, dp_count) for step in range(1, dp_count)]
    greeted = (
        [{"sp": f * inner + near} for f in fars]
        + [{"sp": far * inner + n} for n in nears]
        + [{"dp": d} for d in dps]
    )
    for peer in greeted:
        pl.semaphore_signal(barrier, inc=1, device_id=peer, device_id_type=pl.DeviceIdType.MESH)
    pl.semaphore_wait(barrier, len(greeted))

    def remote(source, target, send, recv, peer):
        copy = pltpu.make_async_remote_copy(
            src_ref=source, dst_ref=target, send_sem=send, recv_sem=recv,
            device_id=peer, device_id_type=pl.DeviceIdType.MESH,
        )
        copy.start()
        return copy

    def pair(row, piece, block, send, recv, peer):
        return [
            remote(row, rows_ref.at[block], send.at[0], recv.at[0], peer),
            remote(piece, pieces_ref.at[dp, block], send.at[1], recv.at[1], peer),
        ]

    out_far = []
    for at, f in enumerate(fars):
        out_far.append(pair(row_ref, piece_ref, me, far_send.at[at], far_recv.at[at], {"sp": f * inner + near}))
    last = []

    def share(block):
        for at, d in enumerate(dps):
            last.append(
                remote(
                    pieces_ref.at[dp, block], pieces_ref.at[dp, block],
                    dp_send.at[len(last)], dp_recv.at[len(last)], {"dp": d},
                )
            )

    sends = []
    for at, n in enumerate(nears):
        sends.append(pair(row_ref, piece_ref, me, near_send.at[0, at], near_recv.at[0, at], {"sp": far * inner + n}))
    own = [
        pltpu.make_async_copy(row_ref, rows_ref.at[me], own_sems.at[0]),
        pltpu.make_async_copy(piece_ref, pieces_ref.at[dp, me], own_sems.at[1]),
    ]
    for copy in own:
        copy.start()
    for copy in own:
        copy.wait()
    share(me)
    for at in range(outer - 1):
        for copy in out_far[at]:
            copy.wait_recv()
        block = lax.rem(far + outer - 1 - at, outer) * inner + near
        for to, n in enumerate(nears):
            sends.append(
                pair(
                    rows_ref.at[block], pieces_ref.at[dp, block], block,
                    near_send.at[at + 1, to], near_recv.at[at + 1, to], {"sp": far * inner + n},
                )
            )
        share(block)
    for at in range(outer):
        for to in range(inner - 1):
            for copy in sends[at * (inner - 1) + to]:
                copy.wait_recv()
            column = lax.rem(near + inner - 1 - to, inner)
            share(lax.rem(far + outer - at, outer) * inner + column)
    for copies in out_far + sends:
        for copy in copies:
            copy.wait_send()
    for copy in last:
        copy.wait()


def gather_shared(row, piece, sp_count, dp_count, number):
    outer, inner = split_of(sp_count)
    dma = pltpu.SemaphoreType.DMA
    return pl.pallas_call(
        functools.partial(gather_kernel, outer, inner, dp_count),
        out_shape=[
            jax.ShapeDtypeStruct((sp_count,) + row.shape, row.dtype),
            jax.ShapeDtypeStruct((dp_count, sp_count) + piece.shape, piece.dtype),
        ],
        in_specs=[pl.BlockSpec(memory_space=pltpu.VMEM)] * 2,
        out_specs=[pl.BlockSpec(memory_space=pltpu.VMEM)] * 2,
        scratch_shapes=[
            dma((2,)),
            dma((max(outer - 1, 1), 2)),
            dma((max(outer - 1, 1), 2)),
            dma((outer, max(inner - 1, 1), 2)),
            dma((outer, max(inner - 1, 1), 2)),
            dma((max(dp_count - 1, 1) * sp_count,)),
            dma((max(dp_count - 1, 1) * sp_count,)),
        ],
        compiler_params=pltpu.CompilerParams(collective_id=number, has_side_effects=True),
        cost_estimate=pl.CostEstimate(flops=2 * 10**10, bytes_accessed=10**7, transcendentals=0),
    )(row, piece)


def split_of(sp_count):
    inner = max(d for d in range(1, math.isqrt(sp_count) + 1) if sp_count % d == 0)
    return sp_count // inner, inner


def experts_kernel(
    outer, inner, capacity,
    normed_ref, meta_ref, after_ref, gate_hbm, up_hbm, down_hbm, out_ref,
    gate_w, up_w, down_w, blocks, metas, picked, rows, made, back, partial, coming, total, gate_acc, up_acc,
    select, columns, spread,
    weight_sems, meta_send, meta_recv, block_send, block_recv, row_send, row_recv,
    back_send, back_recv, sum_send, sum_recv,
):
    me = lax.axis_index("sp")
    z, y = me // inner, lax.rem(me, inner)
    parts, tokens, width = normed_ref.shape
    loads = [
        pltpu.make_async_copy(hbm.at[0], ref, weight_sems.at[at])
        for at, (hbm, ref) in enumerate([(gate_hbm, gate_w), (up_hbm, up_w), (down_hbm, down_w)])
    ]
    for load in loads:
        load.start()

    barrier = pltpu.get_barrier_semaphore()
    steps_z = [lax.rem(z + step, outer) for step in range(1, outer)]
    steps_y = [lax.rem(y + step, inner) for step in range(1, inner)]
    greeted = [{"sp": at * inner + y} for at in steps_z] + [{"sp": z * inner + at} for at in steps_y]
    for peer in greeted:
        pl.semaphore_signal(barrier, inc=1, device_id=peer, device_id_type=pl.DeviceIdType.MESH)
    pl.semaphore_wait(barrier, len(greeted))

    def remote(source, target, send, recv, at_z, at_y):
        return pltpu.make_async_remote_copy(
            src_ref=source, dst_ref=target, send_sem=send, recv_sem=recv,
            device_id={"sp": at_z * inner + at_y}, device_id_type=pl.DeviceIdType.MESH,
        )

    def block_copy(source, part, own, way):
        ref = normed_ref.at[part] if own else blocks.at[source, part]
        return remote(
            ref, blocks.at[source, part],
            block_send.at[(way + 1) // 2, source, part], block_recv.at[source, part], z + way, y,
        )

    def meta_copy(step):
        at = lax.rem(z + step, outer)
        return remote(meta_ref.at[at], metas.at[z], meta_send.at[step - 1], meta_recv.at[z], at, y)

    def row_copy(source, step, part):
        at = lax.rem(y + step, inner)
        return remote(
            picked.at[source, at, part], rows.at[source, y, part],
            row_send.at[source, step - 1, part], row_recv.at[source, y, part], z, at,
        )

    def back_copy(source, step, part):
        at = lax.rem(y + step, inner)
        return remote(
            made.at[source, at, part], back.at[source, y, part],
            back_send.at[source, step - 1, part], back_recv.at[source, y, part], z, at,
        )

    def sum_copy(source, part, way):
        slot = source if way < 0 else jnp.where(source == z + 1, outer, source)
        return remote(
            partial.at[source, part], coming.at[slot, part],
            sum_send.at[source, part], sum_recv.at[slot, part], z + way, y,
        )

    def wait_recv(ref, sem):
        remote(ref, ref, block_send.at[0, 0, 0], sem, z, y).wait_recv()

    for step in range(1, outer):
        meta_copy(step).start()
    for part in range(parts):
        for way in (1, -1):

            @pl.when((z + way >= 0) & (z + way < outer))
            def _():
                block_copy(z, part, True, way).start()

    blocks[z] = normed_ref[...]
    metas[z] = meta_ref[z]

    orders = [sorted(range(outer), key=lambda s: (abs(s - at), s)) for at in range(outer)]

    def source_of(turn):
        found = jnp.int32(0)
        for at in range(outer):
            for index in range(outer):
                found = jnp.where((z == at) & (turn == index), orders[at][index], found)
        return found

    def forwards(source):
        return [
            (1, (source < z) & (z < outer - 1)),
            (-1, (source > z) & (z > 0)),
        ]

    def ends(source):
        return [
            (-1, (source < z) & (z == outer - 1)),
            (1, (source > z) & (z == 0)),
        ]

    def needs(source):
        return functools.reduce(jnp.logical_or, [needed for _, needed in forwards(source)])

    def arrive(source, part):
        wait_recv(blocks.at[source, part], block_recv.at[source, part])

    def forward(source, part):
        for way, needed in forwards(source):

            @pl.when(needed)
            def _():
                block_copy(source, part, False, way).start()

    def open_turn(turn):
        source = source_of(turn)

        @pl.when(turn > 0)
        def _():
            wait_recv(metas.at[source], meta_recv.at[source])

        slot_ids = lax.broadcasted_iota(jnp.int32, (capacity, tokens), 0).astype(jnp.float32)
        for at in range(inner):
            select[at * capacity : (at + 1) * capacity] = jnp.where(
                metas[source, at : at + 1, :] == slot_ids, 1.0, 0.0
            ).astype(jnp.bfloat16)

    def pick(turn, part):
        source = source_of(turn)

        @pl.when((turn == 1) | ((turn > 1) & ~needs(source)))
        def _():
            arrive(source, part)

        @pl.when(turn == 1)
        def _():
            forward(source, part)

        later = source_of(turn + 1)

        @pl.when((turn > 0) & (turn + 1 < outer) & needs(later))
        def _():
            arrive(later, part)
            forward(later, part)

        found = jnp.dot(
            select[...], blocks[source, part], preferred_element_type=jnp.float32
        ).astype(jnp.bfloat16)
        for at in range(inner):
            picked[source, at, part] = found[at * capacity : (at + 1) * capacity]
        rows[source, y, part] = picked[source, y, part]
        for step in range(1, inner):
            row_copy(source, step, part).start()

    def apply_experts(turn):
        source = source_of(turn)

        @pl.when(turn == 0)
        def _():
            for load in loads:
                load.wait()

        gate_acc[...] = jnp.zeros_like(gate_acc)
        up_acc[...] = jnp.zeros_like(up_acc)

        def widen(part, carry):
            for step in range(1, inner):
                at = lax.rem(y + step, inner)
                wait_recv(rows.at[source, at, part], row_recv.at[source, at, part])
            taken = jnp.concatenate([rows[source, at, part] for at in range(inner)], axis=0)
            depth = pl.ds(pl.multiple_of(part * width, width), width)
            gate_acc[...] += jnp.dot(taken, gate_w[depth, :], preferred_element_type=jnp.float32)
            up_acc[...] += jnp.dot(taken, up_w[depth, :], preferred_element_type=jnp.float32)
            return carry

        lax.fori_loop(0, parts, widen, 0)
        gate = gate_acc[...]
        hidden = (gate / (1.0 + jnp.exp(-gate)) * up_acc[...]).astype(jnp.bfloat16)

        for part in range(parts):
            cols = slice(part * width, (part + 1) * width)
            result = jnp.dot(hidden, down_w[:, cols], preferred_element_type=jnp.float32).astype(
                jnp.bfloat16
            )
            for at in range(inner):
                made[source, at, part] = result[at * capacity : (at + 1) * capacity]
            back[source, y, part] = made[source, y, part]
            for step in range(1, inner):
                back_copy(source, step, part).start()

        columns[...] = jnp.transpose(metas[source])
        slot_lanes = lax.broadcasted_iota(jnp.int32, (tokens, capacity), 1).astype(jnp.float32)
        for at in range(inner):
            spread[at] = jnp.where(columns[:, at : at + 1] == slot_lanes, 1.0, 0.0).astype(
                jnp.bfloat16
            )

    def combine(turn, part):
        source = source_of(turn)
        for step in range(1, inner):
            at = lax.rem(y + step, inner)
            wait_recv(back.at[source, at, part], back_recv.at[source, at, part])
        summed = sum(
            jnp.dot(spread[at], back[source, at, part], preferred_element_type=jnp.float32)
            * columns[:, inner + at : inner + at + 1]
            for at in range(inner)
        )

        @pl.when(turn == 0)
        def _():
            total[part] = after_ref[part] + summed

        @pl.when(turn > 0)
        def _():
            partial[source, part] = summed.astype(jnp.bfloat16)

        for way, needed in ends(source):

            @pl.when(needed)
            def _():
                sum_copy(source, part, way).start()

    def turn_body(turn, carry):
        here, before = turn < outer, turn > 0

        @pl.when(here)
        def _():
            open_turn(turn)
            pick(turn, 0)

        @pl.when(before)
        def _():
            apply_experts(turn - 1)

        done = 0
        for part in range(1, parts):

            @pl.when(here)
            def _():
                pick(turn, part)

            upto = parts * part // (parts - 1)

            @pl.when(before)
            def _():
                for at in range(done, upto):
                    combine(turn - 1, at)

            done = upto
        return carry

    lax.fori_loop(0, outer + 1, turn_body, 0)

    def relay(tick, carry):
        for way in (-1, 1):
            since = tick - (z if way > 0 else outer - 1 - z)
            part = lax.rem(since + parts * outer, parts)
            steps = (since + parts * outer) // parts - outer
            source = steps if way > 0 else outer - 1 - steps
            passing = (source > z) if way > 0 else (source < z)
            valid = (source >= 0) & (source < outer) & passing & (z - way >= 0) & (z - way < outer)

            @pl.when(valid)
            def _():
                wait_recv(coming.at[source, part], sum_recv.at[source, part])
                partial[source, part] = (
                    partial[source, part].astype(jnp.float32)
                    + coming[source, part].astype(jnp.float32)
                ).astype(jnp.bfloat16)
                sum_copy(source, part, way).start()

        return carry

    lax.fori_loop(0, outer * (parts + 1), relay, 0)

    for part in range(parts):
        for slot, valid in ((z, z < outer - 1), (outer, z > 0)):

            @pl.when(valid)
            def _():
                wait_recv(coming.at[slot, part], sum_recv.at[slot, part])
                total[part] += coming[slot, part].astype(jnp.float32)

        out_ref[:, part * width : (part + 1) * width] = total[part].astype(out_ref.dtype)

    for step in range(1, outer):
        meta_copy(step).wait_send()
    def drain(source, carry):
        for part in range(parts):
            for way in (1, -1):
                onward = (z + way >= 0) & (z + way < outer)
                passing = (source == z) | ((source < z) if way > 0 else (source > z))

                @pl.when(onward & passing)
                def _():
                    block_copy(source, part, False, way).wait_send()

                @pl.when(onward & ((source > z) if way > 0 else (source < z)))
                def _():
                    sum_copy(source, part, way).wait_send()

            for step in range(1, inner):
                row_copy(source, step, part).wait_send()
                back_copy(source, step, part).wait_send()
        return carry

    lax.fori_loop(0, outer, drain, 0)


def run_experts(normed, meta, after, gate, up, down, sp_count, capacity, number):
    outer, inner = split_of(sp_count)
    parts, tokens, width = normed.shape
    model, hidden = gate.shape[1:]
    dma = pltpu.SemaphoreType.DMA
    bf16, f32 = jnp.bfloat16, jnp.float32
    steps_y = max(inner - 1, 1)
    vmem = pl.BlockSpec(memory_space=pltpu.VMEM)
    anywhere = pl.BlockSpec(memory_space=pl.ANY)
    return pl.pallas_call(
        functools.partial(experts_kernel, outer, inner, capacity),
        out_shape=jax.ShapeDtypeStruct((tokens, parts * width), bf16),
        in_specs=[vmem, vmem, vmem, anywhere, anywhere, anywhere],
        out_specs=vmem,
        scratch_shapes=[
            pltpu.VMEM((model, hidden), bf16),
            pltpu.VMEM((model, hidden), bf16),
            pltpu.VMEM((hidden, model), bf16),
            pltpu.VMEM((outer, parts, tokens, width), bf16),
            pltpu.VMEM((outer,) + meta.shape[1:], f32),
            pltpu.VMEM((outer, inner, parts, capacity, width), bf16),
            pltpu.VMEM((outer, inner, parts, capacity, width), bf16),
            pltpu.VMEM((outer, inner, parts, capacity, width), bf16),
            pltpu.VMEM((outer, inner, parts, capacity, width), bf16),
            pltpu.VMEM((outer, parts, tokens, width), bf16),
            pltpu.VMEM((outer + 1, parts, tokens, width), bf16),
            pltpu.VMEM((parts, tokens, width), f32),
            pltpu.VMEM((inner * capacity, hidden), f32),
            pltpu.VMEM((inner * capacity, hidden), f32),
            pltpu.VMEM((inner * capacity, tokens), bf16),
            pltpu.VMEM((tokens, meta.shape[1]), f32),
            pltpu.VMEM((inner, tokens, capacity), bf16),
            dma((3,)),
            dma((outer,)),
            dma((outer,)),
            dma((2, outer, parts)),
            dma((outer, parts)),
            dma((outer, steps_y, parts)),
            dma((outer, inner, parts)),
            dma((outer, steps_y, parts)),
            dma((outer, inner, parts)),
            dma((outer, parts)),
            dma((outer + 1, parts)),
        ],
        compiler_params=pltpu.CompilerParams(
            collective_id=number, has_side_effects=True, vmem_limit_bytes=60 * 2**20
        ),
        cost_estimate=pl.CostEstimate(
            flops=6 * sp_count * capacity * model * hidden, bytes_accessed=10**7, transcendentals=0
        ),
    )(normed, meta, after, gate, up, down)


def shards(
    query_nope,
    query_rope,
    latent,
    key_rope,
    resid,
    latent_gain,
    key_up,
    value_up,
    out_proj,
    norm_gain,
    expert_gate,
    expert_up,
    expert_down,
    routes,
    route_weight,
):
    tokens, channels = latent.shape[1:]
    sp_count = lax.axis_size("sp")
    dp_count = lax.axis_size("dp")
    me = lax.axis_index("sp")
    nope, rope = query_nope.shape[-1], query_rope.shape[-1]
    heads_here = key_up.shape[1] // nope
    scale = (nope + rope) ** (-0.5)
    local_pos = me * tokens + jnp.arange(tokens, dtype=jnp.int32)
    latent_normed = rms_scaled(latent[0], latent_gain).astype(jnp.bfloat16)
    key_turned = rotate(key_rope[0], local_pos)
    spare = 128 - rope
    row = jnp.concatenate(
        [latent_normed, key_turned, jnp.zeros((tokens, spare), jnp.bfloat16)], axis=1
    )
    piece = channels // dp_count
    ups = lax.dynamic_slice_in_dim(
        jnp.concatenate([key_up, value_up], axis=1), lax.axis_index("dp") * piece, piece, axis=0
    )
    shared, ups = gather_shared(row, ups, sp_count, dp_count, 0)
    weights = lax.all_gather(out_proj, ("sp", "dp"), axis=0)
    weights = weights.reshape(sp_count, dp_count, *out_proj.shape)
    query_turned = rotate(query_rope[0], local_pos)
    queries = jnp.concatenate(
        [query_nope[0], query_turned, jnp.zeros(query_turned.shape[:2] + (128 - rope,), jnp.bfloat16)],
        axis=-1,
    )
    queries_t = jnp.transpose(queries, (1, 2, 0))
    heads = attend(
        me.astype(jnp.int32)[None], queries_t, shared, ups, heads_here, nope, channels, scale
    )
    after, normed = project(heads, weights, resid[0], norm_gain[None])

    experts_all = sp_count * expert_gate.shape[0]
    capacity = 4 * tokens // experts_all
    ids = jnp.arange(experts_all, dtype=jnp.int32)[:, None, None]
    mine = routes[0][None] == ids
    named = jnp.any(mine, axis=-1)
    weight = jnp.sum(jnp.where(mine, route_weight[0][None], 0.0), axis=-1)
    place = jnp.cumsum(named.astype(jnp.int32), axis=1) - 1
    outer, inner = split_of(sp_count)
    slot = jnp.where(named, place, -1).astype(jnp.float32).reshape(outer, inner, tokens)
    meta = jnp.concatenate([slot, weight.reshape(outer, inner, tokens)], axis=1)
    meta = jnp.pad(meta, ((0, 0), (0, -2 * inner % 8), (0, 0)))
    mixed = run_experts(
        normed, meta, after, expert_gate, expert_up, expert_down, sp_count, capacity, 1
    )
    return mixed[None]


def solution(mesh):
    return jax.shard_map(
        shards,
        mesh=mesh,
        in_specs=(
            P("dp", "sp", None, None),
            P("dp", "sp", None, None),
            P("dp", "sp", None),
            P("dp", "sp", None),
            P("dp", "sp", None),
            P(),
            P(None, "sp"),
            P(None, "sp"),
            P("sp", "dp"),
            P(),
            P("sp", None, None),
            P("sp", None, None),
            P("sp", None, None),
            P("dp", "sp", None),
            P("dp", "sp", None),
        ),
        out_specs=P("dp", "sp", None),
        check_vma=False,
    )
```

```python
import functools
import math

import jax
import jax.numpy as jnp
from jax import lax
from jax.experimental import pallas as pl
from jax.experimental.pallas import tpu as pltpu
from jax.sharding import PartitionSpec as P

epsilon = 1e-06
rope_base = 10000.0
masked_score = -1e30
log2_e = 1.4426950408889634


def rotate(values, positions):
    half_width = values.shape[-1] // 2
    frequency = rope_base ** (-jnp.arange(half_width, dtype=jnp.float32) / half_width)
    angles = positions.astype(jnp.float32)[:, None] * frequency[None, :]
    cosine = jnp.cos(angles)
    sine_part = jnp.sin(angles)
    if values.ndim == 3:
        cosine = cosine[:, None, :]
        sine_part = sine_part[:, None, :]
    floats = values.astype(jnp.float32)
    first_half = floats[..., :half_width]
    second_half = floats[..., half_width:]
    turned = jnp.concatenate(
        [
            first_half * cosine - second_half * sine_part,
            second_half * cosine + first_half * sine_part,
        ],
        axis=-1,
    )
    return turned.astype(jnp.bfloat16)


def rms_scaled(values, gain):
    floats = values.astype(jnp.float32)
    return floats * lax.rsqrt(jnp.mean(floats * floats, axis=-1, keepdims=True) + epsilon) * gain


def front_kernel(
    outer, inner, cores, heads_here, nope, channels, scale,
    row_ref, piece_ref, block_ref, query_ref, resid_ref, gain_ref, after_ref, normed_ref,
    shared, ups, weights, heads, *sems,
):
    me, dp = lax.axis_index("sp"), lax.axis_index("dp")
    z, y = me // inner, lax.rem(me, inner)
    lanes = weights.shape[0] // cores
    x, core = dp // cores, lax.rem(dp, cores)
    groups, tokens = shared.shape[0], shared.shape[1]
    columns = heads_here * nope
    total = groups * columns
    row_sems, piece_sems, block_sems = sems[0:4], sems[4:12], sems[12:20]

    def remote(source, target, send, recv, peer):
        return pltpu.make_async_remote_copy(
            src_ref=source, dst_ref=target, send_sem=send, recv_sem=recv,
            device_id=peer, device_id_type=pl.DeviceIdType.MESH,
        )

    def at_z(step):
        return {"sp": lax.rem(z + step, outer) * inner + y}

    def at_y(step):
        return {"sp": z * inner + lax.rem(y + step, inner)}

    def at_x(step):
        return {"dp": lax.rem(x + step, lanes) * cores + core}

    def at_core(step):
        return {"dp": x * cores + lax.rem(core + step, cores)}

    barrier = pltpu.get_barrier_semaphore()
    greeted = (
        [at_z(step) for step in range(1, outer)]
        + [at_y(step) for step in range(1, inner)]
        + [at_x(step) for step in range(1, lanes)]
        + [at_core(step) for step in range(1, cores)]
    )
    for peer in greeted:
        pl.semaphore_signal(barrier, inc=1, device_id=peer, device_id_type=pl.DeviceIdType.MESH)
    pl.semaphore_wait(barrier, len(greeted))

    def member(index):
        along_z, along_y = lax.rem(index, outer), index // outer
        return lax.rem(z + along_z, outer) * inner + lax.rem(y + along_y, inner)

    class Spread:
        def __init__(self, own, held, sems, wide):
            self.own, self.held, self.sems, self.wide = own, held, sems, wide

        def place(self, block, row=None):
            return self.held.at[block] if not self.wide else self.held.at[dp if row is None else row, block]

        def along_z(self, step):
            return remote(self.own, self.place(me), self.sems[0].at[step - 1], self.sems[1].at[step - 1], at_z(step))

        def along_y(self, step, index):
            source = self.own if isinstance(index, int) and index == 0 else self.place(member(index))
            return remote(
                source, self.place(member(index)),
                self.sems[2].at[step - 1, index], self.sems[3].at[step - 1, index], at_y(step),
            )

        def along_x(self, step, index):
            source = self.own if isinstance(index, int) and index == 0 else self.place(member(index))
            return remote(
                source, self.place(member(index)),
                self.sems[4].at[step - 1, index], self.sems[5].at[step - 1, index], at_x(step),
            )

        def across(self, step, lane, index):
            row = lax.rem(x + lane, lanes) * cores + core
            own = isinstance(index, int) and index == 0 and lane == 0
            source = self.own if own else self.place(member(index), row)
            return remote(
                source, self.place(member(index), row),
                self.sems[6].at[step - 1, lane, index], self.sems[7].at[step - 1, lane, index], at_core(step),
            )

        def wait(self, ref, sem):
            remote(ref, ref, self.sems[0].at[0], sem, at_z(0)).wait_recv()

        def start_z(self):
            for step in range(1, outer):
                self.along_z(step).start()

        def start_y(self, index):
            for step in range(1, inner):
                self.along_y(step, index).start()

        def start_wide(self, index):
            for step in range(1, lanes):
                self.along_x(step, index).start()
            for step in range(1, cores):
                self.across(step, 0, index).start()

        def from_z(self, index):
            step = (outer - index) % outer
            self.wait(self.place(member(index)), self.sems[1].at[step - 1])

        def from_y(self, index):
            step = inner - index // outer
            self.wait(self.place(member(index)), self.sems[3].at[step - 1, lax.rem(index, outer)])

        def from_x(self, lane, index):
            row = lax.rem(x + lane, lanes) * cores + core
            self.wait(self.place(member(index), row), self.sems[5].at[lanes - lane - 1, index])
            for step in range(1, cores):
                self.across(step, lane, index).start()

        def from_core(self, step, lane, index):
            row = lax.rem(x + lane, lanes) * cores + lax.rem(core + step, cores)
            self.wait(self.place(member(index), row), self.sems[7].at[cores - step - 1, lane, index])

        def drain(self):
            for step in range(1, outer):
                self.along_z(step).wait_send()
            for index in range(outer):
                for step in range(1, inner):
                    self.along_y(step, index).wait_send()
            if self.wide:

                def one(index, carry):
                    for step in range(1, lanes):
                        self.along_x(step, index).wait_send()
                    for step in range(1, cores):
                        for lane in range(lanes):
                            self.across(step, lane, index).wait_send()
                    return carry

                lax.fori_loop(0, groups, one, 0)

    row = Spread(row_ref, shared, row_sems, False)
    piece = Spread(piece_ref, ups, piece_sems, True)
    block = Spread(block_ref, weights, block_sems, True)
    row.start_z()
    piece.start_z()
    row.start_y(0)
    piece.start_y(0)
    piece.start_wide(0)
    shared[me] = row_ref[...]
    ups[dp, me] = piece_ref[...]
    weights[dp, me] = block_ref[...]
    for index in range(1, outer):
        row.from_z(index)
        row.start_y(index)
        piece.from_z(index)
        piece.start_y(index)
        piece.start_wide(index)
    block.start_z()
    block.start_y(0)
    block.start_wide(0)
    for index in range(outer, groups):
        row.from_y(index)
        piece.from_y(index)
        piece.start_wide(index)
    for lane in range(1, lanes):
        for index in range(groups):
            piece.from_x(lane, index)

    def settle(spread):
        def one(index, carry):
            for lane in range(lanes):
                for step in range(1, cores):
                    spread.from_core(step, lane, index)
            return carry

        lax.fori_loop(0, groups, one, 0)

    settle(piece)

    key_ids = lax.broadcasted_iota(jnp.int32, (tokens, tokens), 0)
    query_ids = lax.broadcasted_iota(jnp.int32, (tokens, tokens), 1)
    allowed = key_ids <= query_ids

    def attend_group(group):
        up = ups[:, group].reshape(channels, 2 * columns)
        up_keys = up[:, 0:columns]
        up_values = up[:, columns : 2 * columns]
        up_values_t = jnp.transpose(up_values.astype(jnp.float32)).astype(jnp.bfloat16)

        def scores_of(chunk):
            latent = shared[chunk, :, 0:channels]
            turned = shared[chunk, :, channels:]
            keys = jnp.dot(latent, up_keys, preferred_element_type=jnp.float32).astype(jnp.bfloat16)
            values_t = lax.dot_general(
                up_values_t, latent, (((1,), (1,)), ((), ())), preferred_element_type=jnp.float32
            ).astype(jnp.bfloat16)
            scores = []
            for head in range(heads_here):
                full = jnp.concatenate([keys[:, head * nope : (head + 1) * nope], turned], axis=1)
                scores.append(
                    jnp.dot(
                        full, query_ref[group * heads_here + head], preferred_element_type=jnp.float32
                    )
                    * (scale * log2_e)
                )
            return scores, [values_t[h * nope : (h + 1) * nope, :] for h in range(heads_here)]

        scores, values = scores_of(me)
        state = []
        for score, value in zip(scores, values):
            score = jnp.where(allowed, score, masked_score)
            largest = jnp.max(score, axis=0, keepdims=True)
            powers = jnp.exp2(score - largest)
            state.append(
                (
                    largest,
                    jnp.sum(powers, axis=0, keepdims=True),
                    jnp.dot(value, powers.astype(jnp.bfloat16), preferred_element_type=jnp.float32),
                )
            )

        def step(chunk, state):
            scores, values = scores_of(chunk)
            after = []
            for (largest, total, kept), score, value in zip(state, scores, values):
                now = jnp.maximum(largest, jnp.max(score, axis=0, keepdims=True))
                fade = jnp.exp2(largest - now)
                powers = jnp.exp2(score - now)
                after.append(
                    (
                        now,
                        total * fade + jnp.sum(powers, axis=0, keepdims=True),
                        kept * fade
                        + jnp.dot(
                            value, powers.astype(jnp.bfloat16), preferred_element_type=jnp.float32
                        ),
                    )
                )
            return tuple(after)

        state = lax.fori_loop(0, me, step, tuple(state))
        for head, (_, total, kept) in enumerate(state):
            start = pl.multiple_of(group * columns + head * nope, nope)
            heads[:, pl.ds(start, nope)] = jnp.transpose(kept / total).astype(heads.dtype)

    def one_group(group, carry):
        attend_group(group)

        @pl.when(group == 0)
        def _():
            for index in range(1, outer):
                block.from_z(index)
                block.start_y(index)
                block.start_wide(index)

        nearby = group + outer - 1

        @pl.when((group > 0) & (nearby < groups))
        def _():
            block.from_y(nearby)
            block.start_wide(nearby)

        @pl.when(group >= 2)
        def _():
            for lane in range(1, lanes):
                block.from_x(lane, group - 2)

        return carry

    lax.fori_loop(0, groups, one_group, 0)
    for index in range(groups - 2, groups):
        for lane in range(1, lanes):
            block.from_x(lane, index)
    settle(block)

    parts, width = normed_ref.shape[0], normed_ref.shape[2]
    squares = jnp.zeros((tokens, 1), jnp.float32)
    for part in range(parts):
        projected = (
            jnp.dot(
                heads[...], weights[part].reshape(total, width), preferred_element_type=jnp.float32
            )
            .astype(jnp.bfloat16)
            .astype(jnp.float32)
        )
        cols = slice(part * width, (part + 1) * width)
        after = resid_ref[:, cols].astype(jnp.float32) + projected
        after_ref[part] = after
        squares += jnp.sum(after * after, axis=1, keepdims=True)
    factor = lax.rsqrt(squares / (parts * width) + epsilon)
    for part in range(parts):
        cols = slice(part * width, (part + 1) * width)
        normed_ref[part] = (after_ref[part] * factor * gain_ref[:, cols]).astype(normed_ref.dtype)
    row.drain()
    piece.drain()
    block.drain()


def run_front(row, piece, block, queries_t, resid, gain, sp_count, dp_count, heads_here, nope, channels, scale, number):
    outer, inner = split_of(sp_count)
    cores = 2 if dp_count % 2 == 0 else 1
    lanes = dp_count // cores
    tokens, model = resid.shape
    width = model // dp_count
    dma = pltpu.SemaphoreType.DMA
    narrow = [
        dma((max(outer - 1, 1),)),
        dma((max(outer - 1, 1),)),
        dma((max(inner - 1, 1), outer)),
        dma((max(inner - 1, 1), outer)),
    ]
    wide = narrow + [
        dma((max(lanes - 1, 1), sp_count)),
        dma((max(lanes - 1, 1), sp_count)),
        dma((max(cores - 1, 1), lanes, sp_count)),
        dma((max(cores - 1, 1), lanes, sp_count)),
    ]
    vmem = pl.BlockSpec(memory_space=pltpu.VMEM)
    return pl.pallas_call(
        functools.partial(front_kernel, outer, inner, cores, heads_here, nope, channels, scale),
        out_shape=[
            jax.ShapeDtypeStruct((dp_count, tokens, width), jnp.float32),
            jax.ShapeDtypeStruct((dp_count, tokens, width), jnp.bfloat16),
        ],
        in_specs=[vmem] * 6,
        out_specs=[vmem] * 2,
        scratch_shapes=[
            pltpu.VMEM((sp_count,) + row.shape, row.dtype),
            pltpu.VMEM((dp_count, sp_count) + piece.shape, piece.dtype),
            pltpu.VMEM((dp_count, sp_count) + block.shape, block.dtype),
            pltpu.VMEM((tokens, model), jnp.bfloat16),
        ]
        + narrow
        + wide
        + wide,
        compiler_params=pltpu.CompilerParams(
            collective_id=number, has_side_effects=True, vmem_limit_bytes=40 * 2**20
        ),
        cost_estimate=pl.CostEstimate(flops=2 * 10**10, bytes_accessed=10**7, transcendentals=0),
    )(row, piece, block, queries_t, resid, gain)


def split_of(sp_count):
    inner = max(d for d in range(1, math.isqrt(sp_count) + 1) if sp_count % d == 0)
    return sp_count // inner, inner


def experts_kernel(
    outer, inner, capacity,
    normed_ref, meta_ref, after_ref, gate_hbm, up_hbm, down_hbm, out_ref,
    gate_w, up_w, down_w, blocks, metas, picked, rows, made, back, partial, coming, total, gate_acc, up_acc,
    select, columns, spread,
    weight_sems, meta_send, meta_recv, block_send, block_recv, row_send, row_recv,
    back_send, back_recv, sum_send, sum_recv,
):
    me = lax.axis_index("sp")
    z, y = me // inner, lax.rem(me, inner)
    parts, tokens, width = normed_ref.shape
    loads = [
        pltpu.make_async_copy(hbm.at[0], ref, weight_sems.at[at])
        for at, (hbm, ref) in enumerate([(gate_hbm, gate_w), (up_hbm, up_w), (down_hbm, down_w)])
    ]
    for load in loads:
        load.start()

    barrier = pltpu.get_barrier_semaphore()
    steps_z = [lax.rem(z + step, outer) for step in range(1, outer)]
    steps_y = [lax.rem(y + step, inner) for step in range(1, inner)]
    greeted = [{"sp": at * inner + y} for at in steps_z] + [{"sp": z * inner + at} for at in steps_y]
    for peer in greeted:
        pl.semaphore_signal(barrier, inc=1, device_id=peer, device_id_type=pl.DeviceIdType.MESH)
    pl.semaphore_wait(barrier, len(greeted))

    def remote(source, target, send, recv, at_z, at_y):
        return pltpu.make_async_remote_copy(
            src_ref=source, dst_ref=target, send_sem=send, recv_sem=recv,
            device_id={"sp": at_z * inner + at_y}, device_id_type=pl.DeviceIdType.MESH,
        )

    def block_copy(source, part, own, way):
        ref = normed_ref.at[part] if own else blocks.at[source, part]
        return remote(
            ref, blocks.at[source, part],
            block_send.at[(way + 1) // 2, source, part], block_recv.at[source, part], z + way, y,
        )

    def meta_copy(step):
        at = lax.rem(z + step, outer)
        return remote(meta_ref.at[at], metas.at[z], meta_send.at[step - 1], meta_recv.at[z], at, y)

    def row_copy(source, step, part):
        at = lax.rem(y + step, inner)
        return remote(
            picked.at[source, at, part], rows.at[source, y, part],
            row_send.at[source, step - 1, part], row_recv.at[source, y, part], z, at,
        )

    def back_copy(source, step, part):
        at = lax.rem(y + step, inner)
        return remote(
            made.at[source, at, part], back.at[source, y, part],
            back_send.at[source, step - 1, part], back_recv.at[source, y, part], z, at,
        )

    def sum_copy(source, part, way):
        slot = source if way < 0 else jnp.where(source == z + 1, outer, source)
        return remote(
            partial.at[source, part], coming.at[slot, part],
            sum_send.at[source, part], sum_recv.at[slot, part], z + way, y,
        )

    def wait_recv(ref, sem):
        remote(ref, ref, block_send.at[0, 0, 0], sem, z, y).wait_recv()

    for step in range(1, outer):
        meta_copy(step).start()
    for part in range(parts):
        for way in (1, -1):

            @pl.when((z + way >= 0) & (z + way < outer))
            def _():
                block_copy(z, part, True, way).start()

    blocks[z] = normed_ref[...]
    metas[z] = meta_ref[z]

    orders = [sorted(range(outer), key=lambda s: (abs(s - at), s)) for at in range(outer)]

    def source_of(turn):
        found = jnp.int32(0)
        for at in range(outer):
            for index in range(outer):
                found = jnp.where((z == at) & (turn == index), orders[at][index], found)
        return found

    def forwards(source):
        return [
            (1, (source < z) & (z < outer - 1)),
            (-1, (source > z) & (z > 0)),
        ]

    def ends(source):
        return [
            (-1, (source < z) & (z == outer - 1)),
            (1, (source > z) & (z == 0)),
        ]

    def needs(source):
        return functools.reduce(jnp.logical_or, [needed for _, needed in forwards(source)])

    def arrive(source, part):
        wait_recv(blocks.at[source, part], block_recv.at[source, part])

    def forward(source, part):
        for way, needed in forwards(source):

            @pl.when(needed)
            def _():
                block_copy(source, part, False, way).start()

    def open_turn(turn):
        source = source_of(turn)

        @pl.when(turn > 0)
        def _():
            wait_recv(metas.at[source], meta_recv.at[source])

        slot_ids = lax.broadcasted_iota(jnp.int32, (capacity, tokens), 0).astype(jnp.float32)
        for at in range(inner):
            select[at * capacity : (at + 1) * capacity] = jnp.where(
                metas[source, at : at + 1, :] == slot_ids, 1.0, 0.0
            ).astype(jnp.bfloat16)

    def pick(turn, part):
        source = source_of(turn)

        @pl.when((turn == 1) | ((turn > 1) & ~needs(source)))
        def _():
            arrive(source, part)

        @pl.when(turn == 1)
        def _():
            forward(source, part)

        later = source_of(turn + 1)

        @pl.when((turn > 0) & (turn + 1 < outer) & needs(later))
        def _():
            arrive(later, part)
            forward(later, part)

        found = jnp.dot(
            select[...], blocks[source, part], preferred_element_type=jnp.float32
        ).astype(jnp.bfloat16)
        for at in range(inner):
            picked[source, at, part] = found[at * capacity : (at + 1) * capacity]
        rows[source, y, part] = picked[source, y, part]
        for step in range(1, inner):
            row_copy(source, step, part).start()

    def apply_experts(turn):
        source = source_of(turn)

        @pl.when(turn == 0)
        def _():
            for load in loads:
                load.wait()

        gate_acc[...] = jnp.zeros_like(gate_acc)
        up_acc[...] = jnp.zeros_like(up_acc)

        def widen(part, carry):
            for step in range(1, inner):
                at = lax.rem(y + step, inner)
                wait_recv(rows.at[source, at, part], row_recv.at[source, at, part])
            taken = jnp.concatenate([rows[source, at, part] for at in range(inner)], axis=0)
            depth = pl.ds(pl.multiple_of(part * width, width), width)
            gate_acc[...] += jnp.dot(taken, gate_w[depth, :], preferred_element_type=jnp.float32)
            up_acc[...] += jnp.dot(taken, up_w[depth, :], preferred_element_type=jnp.float32)
            return carry

        lax.fori_loop(0, parts, widen, 0)
        gate = gate_acc[...]
        hidden = (gate / (1.0 + jnp.exp(-gate)) * up_acc[...]).astype(jnp.bfloat16)

        for part in range(parts):
            cols = slice(part * width, (part + 1) * width)
            result = jnp.dot(hidden, down_w[:, cols], preferred_element_type=jnp.float32).astype(
                jnp.bfloat16
            )
            for at in range(inner):
                made[source, at, part] = result[at * capacity : (at + 1) * capacity]
            back[source, y, part] = made[source, y, part]
            for step in range(1, inner):
                back_copy(source, step, part).start()

        columns[...] = jnp.transpose(metas[source])
        slot_lanes = lax.broadcasted_iota(jnp.int32, (tokens, capacity), 1).astype(jnp.float32)
        for at in range(inner):
            spread[at] = jnp.where(columns[:, at : at + 1] == slot_lanes, 1.0, 0.0).astype(
                jnp.bfloat16
            )

    def combine(turn, part):
        source = source_of(turn)
        for step in range(1, inner):
            at = lax.rem(y + step, inner)
            wait_recv(back.at[source, at, part], back_recv.at[source, at, part])
        summed = sum(
            jnp.dot(spread[at], back[source, at, part], preferred_element_type=jnp.float32)
            * columns[:, inner + at : inner + at + 1]
            for at in range(inner)
        )

        @pl.when(turn == 0)
        def _():
            total[part] = after_ref[part] + summed

        @pl.when(turn > 0)
        def _():
            partial[source, part] = summed.astype(jnp.bfloat16)

        for way, needed in ends(source):

            @pl.when(needed)
            def _():
                sum_copy(source, part, way).start()

    def turn_body(turn, carry):
        here, before = turn < outer, turn > 0

        @pl.when(here)
        def _():
            open_turn(turn)
            pick(turn, 0)

        @pl.when(before)
        def _():
            apply_experts(turn - 1)

        done = 0
        for part in range(1, parts):

            @pl.when(here)
            def _():
                pick(turn, part)

            upto = parts * part // (parts - 1)

            @pl.when(before)
            def _():
                for at in range(done, upto):
                    combine(turn - 1, at)

            done = upto
        return carry

    lax.fori_loop(0, outer + 1, turn_body, 0)

    def relay(tick, carry):
        for way in (-1, 1):
            since = tick - (z if way > 0 else outer - 1 - z)
            part = lax.rem(since + parts * outer, parts)
            steps = (since + parts * outer) // parts - outer
            source = steps if way > 0 else outer - 1 - steps
            passing = (source > z) if way > 0 else (source < z)
            valid = (source >= 0) & (source < outer) & passing & (z - way >= 0) & (z - way < outer)

            @pl.when(valid)
            def _():
                wait_recv(coming.at[source, part], sum_recv.at[source, part])
                partial[source, part] = (
                    partial[source, part].astype(jnp.float32)
                    + coming[source, part].astype(jnp.float32)
                ).astype(jnp.bfloat16)
                sum_copy(source, part, way).start()

        return carry

    lax.fori_loop(0, outer * (parts + 1), relay, 0)

    for part in range(parts):
        for slot, valid in ((z, z < outer - 1), (outer, z > 0)):

            @pl.when(valid)
            def _():
                wait_recv(coming.at[slot, part], sum_recv.at[slot, part])
                total[part] += coming[slot, part].astype(jnp.float32)

        out_ref[:, part * width : (part + 1) * width] = total[part].astype(out_ref.dtype)

    for step in range(1, outer):
        meta_copy(step).wait_send()
    def drain(source, carry):
        for part in range(parts):
            for way in (1, -1):
                onward = (z + way >= 0) & (z + way < outer)
                passing = (source == z) | ((source < z) if way > 0 else (source > z))

                @pl.when(onward & passing)
                def _():
                    block_copy(source, part, False, way).wait_send()

                @pl.when(onward & ((source > z) if way > 0 else (source < z)))
                def _():
                    sum_copy(source, part, way).wait_send()

            for step in range(1, inner):
                row_copy(source, step, part).wait_send()
                back_copy(source, step, part).wait_send()
        return carry

    lax.fori_loop(0, outer, drain, 0)


def run_experts(normed, meta, after, gate, up, down, sp_count, capacity, number):
    outer, inner = split_of(sp_count)
    parts, tokens, width = normed.shape
    model, hidden = gate.shape[1:]
    dma = pltpu.SemaphoreType.DMA
    bf16, f32 = jnp.bfloat16, jnp.float32
    steps_y = max(inner - 1, 1)
    vmem = pl.BlockSpec(memory_space=pltpu.VMEM)
    anywhere = pl.BlockSpec(memory_space=pl.ANY)
    return pl.pallas_call(
        functools.partial(experts_kernel, outer, inner, capacity),
        out_shape=jax.ShapeDtypeStruct((tokens, parts * width), bf16),
        in_specs=[vmem, vmem, vmem, anywhere, anywhere, anywhere],
        out_specs=vmem,
        scratch_shapes=[
            pltpu.VMEM((model, hidden), bf16),
            pltpu.VMEM((model, hidden), bf16),
            pltpu.VMEM((hidden, model), bf16),
            pltpu.VMEM((outer, parts, tokens, width), bf16),
            pltpu.VMEM((outer,) + meta.shape[1:], f32),
            pltpu.VMEM((outer, inner, parts, capacity, width), bf16),
            pltpu.VMEM((outer, inner, parts, capacity, width), bf16),
            pltpu.VMEM((outer, inner, parts, capacity, width), bf16),
            pltpu.VMEM((outer, inner, parts, capacity, width), bf16),
            pltpu.VMEM((outer, parts, tokens, width), bf16),
            pltpu.VMEM((outer + 1, parts, tokens, width), bf16),
            pltpu.VMEM((parts, tokens, width), f32),
            pltpu.VMEM((inner * capacity, hidden), f32),
            pltpu.VMEM((inner * capacity, hidden), f32),
            pltpu.VMEM((inner * capacity, tokens), bf16),
            pltpu.VMEM((tokens, meta.shape[1]), f32),
            pltpu.VMEM((inner, tokens, capacity), bf16),
            dma((3,)),
            dma((outer,)),
            dma((outer,)),
            dma((2, outer, parts)),
            dma((outer, parts)),
            dma((outer, steps_y, parts)),
            dma((outer, inner, parts)),
            dma((outer, steps_y, parts)),
            dma((outer, inner, parts)),
            dma((outer, parts)),
            dma((outer + 1, parts)),
        ],
        compiler_params=pltpu.CompilerParams(
            collective_id=number, has_side_effects=True, vmem_limit_bytes=60 * 2**20
        ),
        cost_estimate=pl.CostEstimate(
            flops=6 * sp_count * capacity * model * hidden, bytes_accessed=10**7, transcendentals=0
        ),
    )(normed, meta, after, gate, up, down)


def shards(
    query_nope,
    query_rope,
    latent,
    key_rope,
    resid,
    latent_gain,
    key_up,
    value_up,
    out_proj,
    norm_gain,
    expert_gate,
    expert_up,
    expert_down,
    routes,
    route_weight,
):
    tokens, channels = latent.shape[1:]
    sp_count = lax.axis_size("sp")
    dp_count = lax.axis_size("dp")
    me = lax.axis_index("sp")
    nope, rope = query_nope.shape[-1], query_rope.shape[-1]
    heads_here = key_up.shape[1] // nope
    scale = (nope + rope) ** (-0.5)
    local_pos = me * tokens + jnp.arange(tokens, dtype=jnp.int32)
    latent_normed = rms_scaled(latent[0], latent_gain).astype(jnp.bfloat16)
    key_turned = rotate(key_rope[0], local_pos)
    spare = 128 - rope
    row = jnp.concatenate(
        [latent_normed, key_turned, jnp.zeros((tokens, spare), jnp.bfloat16)], axis=1
    )
    piece = channels // dp_count
    ups = lax.dynamic_slice_in_dim(
        jnp.concatenate([key_up, value_up], axis=1), lax.axis_index("dp") * piece, piece, axis=0
    )
    query_turned = rotate(query_rope[0], local_pos)
    queries = jnp.concatenate(
        [query_nope[0], query_turned, jnp.zeros(query_turned.shape[:2] + (128 - rope,), jnp.bfloat16)],
        axis=-1,
    )
    queries_t = jnp.transpose(queries, (1, 2, 0))
    after, normed = run_front(
        row, ups, out_proj, queries_t, resid[0], norm_gain[None],
        sp_count, dp_count, heads_here, nope, channels, scale, 0,
    )

    experts_all = sp_count * expert_gate.shape[0]
    capacity = 4 * tokens // experts_all
    ids = jnp.arange(experts_all, dtype=jnp.int32)[:, None, None]
    mine = routes[0][None] == ids
    named = jnp.any(mine, axis=-1)
    weight = jnp.sum(jnp.where(mine, route_weight[0][None], 0.0), axis=-1)
    place = jnp.cumsum(named.astype(jnp.int32), axis=1) - 1
    outer, inner = split_of(sp_count)
    slot = jnp.where(named, place, -1).astype(jnp.float32).reshape(outer, inner, tokens)
    meta = jnp.concatenate([slot, weight.reshape(outer, inner, tokens)], axis=1)
    meta = jnp.pad(meta, ((0, 0), (0, -2 * inner % 8), (0, 0)))
    mixed = run_experts(
        normed, meta, after, expert_gate, expert_up, expert_down, sp_count, capacity, 1
    )
    return mixed[None]


def solution(mesh):
    return jax.shard_map(
        shards,
        mesh=mesh,
        in_specs=(
            P("dp", "sp", None, None),
            P("dp", "sp", None, None),
            P("dp", "sp", None),
            P("dp", "sp", None),
            P("dp", "sp", None),
            P(),
            P(None, "sp"),
            P(None, "sp"),
            P("sp", "dp"),
            P(),
            P("sp", None, None),
            P("sp", None, None),
            P("sp", None, None),
            P("dp", "sp", None),
            P("dp", "sp", None),
        ),
        out_specs=P("dp", "sp", None),
        check_vma=False,
    )
```

```python
import functools
import math

import jax
import jax.numpy as jnp
from jax import lax
from jax.experimental import pallas as pl
from jax.experimental.pallas import tpu as pltpu
from jax.sharding import PartitionSpec as P

epsilon = 1e-06
rope_base = 10000.0
masked_score = -1e30
log2_e = 1.4426950408889634
part_width = 256
link_rate = 46.6e3
link_delay = 2.2


def rotate(values, positions):
    half_width = values.shape[-1] // 2
    frequency = rope_base ** (-jnp.arange(half_width, dtype=jnp.float32) / half_width)
    angles = positions.astype(jnp.float32)[:, None] * frequency[None, :]
    cosine = jnp.cos(angles)
    sine_part = jnp.sin(angles)
    if values.ndim == 3:
        cosine = cosine[:, None, :]
        sine_part = sine_part[:, None, :]
    floats = values.astype(jnp.float32)
    first_half = floats[..., :half_width]
    second_half = floats[..., half_width:]
    turned = jnp.concatenate(
        [
            first_half * cosine - second_half * sine_part,
            second_half * cosine + first_half * sine_part,
        ],
        axis=-1,
    )
    return turned.astype(jnp.bfloat16)


def rms_scaled(values, gain):
    floats = values.astype(jnp.float32)
    return floats * lax.rsqrt(jnp.mean(floats * floats, axis=-1, keepdims=True) + epsilon) * gain


def front_kernel(
    outer, inner, cores, heads_here, nope, channels, scale,
    row_ref, piece_ref, block_ref, query_ref, resid_ref, gain_ref, after_ref, normed_ref,
    shared, ups, weights, heads, *sems,
):
    me, dp = lax.axis_index("sp"), lax.axis_index("dp")
    z, y = me // inner, lax.rem(me, inner)
    lanes = weights.shape[0] // cores
    x, core = dp // cores, lax.rem(dp, cores)
    groups, tokens = shared.shape[0], shared.shape[1]
    columns = heads_here * nope
    total = groups * columns
    row_sems, piece_sems, block_sems = sems[0:4], sems[4:12], sems[12:20]

    def remote(source, target, send, recv, peer):
        return pltpu.make_async_remote_copy(
            src_ref=source, dst_ref=target, send_sem=send, recv_sem=recv,
            device_id=peer, device_id_type=pl.DeviceIdType.MESH,
        )

    def at_z(step):
        return {"sp": lax.rem(z + step, outer) * inner + y}

    def at_y(step):
        return {"sp": z * inner + lax.rem(y + step, inner)}

    def at_x(step):
        return {"dp": lax.rem(x + step, lanes) * cores + core}

    def at_core(step):
        return {"dp": x * cores + lax.rem(core + step, cores)}

    barrier = pltpu.get_barrier_semaphore()
    greeted = (
        [at_z(step) for step in range(1, outer)]
        + [at_y(step) for step in range(1, inner)]
        + [at_x(step) for step in range(1, lanes)]
        + [at_core(step) for step in range(1, cores)]
    )
    for peer in greeted:
        pl.semaphore_signal(barrier, inc=1, device_id=peer, device_id_type=pl.DeviceIdType.MESH)
    pl.semaphore_wait(barrier, len(greeted))

    def member(index):
        along_z, along_y = lax.rem(index, outer), index // outer
        return lax.rem(z + along_z, outer) * inner + lax.rem(y + along_y, inner)

    class Spread:
        def __init__(self, own, held, sems, wide):
            self.own, self.held, self.sems, self.wide = own, held, sems, wide

        def place(self, block, row=None):
            return self.held.at[block] if not self.wide else self.held.at[dp if row is None else row, block]

        def along_z(self, step):
            return remote(self.own, self.place(me), self.sems[0].at[step - 1], self.sems[1].at[step - 1], at_z(step))

        def along_y(self, step, index):
            source = self.own if isinstance(index, int) and index == 0 else self.place(member(index))
            return remote(
                source, self.place(member(index)),
                self.sems[2].at[step - 1, index], self.sems[3].at[step - 1, index], at_y(step),
            )

        def along_x(self, step, index):
            source = self.own if isinstance(index, int) and index == 0 else self.place(member(index))
            return remote(
                source, self.place(member(index)),
                self.sems[4].at[step - 1, index], self.sems[5].at[step - 1, index], at_x(step),
            )

        def across(self, step, lane, index):
            row = lax.rem(x + lane, lanes) * cores + core
            own = isinstance(index, int) and index == 0 and lane == 0
            source = self.own if own else self.place(member(index), row)
            return remote(
                source, self.place(member(index), row),
                self.sems[6].at[step - 1, lane, index], self.sems[7].at[step - 1, lane, index], at_core(step),
            )

        def wait(self, ref, sem):
            remote(ref, ref, self.sems[0].at[0], sem, at_z(0)).wait_recv()

        def start_z(self):
            for step in range(1, outer):
                self.along_z(step).start()

        def start_y(self, index):
            for step in range(1, inner):
                self.along_y(step, index).start()

        def start_wide(self, index):
            for step in range(1, lanes):
                self.along_x(step, index).start()
            for step in range(1, cores):
                self.across(step, 0, index).start()

        def from_z(self, index):
            step = (outer - index) % outer
            self.wait(self.place(member(index)), self.sems[1].at[step - 1])

        def from_y(self, index):
            step = inner - index // outer
            self.wait(self.place(member(index)), self.sems[3].at[step - 1, lax.rem(index, outer)])

        def from_x(self, lane, index):
            row = lax.rem(x + lane, lanes) * cores + core
            self.wait(self.place(member(index), row), self.sems[5].at[lanes - lane - 1, index])
            for step in range(1, cores):
                self.across(step, lane, index).start()

        def from_core(self, step, lane, index):
            row = lax.rem(x + lane, lanes) * cores + lax.rem(core + step, cores)
            self.wait(self.place(member(index), row), self.sems[7].at[cores - step - 1, lane, index])

        def drain(self):
            for step in range(1, outer):
                self.along_z(step).wait_send()
            for index in range(outer):
                for step in range(1, inner):
                    self.along_y(step, index).wait_send()
            if self.wide:

                def one(index, carry):
                    for step in range(1, lanes):
                        self.along_x(step, index).wait_send()
                    for step in range(1, cores):
                        for lane in range(lanes):
                            self.across(step, lane, index).wait_send()
                    return carry

                lax.fori_loop(0, groups, one, 0)

    row = Spread(row_ref, shared, row_sems, False)
    piece = Spread(piece_ref, ups, piece_sems, True)
    block = Spread(block_ref, weights, block_sems, True)
    row.start_z()
    piece.start_z()
    row.start_y(0)
    piece.start_y(0)
    piece.start_wide(0)
    shared[me] = row_ref[...]
    ups[dp, me] = piece_ref[...]
    weights[dp, me] = block_ref[...]
    for index in range(1, outer):
        row.from_z(index)
        row.start_y(index)
        piece.from_z(index)
        piece.start_y(index)
        piece.start_wide(index)
    block.start_z()
    block.start_y(0)
    block.start_wide(0)
    for index in range(outer, groups):
        row.from_y(index)
        piece.from_y(index)
        piece.start_wide(index)
    for lane in range(1, lanes):
        for index in range(groups):
            piece.from_x(lane, index)

    def settle(spread):
        def one(index, carry):
            for lane in range(lanes):
                for step in range(1, cores):
                    spread.from_core(step, lane, index)
            return carry

        lax.fori_loop(0, groups, one, 0)

    settle(piece)

    key_ids = lax.broadcasted_iota(jnp.int32, (tokens, tokens), 0)
    query_ids = lax.broadcasted_iota(jnp.int32, (tokens, tokens), 1)
    allowed = key_ids <= query_ids

    def attend_group(group):
        up = ups[:, group].reshape(channels, 2 * columns)
        up_keys = up[:, 0:columns]
        up_values = up[:, columns : 2 * columns]
        up_values_t = jnp.transpose(up_values.astype(jnp.float32)).astype(jnp.bfloat16)

        def scores_of(chunk):
            latent = shared[chunk, :, 0:channels]
            turned = shared[chunk, :, channels:]
            keys = jnp.dot(latent, up_keys, preferred_element_type=jnp.float32).astype(jnp.bfloat16)
            values_t = lax.dot_general(
                up_values_t, latent, (((1,), (1,)), ((), ())), preferred_element_type=jnp.float32
            ).astype(jnp.bfloat16)
            scores = []
            for head in range(heads_here):
                full = jnp.concatenate([keys[:, head * nope : (head + 1) * nope], turned], axis=1)
                scores.append(
                    jnp.dot(
                        full, query_ref[group * heads_here + head], preferred_element_type=jnp.float32
                    )
                    * (scale * log2_e)
                )
            return scores, [values_t[h * nope : (h + 1) * nope, :] for h in range(heads_here)]

        scores, values = scores_of(me)
        state = []
        for score, value in zip(scores, values):
            score = jnp.where(allowed, score, masked_score)
            largest = jnp.max(score, axis=0, keepdims=True)
            powers = jnp.exp2(score - largest)
            state.append(
                (
                    largest,
                    jnp.sum(powers, axis=0, keepdims=True),
                    jnp.dot(value, powers.astype(jnp.bfloat16), preferred_element_type=jnp.float32),
                )
            )

        def step(chunk, state):
            scores, values = scores_of(chunk)
            after = []
            for (largest, total, kept), score, value in zip(state, scores, values):
                now = jnp.maximum(largest, jnp.max(score, axis=0, keepdims=True))
                fade = jnp.exp2(largest - now)
                powers = jnp.exp2(score - now)
                after.append(
                    (
                        now,
                        total * fade + jnp.sum(powers, axis=0, keepdims=True),
                        kept * fade
                        + jnp.dot(
                            value, powers.astype(jnp.bfloat16), preferred_element_type=jnp.float32
                        ),
                    )
                )
            return tuple(after)

        state = lax.fori_loop(0, me, step, tuple(state))
        for head, (_, total, kept) in enumerate(state):
            start = pl.multiple_of(group * columns + head * nope, nope)
            heads[:, pl.ds(start, nope)] = jnp.transpose(kept / total).astype(heads.dtype)

    def one_group(group, carry):
        attend_group(group)

        @pl.when(group == 0)
        def _():
            for index in range(1, outer):
                block.from_z(index)
                block.start_y(index)
                block.start_wide(index)

        nearby = group + outer - 1

        @pl.when((group > 0) & (nearby < groups))
        def _():
            block.from_y(nearby)
            block.start_wide(nearby)

        @pl.when(group >= 2)
        def _():
            for lane in range(1, lanes):
                block.from_x(lane, group - 2)

        return carry

    lax.fori_loop(0, groups, one_group, 0)
    for index in range(groups - 2, groups):
        for lane in range(1, lanes):
            block.from_x(lane, index)
    settle(block)

    parts, width = weights.shape[0], weights.shape[3]
    pieces, narrow = normed_ref.shape[0], normed_ref.shape[2]
    squares = jnp.zeros((tokens, 1), jnp.float32)
    for part in range(parts):
        projected = (
            jnp.dot(
                heads[...], weights[part].reshape(total, width), preferred_element_type=jnp.float32
            )
            .astype(jnp.bfloat16)
            .astype(jnp.float32)
        )
        cols = slice(part * width, (part + 1) * width)
        after = resid_ref[:, cols].astype(jnp.float32) + projected
        each = width // narrow
        for at in range(each):
            after_ref[part * each + at] = after[:, at * narrow : (at + 1) * narrow]
        squares += jnp.sum(after * after, axis=1, keepdims=True)
    factor = lax.rsqrt(squares / (parts * width) + epsilon)
    for part in range(pieces):
        cols = slice(part * narrow, (part + 1) * narrow)
        normed_ref[part] = (after_ref[part] * factor * gain_ref[:, cols]).astype(normed_ref.dtype)
    row.drain()
    piece.drain()
    block.drain()


def run_front(row, piece, block, queries_t, resid, gain, sp_count, dp_count, heads_here, nope, channels, scale, number):
    outer, inner = split_of(sp_count)
    cores = 2 if dp_count % 2 == 0 else 1
    lanes = dp_count // cores
    tokens, model = resid.shape
    width = min(model // dp_count, part_width)
    dma = pltpu.SemaphoreType.DMA
    narrow = [
        dma((max(outer - 1, 1),)),
        dma((max(outer - 1, 1),)),
        dma((max(inner - 1, 1), outer)),
        dma((max(inner - 1, 1), outer)),
    ]
    wide = narrow + [
        dma((max(lanes - 1, 1), sp_count)),
        dma((max(lanes - 1, 1), sp_count)),
        dma((max(cores - 1, 1), lanes, sp_count)),
        dma((max(cores - 1, 1), lanes, sp_count)),
    ]
    vmem = pl.BlockSpec(memory_space=pltpu.VMEM)
    return pl.pallas_call(
        functools.partial(front_kernel, outer, inner, cores, heads_here, nope, channels, scale),
        out_shape=[
            jax.ShapeDtypeStruct((model // width, tokens, width), jnp.float32),
            jax.ShapeDtypeStruct((model // width, tokens, width), jnp.bfloat16),
        ],
        in_specs=[vmem] * 6,
        out_specs=[vmem] * 2,
        scratch_shapes=[
            pltpu.VMEM((sp_count,) + row.shape, row.dtype),
            pltpu.VMEM((dp_count, sp_count) + piece.shape, piece.dtype),
            pltpu.VMEM((dp_count, sp_count) + block.shape, block.dtype),
            pltpu.VMEM((tokens, model), jnp.bfloat16),
        ]
        + narrow
        + wide
        + wide,
        compiler_params=pltpu.CompilerParams(
            collective_id=number, has_side_effects=True, vmem_limit_bytes=40 * 2**20
        ),
        cost_estimate=pl.CostEstimate(flops=2 * 10**10, bytes_accessed=10**7, transcendentals=0),
    )(row, piece, block, queries_t, resid, gain)


def split_of(sp_count):
    inner = max(d for d in range(1, math.isqrt(sp_count) + 1) if sp_count % d == 0)
    return sp_count // inner, inner


def plan_tasks(outer, parts, across_z, across_y):
    def forward(at, source):
        return 1 if source < at < outer - 1 else (-1 if 0 < at < source else 0)

    spent = {"A": 0.5, "B": 4.5, "C": 0.6, "F": 0.05, "R": 0.3}
    todo = [
        [("B", s, 0) for s in range(outer)]
        + [(kind, s, p) for s in range(outer) for p in range(parts) for kind in "AC"]
        + [("F", s, p) for s in range(outer) for p in range(parts) if forward(at, s)]
        + [("R", s, p) for s in range(outer) for p in range(parts) if s != at and 0 < at < outer - 1]
        for at in range(outer)
    ]
    free, landed = {}, {}
    clock, done, order = [2.0] * outer, [set() for _ in range(outer)], [[] for _ in range(outer)]

    def send(at, link, target, key, time, length):
        free[at, link] = max(time, free.get((at, link), 0.0)) + length
        landed[target, key] = free[at, link] + link_delay

    def ready(at, task):
        kind, source, part = task
        needed, before = [], []
        wait = 0.0
        if kind in "AF" and source != at:
            needed.append(("block", source, part))
        if kind == "A":
            before += [("F", source, part)] if forward(at, source) else []
            before += [("A", source, part - 1)] if part else []
            wait = free.get((at, "y"), 0.0) - 3.0
        if kind == "F" and part:
            before.append(("F", source, part - 1))
        if kind == "B":
            before += [("A", source, p) for p in range(parts)]
            before += [("B", s, 0) for s in range(outer) if s != at and source == at]
            needed += [("row", source, p) for p in range(parts)]
            wait = free.get((at, "y"), 0.0) - 6.0
        if kind == "C":
            before.append(("B", source, 0))
            needed.append(("back", source, part))
        if kind == "R":
            before.append(("C", source, part))
            needed.append(("sum", source, part))
        if any(task not in done[at] for task in before) or any((at, key) not in landed for key in needed):
            return None
        return max([clock[at], wait] + [landed[at, key] for key in needed])

    def rank(at, task):
        kind, source, part = task
        own = source == at
        return (8 if own and kind == "C" else "FRBCA".index(kind), abs(source - at), part)

    for at in range(outer):
        for part in range(parts):
            for way in (1, -1):
                if 0 <= at + way < outer:
                    send(at, way, at + way, ("block", at, part), 2.0, across_z)
    while any(todo):
        chosen = None
        for at in range(outer):
            times = [(ready(at, task), task) for task in todo[at]]
            times = [(time, task) for time, task in times if time is not None]
            if times:
                first = min(time for time, _ in times)
                task = min((t for time, t in times if time <= first), key=lambda t: rank(at, t))
                if chosen is None or first < chosen[0]:
                    chosen = (first, at, task)
        time, at, task = chosen
        kind, source, part = task
        todo[at].remove(task)
        order[at].append(task)
        done[at].add(task)
        clock[at] = end = time + spent[kind]
        way = -1 if source < at else 1
        if kind == "F":
            send(at, forward(at, source), at + forward(at, source), ("block", source, part), end, across_z)
        if kind == "A":
            send(at, "y", at, ("row", source, part), end, across_y)
        if kind == "B":
            for p in range(parts):
                begun = end - spent["B"] * 0.5 * (parts - 1 - p) / parts
                send(at, "y", at, ("back", source, p), begun, across_y)
        last = at == (outer - 1 if way < 0 else 0)
        if source != at and (kind == "R" or (kind == "C" and last)):
            key = ("last", at + way, part) if way > 0 and source == at + way else ("sum", source, part)
            send(at, way, at + way, key, end, across_z)
    return order


def experts_kernel(
    outer, inner, capacity, order,
    normed_ref, meta_ref, after_ref, gate_hbm, up_hbm, down_hbm, out_ref,
    gate_w, up_w, down_w, blocks, metas, picked, rows, made, back, partial, coming, total, gate_acc, up_acc,
    select, columns, spread,
    weight_sems, meta_send, meta_recv, block_send, block_recv, row_send, row_recv,
    back_send, back_recv, sum_send, sum_recv,
):
    me = lax.axis_index("sp")
    z, y = me // inner, lax.rem(me, inner)
    parts, tokens, width = normed_ref.shape
    loads = [
        pltpu.make_async_copy(hbm.at[0], ref, weight_sems.at[at])
        for at, (hbm, ref) in enumerate([(gate_hbm, gate_w), (up_hbm, up_w), (down_hbm, down_w)])
    ]
    for load in loads:
        load.start()

    barrier = pltpu.get_barrier_semaphore()
    steps_z = [lax.rem(z + step, outer) for step in range(1, outer)]
    steps_y = [lax.rem(y + step, inner) for step in range(1, inner)]
    greeted = [{"sp": at * inner + y} for at in steps_z] + [{"sp": z * inner + at} for at in steps_y]
    for peer in greeted:
        pl.semaphore_signal(barrier, inc=1, device_id=peer, device_id_type=pl.DeviceIdType.MESH)
    pl.semaphore_wait(barrier, len(greeted))

    def remote(source, target, send, recv, at_z, at_y):
        return pltpu.make_async_remote_copy(
            src_ref=source, dst_ref=target, send_sem=send, recv_sem=recv,
            device_id={"sp": at_z * inner + at_y}, device_id_type=pl.DeviceIdType.MESH,
        )

    def block_copy(source, part, own, way):
        ref = normed_ref.at[part] if own else blocks.at[source, part]
        return remote(
            ref, blocks.at[source, part],
            block_send.at[(way + 1) // 2, source, part], block_recv.at[source, part], z + way, y,
        )

    def meta_copy(step):
        at = lax.rem(z + step, outer)
        return remote(meta_ref.at[at], metas.at[z], meta_send.at[step - 1], meta_recv.at[z], at, y)

    def row_copy(source, step, part):
        at = lax.rem(y + step, inner)
        return remote(
            picked.at[source, at, part], rows.at[source, y, part],
            row_send.at[source, step - 1, part], row_recv.at[source, y, part], z, at,
        )

    def back_copy(source, step, part):
        at = lax.rem(y + step, inner)
        return remote(
            made.at[source, at, part], back.at[source, y, part],
            back_send.at[source, step - 1, part], back_recv.at[source, y, part], z, at,
        )

    def sum_copy(source, part, way):
        slot = source if way < 0 else jnp.where(source == z + 1, outer, source)
        return remote(
            partial.at[source, part], coming.at[slot, part],
            sum_send.at[source, part], sum_recv.at[slot, part], z + way, y,
        )

    def wait_recv(ref, sem):
        remote(ref, ref, block_send.at[0, 0, 0], sem, z, y).wait_recv()

    for step in range(1, outer):
        meta_copy(step).start()
    for part in range(parts):
        for way in (1, -1):

            @pl.when((z + way >= 0) & (z + way < outer))
            def _():
                block_copy(z, part, True, way).start()

    blocks[z] = normed_ref[...]
    metas[z] = meta_ref[z]

    kinds = "ABCFRW"
    steps = max(len(row) for row in order) + 1

    def coded(row):
        first = [kind for kind, _, _ in row].index("B")
        row = row[:first] + [("W", 0, 0)] + row[first:]
        codes = [(kinds.index(kind) * outer + source) * parts + part for kind, source, part in row]
        return codes + [len(kinds) * outer * parts] * (steps - len(codes))

    base = (len(kinds) + 1) * outer * parts
    rows_coded = [coded(row) for row in order]
    words = []
    for start in range(0, steps, 3):
        value = None
        for at in range(outer):
            word = sum(code * base**index for index, code in enumerate(rows_coded[at][start : start + 3]))
            value = jnp.int32(word) if value is None else jnp.where(z == at, word, value)
        words.append(value)

    def task_of(step):
        index, digit = step // 3, lax.rem(step, 3)
        level = words
        while len(level) > 1:
            even = lax.rem(index, 2) == 0
            level = [
                jnp.where(even, level[at], level[at + 1]) if at + 1 < len(level) else level[at]
                for at in range(0, len(level), 2)
            ]
            index = index // 2
        word = level[0]
        code = jnp.where(digit == 0, word, jnp.where(digit == 1, word // base, word // base**2))
        code = lax.rem(code, base)
        return code // (outer * parts), lax.rem(code // parts, outer), lax.rem(code, parts)

    def forwards(source):
        return [
            (1, (source < z) & (z < outer - 1)),
            (-1, (source > z) & (z > 0)),
        ]

    def ends(source):
        return [
            (-1, (source < z) & (z == outer - 1)),
            (1, (source > z) & (z == 0)),
        ]

    def needs(source):
        return functools.reduce(jnp.logical_or, [needed for _, needed in forwards(source)])

    def arrive(source, part):
        wait_recv(blocks.at[source, part], block_recv.at[source, part])

    def pick(source, part):
        @pl.when((source != z) & (part == 0))
        def _():
            wait_recv(metas.at[source], meta_recv.at[source])

        @pl.when(part == 0)
        def _():
            slot_ids = lax.broadcasted_iota(jnp.int32, (capacity, tokens), 0).astype(jnp.float32)
            for at in range(inner):
                select[source, at * capacity : (at + 1) * capacity] = jnp.where(
                    metas[source, at : at + 1, :] == slot_ids, 1.0, 0.0
                ).astype(jnp.bfloat16)

        @pl.when((source != z) & ~needs(source))
        def _():
            arrive(source, part)

        found = jnp.dot(
            select[source], blocks[source, part], preferred_element_type=jnp.float32
        ).astype(jnp.bfloat16)
        for at in range(inner):
            picked[source, at, part] = found[at * capacity : (at + 1) * capacity]
        rows[source, y, part] = picked[source, y, part]
        for step in range(1, inner):
            row_copy(source, step, part).start()

    def apply_experts(source):
        gate_acc[...] = jnp.zeros_like(gate_acc)
        up_acc[...] = jnp.zeros_like(up_acc)

        def widen(pair, carry):
            for part in (2 * pair, 2 * pair + 1):
                for step in range(1, inner):
                    at = lax.rem(y + step, inner)
                    wait_recv(rows.at[source, at, part], row_recv.at[source, at, part])
            taken = jnp.concatenate(
                [
                    jnp.concatenate([rows[source, at, 2 * pair + half] for half in range(2)], axis=1)
                    for at in range(inner)
                ],
                axis=0,
            )
            depth = pl.ds(pl.multiple_of(pair * 2 * width, 2 * width), 2 * width)
            gate_acc[...] += jnp.dot(taken, gate_w[depth, :], preferred_element_type=jnp.float32)
            up_acc[...] += jnp.dot(taken, up_w[depth, :], preferred_element_type=jnp.float32)
            return carry

        lax.fori_loop(0, parts // 2, widen, 0)
        gate = gate_acc[...]
        hidden = (gate / (1.0 + jnp.exp(-gate)) * up_acc[...]).astype(jnp.bfloat16)

        for part in range(parts):
            cols = slice(part * width, (part + 1) * width)
            result = jnp.dot(hidden, down_w[:, cols], preferred_element_type=jnp.float32).astype(
                jnp.bfloat16
            )
            for at in range(inner):
                made[source, at, part] = result[at * capacity : (at + 1) * capacity]
            back[source, y, part] = made[source, y, part]
            for step in range(1, inner):
                back_copy(source, step, part).start()

        columns[source] = jnp.transpose(metas[source])
        slot_lanes = lax.broadcasted_iota(jnp.int32, (tokens, capacity), 1).astype(jnp.float32)
        for at in range(inner):
            spread[source, at] = jnp.where(
                columns[source, :, at : at + 1] == slot_lanes, 1.0, 0.0
            ).astype(jnp.bfloat16)

    def combine(source, part):
        for step in range(1, inner):
            at = lax.rem(y + step, inner)
            wait_recv(back.at[source, at, part], back_recv.at[source, at, part])
        summed = sum(
            jnp.dot(spread[source, at], back[source, at, part], preferred_element_type=jnp.float32)
            * columns[source, :, inner + at : inner + at + 1]
            for at in range(inner)
        )

        @pl.when(source == z)
        def _():
            total[part] = after_ref[part] + summed

        @pl.when(source != z)
        def _():
            partial[source, part] = summed.astype(jnp.bfloat16)

        for way, needed in ends(source):

            @pl.when(needed)
            def _():
                sum_copy(source, part, way).start()

    def relay(source, part):
        wait_recv(coming.at[source, part], sum_recv.at[source, part])
        partial[source, part] = (
            partial[source, part].astype(jnp.float32) + coming[source, part].astype(jnp.float32)
        ).astype(jnp.bfloat16)
        for way in (1, -1):

            @pl.when((source > z) if way > 0 else (source < z))
            def _():
                sum_copy(source, part, way).start()

    def run_task(step, carry):
        kind, source, part = task_of(step)

        @pl.when(kind == 0)
        def _():
            pick(source, part)

        @pl.when(kind == 1)
        def _():
            apply_experts(source)

        @pl.when(kind == 2)
        def _():
            combine(source, part)

        @pl.when(kind == 3)
        def _():
            arrive(source, part)
            for way, needed in forwards(source):

                @pl.when(needed)
                def _():
                    block_copy(source, part, False, way).start()

        @pl.when(kind == 4)
        def _():
            relay(source, part)

        @pl.when(kind == 5)
        def _():
            for load in loads:
                load.wait()

        return carry

    lax.fori_loop(0, steps, run_task, 0)

    for part in range(parts):
        for slot, valid in ((z, z < outer - 1), (outer, z > 0)):

            @pl.when(valid)
            def _():
                wait_recv(coming.at[slot, part], sum_recv.at[slot, part])
                total[part] += coming[slot, part].astype(jnp.float32)

        out_ref[:, part * width : (part + 1) * width] = total[part].astype(out_ref.dtype)

    for step in range(1, outer):
        meta_copy(step).wait_send()
    def drain(source, carry):
        for part in range(parts):
            for way in (1, -1):
                onward = (z + way >= 0) & (z + way < outer)
                passing = (source == z) | ((source < z) if way > 0 else (source > z))

                @pl.when(onward & passing)
                def _():
                    block_copy(source, part, False, way).wait_send()

                @pl.when(onward & ((source > z) if way > 0 else (source < z)))
                def _():
                    sum_copy(source, part, way).wait_send()

            for step in range(1, inner):
                row_copy(source, step, part).wait_send()
                back_copy(source, step, part).wait_send()
        return carry

    lax.fori_loop(0, outer, drain, 0)


def run_experts(normed, meta, after, gate, up, down, sp_count, capacity, number):
    outer, inner = split_of(sp_count)
    parts, tokens, width = normed.shape
    model, hidden = gate.shape[1:]
    across_z = tokens * width * 2 / link_rate
    order = plan_tasks(outer, parts, across_z, across_z * capacity / tokens)
    dma = pltpu.SemaphoreType.DMA
    bf16, f32 = jnp.bfloat16, jnp.float32
    steps_y = max(inner - 1, 1)
    vmem = pl.BlockSpec(memory_space=pltpu.VMEM)
    anywhere = pl.BlockSpec(memory_space=pl.ANY)
    return pl.pallas_call(
        functools.partial(experts_kernel, outer, inner, capacity, order),
        out_shape=jax.ShapeDtypeStruct((tokens, parts * width), bf16),
        in_specs=[vmem, vmem, vmem, anywhere, anywhere, anywhere],
        out_specs=vmem,
        scratch_shapes=[
            pltpu.VMEM((model, hidden), bf16),
            pltpu.VMEM((model, hidden), bf16),
            pltpu.VMEM((hidden, model), bf16),
            pltpu.VMEM((outer, parts, tokens, width), bf16),
            pltpu.VMEM((outer,) + meta.shape[1:], f32),
            pltpu.VMEM((outer, inner, parts, capacity, width), bf16),
            pltpu.VMEM((outer, inner, parts, capacity, width), bf16),
            pltpu.VMEM((outer, inner, parts, capacity, width), bf16),
            pltpu.VMEM((outer, inner, parts, capacity, width), bf16),
            pltpu.VMEM((outer, parts, tokens, width), bf16),
            pltpu.VMEM((outer + 1, parts, tokens, width), bf16),
            pltpu.VMEM((parts, tokens, width), f32),
            pltpu.VMEM((inner * capacity, hidden), f32),
            pltpu.VMEM((inner * capacity, hidden), f32),
            pltpu.VMEM((outer, inner * capacity, tokens), bf16),
            pltpu.VMEM((outer, tokens, meta.shape[1]), f32),
            pltpu.VMEM((outer, inner, tokens, capacity), bf16),
            dma((3,)),
            dma((outer,)),
            dma((outer,)),
            dma((2, outer, parts)),
            dma((outer, parts)),
            dma((outer, steps_y, parts)),
            dma((outer, inner, parts)),
            dma((outer, steps_y, parts)),
            dma((outer, inner, parts)),
            dma((outer, parts)),
            dma((outer + 1, parts)),
        ],
        compiler_params=pltpu.CompilerParams(
            collective_id=number, has_side_effects=True, vmem_limit_bytes=60 * 2**20
        ),
        cost_estimate=pl.CostEstimate(
            flops=6 * sp_count * capacity * model * hidden, bytes_accessed=10**7, transcendentals=0
        ),
    )(normed, meta, after, gate, up, down)


def shards(
    query_nope,
    query_rope,
    latent,
    key_rope,
    resid,
    latent_gain,
    key_up,
    value_up,
    out_proj,
    norm_gain,
    expert_gate,
    expert_up,
    expert_down,
    routes,
    route_weight,
):
    tokens, channels = latent.shape[1:]
    sp_count = lax.axis_size("sp")
    dp_count = lax.axis_size("dp")
    me = lax.axis_index("sp")
    nope, rope = query_nope.shape[-1], query_rope.shape[-1]
    heads_here = key_up.shape[1] // nope
    scale = (nope + rope) ** (-0.5)
    local_pos = me * tokens + jnp.arange(tokens, dtype=jnp.int32)
    latent_normed = rms_scaled(latent[0], latent_gain).astype(jnp.bfloat16)
    key_turned = rotate(key_rope[0], local_pos)
    spare = 128 - rope
    row = jnp.concatenate(
        [latent_normed, key_turned, jnp.zeros((tokens, spare), jnp.bfloat16)], axis=1
    )
    piece = channels // dp_count
    ups = lax.dynamic_slice_in_dim(
        jnp.concatenate([key_up, value_up], axis=1), lax.axis_index("dp") * piece, piece, axis=0
    )
    query_turned = rotate(query_rope[0], local_pos)
    queries = jnp.concatenate(
        [query_nope[0], query_turned, jnp.zeros(query_turned.shape[:2] + (128 - rope,), jnp.bfloat16)],
        axis=-1,
    )
    queries_t = jnp.transpose(queries, (1, 2, 0))
    after, normed = run_front(
        row, ups, out_proj, queries_t, resid[0], norm_gain[None],
        sp_count, dp_count, heads_here, nope, channels, scale, 0,
    )

    experts_all = sp_count * expert_gate.shape[0]
    capacity = 4 * tokens // experts_all
    ids = jnp.arange(experts_all, dtype=jnp.int32)[:, None, None]
    mine = routes[0][None] == ids
    named = jnp.any(mine, axis=-1)
    weight = jnp.sum(jnp.where(mine, route_weight[0][None], 0.0), axis=-1)
    place = jnp.cumsum(named.astype(jnp.int32), axis=1) - 1
    outer, inner = split_of(sp_count)
    slot = jnp.where(named, place, -1).astype(jnp.float32).reshape(outer, inner, tokens)
    meta = jnp.concatenate([slot, weight.reshape(outer, inner, tokens)], axis=1)
    meta = jnp.pad(meta, ((0, 0), (0, -2 * inner % 8), (0, 0)))
    mixed = run_experts(
        normed, meta, after, expert_gate, expert_up, expert_down, sp_count, capacity, 1
    )
    return mixed[None]


def solution(mesh):
    return jax.shard_map(
        shards,
        mesh=mesh,
        in_specs=(
            P("dp", "sp", None, None),
            P("dp", "sp", None, None),
            P("dp", "sp", None),
            P("dp", "sp", None),
            P("dp", "sp", None),
            P(),
            P(None, "sp"),
            P(None, "sp"),
            P("sp", "dp"),
            P(),
            P("sp", None, None),
            P("sp", None, None),
            P("sp", None, None),
            P("dp", "sp", None),
            P("dp", "sp", None),
        ),
        out_specs=P("dp", "sp", None),
        check_vma=False,
    )
```

```python
import functools
import math

import jax
import jax.numpy as jnp
from jax import lax
from jax.experimental import pallas as pl
from jax.experimental.pallas import tpu as pltpu
from jax.sharding import PartitionSpec as P

epsilon = 1e-06
rope_base = 10000.0
masked_score = -1e30
log2_e = 1.4426950408889634
part_width = 256
link_rate = 46.6e3
link_delay = 2.2


def rotate(values, positions):
    half_width = values.shape[-1] // 2
    frequency = rope_base ** (-jnp.arange(half_width, dtype=jnp.float32) / half_width)
    angles = positions.astype(jnp.float32)[:, None] * frequency[None, :]
    cosine = jnp.cos(angles)
    sine_part = jnp.sin(angles)
    if values.ndim == 3:
        cosine = cosine[:, None, :]
        sine_part = sine_part[:, None, :]
    floats = values.astype(jnp.float32)
    first_half = floats[..., :half_width]
    second_half = floats[..., half_width:]
    turned = jnp.concatenate(
        [
            first_half * cosine - second_half * sine_part,
            second_half * cosine + first_half * sine_part,
        ],
        axis=-1,
    )
    return turned.astype(jnp.bfloat16)


def rms_scaled(values, gain):
    floats = values.astype(jnp.float32)
    return floats * lax.rsqrt(jnp.mean(floats * floats, axis=-1, keepdims=True) + epsilon) * gain


def front_kernel(
    outer, inner, cores, heads_here, nope, channels, scale,
    row_ref, piece_ref, block_ref, nope_ref, rope_ref, cosine_ref, sine_ref, resid_ref, gain_ref,
    after_ref, normed_ref, shared, ups, weights, heads, queries, *sems,
):
    me, dp = lax.axis_index("sp"), lax.axis_index("dp")
    z, y = me // inner, lax.rem(me, inner)
    lanes = weights.shape[0] // cores
    x, core = dp // cores, lax.rem(dp, cores)
    groups, tokens = shared.shape[0], shared.shape[1]
    columns = heads_here * nope
    total = groups * columns
    row_sems, piece_sems, block_sems = sems[0:4], sems[4:10], sems[10:18]

    def remote(source, target, send, recv, peer):
        return pltpu.make_async_remote_copy(
            src_ref=source, dst_ref=target, send_sem=send, recv_sem=recv,
            device_id=peer, device_id_type=pl.DeviceIdType.MESH,
        )

    def at_z(step):
        return {"sp": lax.rem(z + step, outer) * inner + y}

    def at_y(step):
        return {"sp": z * inner + lax.rem(y + step, inner)}

    def at_x(step):
        return {"dp": lax.rem(x + step, lanes) * cores + core}

    def at_core(step):
        return {"dp": x * cores + lax.rem(core + step, cores)}

    barrier = pltpu.get_barrier_semaphore()
    greeted = (
        [at_y(step) for step in range(1, inner)]
        + [at_x(step) for step in range(1, lanes)]
        + [at_core(step) for step in range(1, cores)]
    )
    below, above = z > 0, z < outer - 1
    for peer in greeted:
        pl.semaphore_signal(barrier, inc=1, device_id=peer, device_id_type=pl.DeviceIdType.MESH)
    for way, there in ((-1, below), (1, above)):

        @pl.when(there)
        def _():
            pl.semaphore_signal(
                barrier, inc=1, device_id=at_z(way), device_id_type=pl.DeviceIdType.MESH
            )

    pl.semaphore_wait(barrier, len(greeted) + jnp.where(below & above, 2, 1 if outer > 1 else 0))

    orders = [sorted(range(outer), key=lambda s: (abs(s - at), s)) for at in range(outer)]

    def source_of(turn):
        found = z
        for index in range(1, outer):
            value = jnp.int32(orders[0][index])
            for at in range(1, outer):
                value = jnp.where(z == at, orders[at][index], value)
            found = jnp.where(turn == index, value, found)
        return found

    def member(index):
        return source_of(lax.rem(index, outer)) * inner + lax.rem(y + index // outer, inner)

    class Spread:
        def __init__(self, own, held, sems, lanes, row):
            self.own, self.held, self.sems, self.lanes, self.row = own, held, sems, lanes, row

        def place(self, block, lane=0, at_core=None):
            if self.row is None:
                return self.held.at[block]
            return self.held.at[self.row(lane, core if at_core is None else at_core), block]

        def source(self, index, lane=0):
            own = isinstance(index, int) and index == 0 and isinstance(lane, int) and lane == 0
            return self.own if own else self.place(member(index), lane)

        def along_z(self, turn, way):
            block, at = member(turn), source_of(turn)
            return remote(
                self.source(turn), self.place(block),
                self.sems[0].at[(way + 1) // 2, at], self.sems[1].at[at], at_z(way),
            )

        def along_y(self, step, turn):
            return remote(
                self.source(turn), self.place(member(turn)),
                self.sems[2].at[step - 1, turn], self.sems[3].at[step - 1, turn], at_y(step),
            )

        def along_x(self, step, index):
            return remote(
                self.source(index), self.place(member(index)),
                self.sems[4].at[step - 1, index], self.sems[5].at[step - 1, index], at_x(step),
            )

        def across(self, step, lane, index):
            return remote(
                self.source(index, lane), self.place(member(index), lane),
                self.sems[-2].at[step - 1, lane, index], self.sems[-1].at[step - 1, lane, index], at_core(step),
            )

        def wait(self, ref, sem):
            remote(ref, ref, self.sems[0].at[0, 0], sem, at_core(0)).wait_recv()

        def start_z(self, turn):
            at = source_of(turn)
            for way, there in ((-1, below & (at >= z)), (1, above & (at <= z))):

                @pl.when(there)
                def _():
                    self.along_z(turn, way).start()

        def start_y(self, turn):
            for step in range(1, inner):
                self.along_y(step, turn).start()

        def start_wide(self, index):
            if self.row is None:
                return
            for step in range(1, self.lanes):
                self.along_x(step, index).start()
            for step in range(1, cores):
                self.across(step, 0, index).start()

        def from_z(self, turn):
            self.wait(self.place(member(turn)), self.sems[1].at[source_of(turn)])
            self.start_z(turn)
            self.start_y(turn)
            self.start_wide(turn)

        def from_y(self, index):
            step = inner - index // outer
            self.wait(self.place(member(index)), self.sems[3].at[step - 1, lax.rem(index, outer)])
            self.start_wide(index)

        def from_x(self, lane, index):
            self.wait(self.place(member(index), lane), self.sems[5].at[self.lanes - lane - 1, index])
            for step in range(1, cores):
                self.across(step, lane, index).start()

        def settle(self):
            def one(index, carry):
                for lane in range(self.lanes):
                    for step in range(1, cores):
                        self.wait(
                            self.place(member(index), lane, lax.rem(core + step, cores)),
                            self.sems[-1].at[cores - step - 1, lane, index],
                        )
                return carry

            lax.fori_loop(0, groups, one, 0)

        def drain(self):
            for turn in range(outer):
                at = source_of(turn)
                for way, there in ((-1, below & (at >= z)), (1, above & (at <= z))):

                    @pl.when(there)
                    def _():
                        self.along_z(turn, way).wait_send()

                for step in range(1, inner):
                    self.along_y(step, turn).wait_send()
            if self.row is None:
                return

            def one(index, carry):
                for step in range(1, self.lanes):
                    self.along_x(step, index).wait_send()
                for step in range(1, cores):
                    for lane in range(self.lanes):
                        self.across(step, lane, index).wait_send()
                return carry

            lax.fori_loop(0, groups, one, 0)

    row = Spread(row_ref, shared, row_sems, 1, None)
    piece = Spread(piece_ref, ups, piece_sems, 1, lambda lane, at: at)
    block = Spread(
        block_ref, weights, block_sems, lanes, lambda lane, at: lax.rem(x + lane, lanes) * cores + at
    )
    for spread in (row, piece):
        spread.start_z(0)
        spread.start_y(0)
        spread.start_wide(0)
    block.start_z(0)
    block.start_wide(0)
    shared[me] = row_ref[...]
    ups[core, me] = piece_ref[...]
    weights[dp, me] = block_ref[...]

    rope = cosine_ref.shape[0]
    for pair in range(queries.shape[0] // 2):
        both = jnp.transpose(rope_ref[:, pair * 4 * rope : (pair + 1) * 4 * rope].astype(jnp.float32))
        for half in range(2):
            head = 2 * pair + half
            first = both[half * 2 * rope : half * 2 * rope + rope]
            second = both[half * 2 * rope + rope : (half + 1) * 2 * rope]
            cosine, sine_part = cosine_ref[...], sine_ref[...]
            queries[head, nope : nope + 2 * rope] = jnp.concatenate(
                [first * cosine - second * sine_part, second * cosine + first * sine_part], axis=0
            ).astype(queries.dtype)
            queries[head, nope + 2 * rope :] = jnp.zeros(
                (queries.shape[1] - nope - 2 * rope, tokens), queries.dtype
            )
            queries[head, 0:nope] = jnp.transpose(
                nope_ref[:, head * nope : (head + 1) * nope].astype(jnp.float32)
            ).astype(queries.dtype)

    for turn in range(1, outer):
        row.from_z(turn)
        piece.from_z(turn)
    block.start_y(0)
    for turn in range(1, outer - 1):
        block.from_z(turn)
    for index in range(outer, groups):
        row.from_y(index)
        piece.from_y(index)
    piece.settle()

    key_ids = lax.broadcasted_iota(jnp.int32, (tokens, tokens), 0)
    query_ids = lax.broadcasted_iota(jnp.int32, (tokens, tokens), 1)
    allowed = key_ids <= query_ids

    def attend_group(group):
        up = ups[:, group].reshape(channels, 2 * columns)
        up_keys = up[:, 0:columns]
        up_values = up[:, columns : 2 * columns]
        up_values_t = jnp.transpose(up_values.astype(jnp.float32)).astype(jnp.bfloat16)

        def scores_of(chunk):
            latent = shared[chunk, :, 0:channels]
            turned = shared[chunk, :, channels:]
            keys = jnp.dot(latent, up_keys, preferred_element_type=jnp.float32).astype(jnp.bfloat16)
            values_t = lax.dot_general(
                up_values_t, latent, (((1,), (1,)), ((), ())), preferred_element_type=jnp.float32
            ).astype(jnp.bfloat16)
            scores = []
            for head in range(heads_here):
                full = jnp.concatenate([keys[:, head * nope : (head + 1) * nope], turned], axis=1)
                scores.append(
                    jnp.dot(
                        full, queries[group * heads_here + head], preferred_element_type=jnp.float32
                    )
                    * (scale * log2_e)
                )
            return scores, [values_t[h * nope : (h + 1) * nope, :] for h in range(heads_here)]

        scores, values = scores_of(me)
        state = []
        for score, value in zip(scores, values):
            score = jnp.where(allowed, score, masked_score)
            largest = jnp.max(score, axis=0, keepdims=True)
            powers = jnp.exp2(score - largest)
            state.append(
                (
                    largest,
                    jnp.sum(powers, axis=0, keepdims=True),
                    jnp.dot(value, powers.astype(jnp.bfloat16), preferred_element_type=jnp.float32),
                )
            )

        def step(chunk, state):
            scores, values = scores_of(chunk)
            after = []
            for (largest, total, kept), score, value in zip(state, scores, values):
                now = jnp.maximum(largest, jnp.max(score, axis=0, keepdims=True))
                fade = jnp.exp2(largest - now)
                powers = jnp.exp2(score - now)
                after.append(
                    (
                        now,
                        total * fade + jnp.sum(powers, axis=0, keepdims=True),
                        kept * fade
                        + jnp.dot(
                            value, powers.astype(jnp.bfloat16), preferred_element_type=jnp.float32
                        ),
                    )
                )
            return tuple(after)

        state = lax.fori_loop(0, me, step, tuple(state))
        for head, (_, total, kept) in enumerate(state):
            start = pl.multiple_of(group * columns + head * nope, nope)
            heads[:, pl.ds(start, nope)] = jnp.transpose(kept / total).astype(heads.dtype)

    def one_group(group, carry):
        attend_group(group)

        @pl.when(group == 0)
        def _():
            block.from_z(outer - 1)

        nearby = group + outer - 1

        @pl.when((group > 0) & (nearby < groups))
        def _():
            block.from_y(nearby)

        @pl.when(group >= 1)
        def _():
            for lane in range(1, lanes):
                block.from_x(lane, group - 1)

        return carry

    lax.fori_loop(0, groups, one_group, 0)
    for lane in range(1, lanes):
        block.from_x(lane, groups - 1)
    block.settle()

    parts, width = weights.shape[0], weights.shape[3]
    pieces, narrow = normed_ref.shape[0], normed_ref.shape[2]
    squares = jnp.zeros((tokens, 1), jnp.float32)
    for part in range(parts):
        projected = (
            jnp.dot(
                heads[...], weights[part].reshape(total, width), preferred_element_type=jnp.float32
            )
            .astype(jnp.bfloat16)
            .astype(jnp.float32)
        )
        cols = slice(part * width, (part + 1) * width)
        after = resid_ref[:, cols].astype(jnp.float32) + projected
        each = width // narrow
        for at in range(each):
            after_ref[part * each + at] = after[:, at * narrow : (at + 1) * narrow]
        squares += jnp.sum(after * after, axis=1, keepdims=True)
    factor = lax.rsqrt(squares / (parts * width) + epsilon)
    for part in range(pieces):
        cols = slice(part * narrow, (part + 1) * narrow)
        normed_ref[part] = (after_ref[part] * factor * gain_ref[:, cols]).astype(normed_ref.dtype)
    row.drain()
    piece.drain()
    block.drain()


def run_front(
    row, piece, block, query_nope, query_rope, cosine, sine_part, resid, gain,
    sp_count, dp_count, cores, heads_here, nope, channels, scale, number,
):
    outer, inner = split_of(sp_count)
    lanes = dp_count // cores
    tokens, model = resid.shape
    width = min(model // dp_count, part_width)
    dma = pltpu.SemaphoreType.DMA
    narrow = [
        dma((2, outer)),
        dma((outer,)),
        dma((max(inner - 1, 1), outer)),
        dma((max(inner - 1, 1), outer)),
    ]
    beside = [dma((max(lanes - 1, 1), sp_count))] * 2

    def crossing(count):
        return [dma((max(cores - 1, 1), count, sp_count))] * 2

    vmem = pl.BlockSpec(memory_space=pltpu.VMEM)
    return pl.pallas_call(
        functools.partial(front_kernel, outer, inner, cores, heads_here, nope, channels, scale),
        out_shape=[
            jax.ShapeDtypeStruct((model // width, tokens, width), jnp.float32),
            jax.ShapeDtypeStruct((model // width, tokens, width), jnp.bfloat16),
        ],
        in_specs=[vmem] * 9,
        out_specs=[vmem] * 2,
        scratch_shapes=[
            pltpu.VMEM((sp_count,) + row.shape, row.dtype),
            pltpu.VMEM((cores, sp_count) + piece.shape, piece.dtype),
            pltpu.VMEM((dp_count, sp_count) + block.shape, block.dtype),
            pltpu.VMEM((tokens, model), jnp.bfloat16),
            pltpu.VMEM((sp_count * heads_here, nope + 128, tokens), jnp.bfloat16),
        ]
        + narrow
        + narrow
        + crossing(1)
        + narrow
        + beside
        + crossing(lanes),
        compiler_params=pltpu.CompilerParams(
            collective_id=number, has_side_effects=True, vmem_limit_bytes=40 * 2**20
        ),
        cost_estimate=pl.CostEstimate(flops=2 * 10**10, bytes_accessed=10**7, transcendentals=0),
    )(row, piece, block, query_nope, query_rope, cosine, sine_part, resid, gain)


def split_of(sp_count):
    inner = max(d for d in range(1, math.isqrt(sp_count) + 1) if sp_count % d == 0)
    return sp_count // inner, inner


def plan_tasks(outer, parts, across_z, across_y):
    def forward(at, source):
        return 1 if source < at < outer - 1 else (-1 if 0 < at < source else 0)

    spent = {"A": 0.5, "B": 4.5, "C": 0.6, "F": 0.05, "R": 0.3}
    todo = [
        [("B", s, 0) for s in range(outer)]
        + [(kind, s, p) for s in range(outer) for p in range(parts) for kind in "AC"]
        + [("F", s, p) for s in range(outer) for p in range(parts) if forward(at, s)]
        + [("R", s, p) for s in range(outer) for p in range(parts) if s != at and 0 < at < outer - 1]
        for at in range(outer)
    ]
    free, landed = {}, {}
    clock, done, order = [2.0] * outer, [set() for _ in range(outer)], [[] for _ in range(outer)]

    def send(at, link, target, key, time, length):
        free[at, link] = max(time, free.get((at, link), 0.0)) + length
        landed[target, key] = free[at, link] + link_delay

    def ready(at, task):
        kind, source, part = task
        needed, before = [], []
        wait = 0.0
        if kind in "AF" and source != at:
            needed.append(("block", source, part))
        if kind == "A":
            before += [("F", source, part)] if forward(at, source) else []
            before += [("A", source, part - 1)] if part else []
            wait = free.get((at, "y"), 0.0) - 3.0
        if kind == "F" and part:
            before.append(("F", source, part - 1))
        if kind == "B":
            before += [("A", source, p) for p in range(parts)]
            before += [("B", s, 0) for s in range(outer) if s != at and source == at]
            needed += [("row", source, p) for p in range(parts)]
            wait = free.get((at, "y"), 0.0) - 6.0
        if kind == "C":
            before.append(("B", source, 0))
            needed.append(("back", source, part))
        if kind == "R":
            before.append(("C", source, part))
            needed.append(("sum", source, part))
        if any(task not in done[at] for task in before) or any((at, key) not in landed for key in needed):
            return None
        return max([clock[at], wait] + [landed[at, key] for key in needed])

    def rank(at, task):
        kind, source, part = task
        own = source == at
        return (8 if own and kind == "C" else "FRBCA".index(kind), abs(source - at), part)

    for at in range(outer):
        for part in range(parts):
            for way in (1, -1):
                if 0 <= at + way < outer:
                    send(at, way, at + way, ("block", at, part), 2.0, across_z)
    while any(todo):
        chosen = None
        for at in range(outer):
            times = [(ready(at, task), task) for task in todo[at]]
            times = [(time, task) for time, task in times if time is not None]
            if times:
                first = min(time for time, _ in times)
                task = min((t for time, t in times if time <= first), key=lambda t: rank(at, t))
                if chosen is None or first < chosen[0]:
                    chosen = (first, at, task)
        time, at, task = chosen
        kind, source, part = task
        todo[at].remove(task)
        order[at].append(task)
        done[at].add(task)
        clock[at] = end = time + spent[kind]
        way = -1 if source < at else 1
        if kind == "F":
            send(at, forward(at, source), at + forward(at, source), ("block", source, part), end, across_z)
        if kind == "A":
            send(at, "y", at, ("row", source, part), end, across_y)
        if kind == "B":
            for p in range(parts):
                begun = end - spent["B"] * 0.5 * (parts - 1 - p) / parts
                send(at, "y", at, ("back", source, p), begun, across_y)
        last = at == (outer - 1 if way < 0 else 0)
        if source != at and (kind == "R" or (kind == "C" and last)):
            key = ("last", at + way, part) if way > 0 and source == at + way else ("sum", source, part)
            send(at, way, at + way, key, end, across_z)
    return order


def experts_kernel(
    outer, inner, capacity, order,
    normed_ref, meta_ref, after_ref, gate_hbm, up_hbm, down_hbm, out_ref,
    gate_w, up_w, down_w, blocks, metas, picked, rows, made, back, partial, coming, total, gate_acc, up_acc,
    select, columns, spread,
    weight_sems, meta_send, meta_recv, block_send, block_recv, row_send, row_recv,
    back_send, back_recv, sum_send, sum_recv,
):
    me = lax.axis_index("sp")
    z, y = me // inner, lax.rem(me, inner)
    parts, tokens, width = normed_ref.shape
    loads = [
        pltpu.make_async_copy(hbm.at[0], ref, weight_sems.at[at])
        for at, (hbm, ref) in enumerate([(gate_hbm, gate_w), (up_hbm, up_w), (down_hbm, down_w)])
    ]
    for load in loads:
        load.start()

    barrier = pltpu.get_barrier_semaphore()
    steps_z = [lax.rem(z + step, outer) for step in range(1, outer)]
    steps_y = [lax.rem(y + step, inner) for step in range(1, inner)]
    greeted = [{"sp": at * inner + y} for at in steps_z] + [{"sp": z * inner + at} for at in steps_y]
    for peer in greeted:
        pl.semaphore_signal(barrier, inc=1, device_id=peer, device_id_type=pl.DeviceIdType.MESH)
    pl.semaphore_wait(barrier, len(greeted))

    def remote(source, target, send, recv, at_z, at_y):
        return pltpu.make_async_remote_copy(
            src_ref=source, dst_ref=target, send_sem=send, recv_sem=recv,
            device_id={"sp": at_z * inner + at_y}, device_id_type=pl.DeviceIdType.MESH,
        )

    def block_copy(source, part, own, way):
        ref = normed_ref.at[part] if own else blocks.at[source, part]
        return remote(
            ref, blocks.at[source, part],
            block_send.at[(way + 1) // 2, source, part], block_recv.at[source, part], z + way, y,
        )

    def meta_copy(step):
        at = lax.rem(z + step, outer)
        return remote(meta_ref.at[at], metas.at[z], meta_send.at[step - 1], meta_recv.at[z], at, y)

    def row_copy(source, step, part):
        at = lax.rem(y + step, inner)
        return remote(
            picked.at[source, at, part], rows.at[source, y, part],
            row_send.at[source, step - 1, part], row_recv.at[source, y, part], z, at,
        )

    def back_copy(source, step, part):
        at = lax.rem(y + step, inner)
        return remote(
            made.at[source, at, part], back.at[source, y, part],
            back_send.at[source, step - 1, part], back_recv.at[source, y, part], z, at,
        )

    def sum_copy(source, part, way):
        slot = source if way < 0 else jnp.where(source == z + 1, outer, source)
        return remote(
            partial.at[source, part], coming.at[slot, part],
            sum_send.at[source, part], sum_recv.at[slot, part], z + way, y,
        )

    def wait_recv(ref, sem):
        remote(ref, ref, block_send.at[0, 0, 0], sem, z, y).wait_recv()

    for step in range(1, outer):
        meta_copy(step).start()
    for part in range(parts):
        for way in (1, -1):

            @pl.when((z + way >= 0) & (z + way < outer))
            def _():
                block_copy(z, part, True, way).start()

    blocks[z] = normed_ref[...]
    metas[z] = meta_ref[z]

    kinds = "ABCFRW"
    steps = max(len(row) for row in order) + 1

    def coded(row):
        first = [kind for kind, _, _ in row].index("B")
        row = row[:first] + [("W", 0, 0)] + row[first:]
        codes = [(kinds.index(kind) * outer + source) * parts + part for kind, source, part in row]
        return codes + [len(kinds) * outer * parts] * (steps - len(codes))

    base = (len(kinds) + 1) * outer * parts
    rows_coded = [coded(row) for row in order]
    words = []
    for start in range(0, steps, 3):
        value = None
        for at in range(outer):
            word = sum(code * base**index for index, code in enumerate(rows_coded[at][start : start + 3]))
            value = jnp.int32(word) if value is None else jnp.where(z == at, word, value)
        words.append(value)

    def task_of(step):
        index, digit = step // 3, lax.rem(step, 3)
        level = words
        while len(level) > 1:
            even = lax.rem(index, 2) == 0
            level = [
                jnp.where(even, level[at], level[at + 1]) if at + 1 < len(level) else level[at]
                for at in range(0, len(level), 2)
            ]
            index = index // 2
        word = level[0]
        code = jnp.where(digit == 0, word, jnp.where(digit == 1, word // base, word // base**2))
        code = lax.rem(code, base)
        return code // (outer * parts), lax.rem(code // parts, outer), lax.rem(code, parts)

    def forwards(source):
        return [
            (1, (source < z) & (z < outer - 1)),
            (-1, (source > z) & (z > 0)),
        ]

    def ends(source):
        return [
            (-1, (source < z) & (z == outer - 1)),
            (1, (source > z) & (z == 0)),
        ]

    def needs(source):
        return functools.reduce(jnp.logical_or, [needed for _, needed in forwards(source)])

    def arrive(source, part):
        wait_recv(blocks.at[source, part], block_recv.at[source, part])

    def pick(source, part):
        @pl.when((source != z) & (part == 0))
        def _():
            wait_recv(metas.at[source], meta_recv.at[source])

        @pl.when(part == 0)
        def _():
            slot_ids = lax.broadcasted_iota(jnp.int32, (capacity, tokens), 0).astype(jnp.float32)
            for at in range(inner):
                select[source, at * capacity : (at + 1) * capacity] = jnp.where(
                    metas[source, at : at + 1, :] == slot_ids, 1.0, 0.0
                ).astype(jnp.bfloat16)

        @pl.when((source != z) & ~needs(source))
        def _():
            arrive(source, part)

        found = jnp.dot(
            select[source], blocks[source, part], preferred_element_type=jnp.float32
        ).astype(jnp.bfloat16)
        for at in range(inner):
            picked[source, at, part] = found[at * capacity : (at + 1) * capacity]
        rows[source, y, part] = picked[source, y, part]
        for step in range(1, inner):
            row_copy(source, step, part).start()

    def apply_experts(source):
        gate_acc[...] = jnp.zeros_like(gate_acc)
        up_acc[...] = jnp.zeros_like(up_acc)

        def widen(pair, carry):
            for part in (2 * pair, 2 * pair + 1):
                for step in range(1, inner):
                    at = lax.rem(y + step, inner)
                    wait_recv(rows.at[source, at, part], row_recv.at[source, at, part])
            taken = jnp.concatenate(
                [
                    jnp.concatenate([rows[source, at, 2 * pair + half] for half in range(2)], axis=1)
                    for at in range(inner)
                ],
                axis=0,
            )
            depth = pl.ds(pl.multiple_of(pair * 2 * width, 2 * width), 2 * width)
            gate_acc[...] += jnp.dot(taken, gate_w[depth, :], preferred_element_type=jnp.float32)
            up_acc[...] += jnp.dot(taken, up_w[depth, :], preferred_element_type=jnp.float32)
            return carry

        lax.fori_loop(0, parts // 2, widen, 0)
        gate = gate_acc[...]
        hidden = (gate / (1.0 + jnp.exp(-gate)) * up_acc[...]).astype(jnp.bfloat16)

        for part in range(parts):
            cols = slice(part * width, (part + 1) * width)
            result = jnp.dot(hidden, down_w[:, cols], preferred_element_type=jnp.float32).astype(
                jnp.bfloat16
            )
            for at in range(inner):
                made[source, at, part] = result[at * capacity : (at + 1) * capacity]
            back[source, y, part] = made[source, y, part]
            for step in range(1, inner):
                back_copy(source, step, part).start()

        columns[source] = jnp.transpose(metas[source])
        slot_lanes = lax.broadcasted_iota(jnp.int32, (tokens, capacity), 1).astype(jnp.float32)
        for at in range(inner):
            spread[source, at] = jnp.where(
                columns[source, :, at : at + 1] == slot_lanes, 1.0, 0.0
            ).astype(jnp.bfloat16)

    def combine(source, part):
        for step in range(1, inner):
            at = lax.rem(y + step, inner)
            wait_recv(back.at[source, at, part], back_recv.at[source, at, part])
        summed = sum(
            jnp.dot(spread[source, at], back[source, at, part], preferred_element_type=jnp.float32)
            * columns[source, :, inner + at : inner + at + 1]
            for at in range(inner)
        )

        @pl.when(source == z)
        def _():
            total[part] = after_ref[part] + summed

        @pl.when(source != z)
        def _():
            partial[source, part] = summed.astype(jnp.bfloat16)

        for way, needed in ends(source):

            @pl.when(needed)
            def _():
                sum_copy(source, part, way).start()

    def relay(source, part):
        wait_recv(coming.at[source, part], sum_recv.at[source, part])
        partial[source, part] = (
            partial[source, part].astype(jnp.float32) + coming[source, part].astype(jnp.float32)
        ).astype(jnp.bfloat16)
        for way in (1, -1):

            @pl.when((source > z) if way > 0 else (source < z))
            def _():
                sum_copy(source, part, way).start()

    def run_task(step, carry):
        kind, source, part = task_of(step)

        @pl.when(kind == 0)
        def _():
            pick(source, part)

        @pl.when(kind == 1)
        def _():
            apply_experts(source)

        @pl.when(kind == 2)
        def _():
            combine(source, part)

        @pl.when(kind == 3)
        def _():
            arrive(source, part)
            for way, needed in forwards(source):

                @pl.when(needed)
                def _():
                    block_copy(source, part, False, way).start()

        @pl.when(kind == 4)
        def _():
            relay(source, part)

        @pl.when(kind == 5)
        def _():
            for load in loads:
                load.wait()

        return carry

    lax.fori_loop(0, steps, run_task, 0)

    for part in range(parts):
        for slot, valid in ((z, z < outer - 1), (outer, z > 0)):

            @pl.when(valid)
            def _():
                wait_recv(coming.at[slot, part], sum_recv.at[slot, part])
                total[part] += coming[slot, part].astype(jnp.float32)

        out_ref[:, part * width : (part + 1) * width] = total[part].astype(out_ref.dtype)

    for step in range(1, outer):
        meta_copy(step).wait_send()
    def drain(source, carry):
        for part in range(parts):
            for way in (1, -1):
                onward = (z + way >= 0) & (z + way < outer)
                passing = (source == z) | ((source < z) if way > 0 else (source > z))

                @pl.when(onward & passing)
                def _():
                    block_copy(source, part, False, way).wait_send()

                @pl.when(onward & ((source > z) if way > 0 else (source < z)))
                def _():
                    sum_copy(source, part, way).wait_send()

            for step in range(1, inner):
                row_copy(source, step, part).wait_send()
                back_copy(source, step, part).wait_send()
        return carry

    lax.fori_loop(0, outer, drain, 0)


def run_experts(normed, meta, after, gate, up, down, sp_count, capacity, number):
    outer, inner = split_of(sp_count)
    parts, tokens, width = normed.shape
    model, hidden = gate.shape[1:]
    across_z = tokens * width * 2 / link_rate
    order = plan_tasks(outer, parts, across_z, across_z * capacity / tokens)
    dma = pltpu.SemaphoreType.DMA
    bf16, f32 = jnp.bfloat16, jnp.float32
    steps_y = max(inner - 1, 1)
    vmem = pl.BlockSpec(memory_space=pltpu.VMEM)
    anywhere = pl.BlockSpec(memory_space=pl.ANY)
    return pl.pallas_call(
        functools.partial(experts_kernel, outer, inner, capacity, order),
        out_shape=jax.ShapeDtypeStruct((tokens, parts * width), bf16),
        in_specs=[vmem, vmem, vmem, anywhere, anywhere, anywhere],
        out_specs=vmem,
        scratch_shapes=[
            pltpu.VMEM((model, hidden), bf16),
            pltpu.VMEM((model, hidden), bf16),
            pltpu.VMEM((hidden, model), bf16),
            pltpu.VMEM((outer, parts, tokens, width), bf16),
            pltpu.VMEM((outer,) + meta.shape[1:], f32),
            pltpu.VMEM((outer, inner, parts, capacity, width), bf16),
            pltpu.VMEM((outer, inner, parts, capacity, width), bf16),
            pltpu.VMEM((outer, inner, parts, capacity, width), bf16),
            pltpu.VMEM((outer, inner, parts, capacity, width), bf16),
            pltpu.VMEM((outer, parts, tokens, width), bf16),
            pltpu.VMEM((outer + 1, parts, tokens, width), bf16),
            pltpu.VMEM((parts, tokens, width), f32),
            pltpu.VMEM((inner * capacity, hidden), f32),
            pltpu.VMEM((inner * capacity, hidden), f32),
            pltpu.VMEM((outer, inner * capacity, tokens), bf16),
            pltpu.VMEM((outer, tokens, meta.shape[1]), f32),
            pltpu.VMEM((outer, inner, tokens, capacity), bf16),
            dma((3,)),
            dma((outer,)),
            dma((outer,)),
            dma((2, outer, parts)),
            dma((outer, parts)),
            dma((outer, steps_y, parts)),
            dma((outer, inner, parts)),
            dma((outer, steps_y, parts)),
            dma((outer, inner, parts)),
            dma((outer, parts)),
            dma((outer + 1, parts)),
        ],
        compiler_params=pltpu.CompilerParams(
            collective_id=number, has_side_effects=True, vmem_limit_bytes=60 * 2**20
        ),
        cost_estimate=pl.CostEstimate(
            flops=6 * sp_count * capacity * model * hidden, bytes_accessed=10**7, transcendentals=0
        ),
    )(normed, meta, after, gate, up, down)


def shards(
    query_nope,
    query_rope,
    latent,
    key_rope,
    resid,
    latent_gain,
    key_up,
    value_up,
    out_proj,
    norm_gain,
    expert_gate,
    expert_up,
    expert_down,
    routes,
    route_weight,
):
    tokens, channels = latent.shape[1:]
    sp_count = lax.axis_size("sp")
    dp_count = lax.axis_size("dp")
    me = lax.axis_index("sp")
    nope, rope = query_nope.shape[-1], query_rope.shape[-1]
    heads_here = key_up.shape[1] // nope
    scale = (nope + rope) ** (-0.5)
    local_pos = me * tokens + jnp.arange(tokens, dtype=jnp.int32)
    latent_normed = rms_scaled(latent[0], latent_gain).astype(jnp.bfloat16)
    key_turned = rotate(key_rope[0], local_pos)
    spare = 128 - rope
    row = jnp.concatenate(
        [latent_normed, key_turned, jnp.zeros((tokens, spare), jnp.bfloat16)], axis=1
    )
    cores = 2 if dp_count % 2 == 0 else 1
    piece = channels // cores
    ups = lax.dynamic_slice_in_dim(
        jnp.concatenate([key_up, value_up], axis=1),
        lax.rem(lax.axis_index("dp"), cores) * piece, piece, axis=0,
    )
    frequency = rope_base ** (-jnp.arange(rope // 2, dtype=jnp.float32) / (rope // 2))
    angles = frequency[:, None] * local_pos.astype(jnp.float32)[None, :]
    after, normed = run_front(
        row, ups, out_proj, query_nope[0].reshape(tokens, -1), query_rope[0].reshape(tokens, -1),
        jnp.cos(angles), jnp.sin(angles), resid[0], norm_gain[None],
        sp_count, dp_count, cores, heads_here, nope, channels, scale, 0,
    )

    experts_all = sp_count * expert_gate.shape[0]
    capacity = 4 * tokens // experts_all
    ids = jnp.arange(experts_all, dtype=jnp.int32)[:, None, None]
    mine = routes[0][None] == ids
    named = jnp.any(mine, axis=-1)
    weight = jnp.sum(jnp.where(mine, route_weight[0][None], 0.0), axis=-1)
    place = jnp.cumsum(named.astype(jnp.int32), axis=1) - 1
    outer, inner = split_of(sp_count)
    slot = jnp.where(named, place, -1).astype(jnp.float32).reshape(outer, inner, tokens)
    meta = jnp.concatenate([slot, weight.reshape(outer, inner, tokens)], axis=1)
    meta = jnp.pad(meta, ((0, 0), (0, -2 * inner % 8), (0, 0)))
    mixed = run_experts(
        normed, meta, after, expert_gate, expert_up, expert_down, sp_count, capacity, 1
    )
    return mixed[None]


def solution(mesh):
    return jax.shard_map(
        shards,
        mesh=mesh,
        in_specs=(
            P("dp", "sp", None, None),
            P("dp", "sp", None, None),
            P("dp", "sp", None),
            P("dp", "sp", None),
            P("dp", "sp", None),
            P(),
            P(None, "sp"),
            P(None, "sp"),
            P("sp", "dp"),
            P(),
            P("sp", None, None),
            P("sp", None, None),
            P("sp", None, None),
            P("dp", "sp", None),
            P("dp", "sp", None),
        ),
        out_specs=P("dp", "sp", None),
        check_vma=False,
    )
```

```python
import functools
import math

import jax
import jax.numpy as jnp
from jax import lax
from jax.experimental import pallas as pl
from jax.experimental.pallas import tpu as pltpu
from jax.sharding import PartitionSpec as P

epsilon = 1e-06
rope_base = 10000.0
masked_score = -1e30
log2_e = 1.4426950408889634
part_width = 256
extra_vmem = 3 * 2**19
link_rate = 46.6e3
link_delay = 2.2


def rotate(values, positions):
    half_width = values.shape[-1] // 2
    frequency = rope_base ** (-jnp.arange(half_width, dtype=jnp.float32) / half_width)
    angles = positions.astype(jnp.float32)[:, None] * frequency[None, :]
    cosine = jnp.cos(angles)
    sine_part = jnp.sin(angles)
    if values.ndim == 3:
        cosine = cosine[:, None, :]
        sine_part = sine_part[:, None, :]
    floats = values.astype(jnp.float32)
    first_half = floats[..., :half_width]
    second_half = floats[..., half_width:]
    turned = jnp.concatenate(
        [
            first_half * cosine - second_half * sine_part,
            second_half * cosine + first_half * sine_part,
        ],
        axis=-1,
    )
    return turned.astype(jnp.bfloat16)


def rms_scaled(values, gain):
    floats = values.astype(jnp.float32)
    return floats * lax.rsqrt(jnp.mean(floats * floats, axis=-1, keepdims=True) + epsilon) * gain


def front_kernel(
    outer, inner, cores, heads_here, nope, channels, scale,
    row_ref, piece_ref, block_ref, nope_ref, rope_ref, cosine_ref, sine_ref, resid_ref, gain_ref,
    routes_ref, route_weight_ref, after_ref, normed_ref, meta_ref, shared, ups, weights, heads, queries, *sems,
):
    me, dp = lax.axis_index("sp"), lax.axis_index("dp")
    z, y = me // inner, lax.rem(me, inner)
    lanes = weights.shape[0] // cores
    x, core = dp // cores, lax.rem(dp, cores)
    groups, tokens = shared.shape[0], shared.shape[1]
    columns = heads_here * nope
    total = groups * columns
    row_sems, piece_sems, block_sems = sems[0:4], sems[4:10], sems[10:18]

    def remote(source, target, send, recv, peer):
        return pltpu.make_async_remote_copy(
            src_ref=source, dst_ref=target, send_sem=send, recv_sem=recv,
            device_id=peer, device_id_type=pl.DeviceIdType.MESH,
        )

    def at_z(step):
        return {"sp": lax.rem(z + step, outer) * inner + y}

    def at_y(step):
        return {"sp": z * inner + lax.rem(y + step, inner)}

    def at_x(step):
        return {"dp": lax.rem(x + step, lanes) * cores + core}

    def at_core(step):
        return {"dp": x * cores + lax.rem(core + step, cores)}

    barrier = pltpu.get_barrier_semaphore()
    greeted = (
        [at_y(step) for step in range(1, inner)]
        + [at_x(step) for step in range(1, lanes)]
        + [at_core(step) for step in range(1, cores)]
    )
    below, above = z > 0, z < outer - 1
    for peer in greeted:
        pl.semaphore_signal(barrier, inc=1, device_id=peer, device_id_type=pl.DeviceIdType.MESH)
    for way, there in ((-1, below), (1, above)):

        @pl.when(there)
        def _():
            pl.semaphore_signal(
                barrier, inc=1, device_id=at_z(way), device_id_type=pl.DeviceIdType.MESH
            )

    pl.semaphore_wait(barrier, len(greeted) + jnp.where(below & above, 2, 1 if outer > 1 else 0))

    orders = [sorted(range(outer), key=lambda s: (abs(s - at), s)) for at in range(outer)]

    def source_of(turn):
        found = z
        for index in range(1, outer):
            value = jnp.int32(orders[0][index])
            for at in range(1, outer):
                value = jnp.where(z == at, orders[at][index], value)
            found = jnp.where(turn == index, value, found)
        return found

    def member(index):
        return source_of(lax.rem(index, outer)) * inner + lax.rem(y + index // outer, inner)

    class Spread:
        def __init__(self, own, held, sems, lanes, row):
            self.own, self.held, self.sems, self.lanes, self.row = own, held, sems, lanes, row

        def place(self, block, lane=0, at_core=None):
            if self.row is None:
                return self.held.at[block]
            return self.held.at[self.row(lane, core if at_core is None else at_core), block]

        def source(self, index, lane=0):
            own = isinstance(index, int) and index == 0 and isinstance(lane, int) and lane == 0
            return self.own if own else self.place(member(index), lane)

        def along_z(self, turn, way):
            block, at = member(turn), source_of(turn)
            return remote(
                self.source(turn), self.place(block),
                self.sems[0].at[(way + 1) // 2, at], self.sems[1].at[at], at_z(way),
            )

        def along_y(self, step, turn):
            return remote(
                self.source(turn), self.place(member(turn)),
                self.sems[2].at[step - 1, turn], self.sems[3].at[step - 1, turn], at_y(step),
            )

        def along_x(self, step, index):
            return remote(
                self.source(index), self.place(member(index)),
                self.sems[4].at[step - 1, index], self.sems[5].at[step - 1, index], at_x(step),
            )

        def across(self, step, lane, index):
            return remote(
                self.source(index, lane), self.place(member(index), lane),
                self.sems[-2].at[step - 1, lane, index], self.sems[-1].at[step - 1, lane, index], at_core(step),
            )

        def wait(self, ref, sem):
            remote(ref, ref, self.sems[0].at[0, 0], sem, at_core(0)).wait_recv()

        def start_z(self, turn):
            at = source_of(turn)
            for way, there in ((-1, below & (at >= z)), (1, above & (at <= z))):

                @pl.when(there)
                def _():
                    self.along_z(turn, way).start()

        def start_y(self, turn):
            for step in range(1, inner):
                self.along_y(step, turn).start()

        def start_wide(self, index):
            if self.row is None:
                return
            for step in range(1, self.lanes):
                self.along_x(step, index).start()
            for step in range(1, cores):
                self.across(step, 0, index).start()

        def from_z(self, turn):
            self.wait(self.place(member(turn)), self.sems[1].at[source_of(turn)])
            self.start_z(turn)
            self.start_y(turn)
            self.start_wide(turn)

        def from_y(self, index):
            step = inner - index // outer
            self.wait(self.place(member(index)), self.sems[3].at[step - 1, lax.rem(index, outer)])
            self.start_wide(index)

        def from_x(self, lane, index):
            self.wait(self.place(member(index), lane), self.sems[5].at[self.lanes - lane - 1, index])
            for step in range(1, cores):
                self.across(step, lane, index).start()

        def settle(self):
            def one(index, carry):
                for lane in range(self.lanes):
                    for step in range(1, cores):
                        self.wait(
                            self.place(member(index), lane, lax.rem(core + step, cores)),
                            self.sems[-1].at[cores - step - 1, lane, index],
                        )
                return carry

            lax.fori_loop(0, groups, one, 0)

        def drain(self):
            for turn in range(outer):
                at = source_of(turn)
                for way, there in ((-1, below & (at >= z)), (1, above & (at <= z))):

                    @pl.when(there)
                    def _():
                        self.along_z(turn, way).wait_send()

                for step in range(1, inner):
                    self.along_y(step, turn).wait_send()
            if self.row is None:
                return

            def one(index, carry):
                for step in range(1, self.lanes):
                    self.along_x(step, index).wait_send()
                for step in range(1, cores):
                    for lane in range(self.lanes):
                        self.across(step, lane, index).wait_send()
                return carry

            lax.fori_loop(0, groups, one, 0)

    row = Spread(row_ref, shared, row_sems, 1, None)
    piece = Spread(piece_ref, ups, piece_sems, 1, lambda lane, at: at)
    block = Spread(
        block_ref, weights, block_sems, lanes, lambda lane, at: lax.rem(x + lane, lanes) * cores + at
    )
    for spread in (row, piece):
        spread.start_z(0)
        spread.start_y(0)
        spread.start_wide(0)
    block.start_z(0)
    block.start_wide(0)
    shared[me] = row_ref[...]
    ups[core, me] = piece_ref[...]
    weights[dp, me] = block_ref[...]

    rope = cosine_ref.shape[0]
    for pair in range(queries.shape[0] // 2):
        both = jnp.transpose(rope_ref[:, pair * 4 * rope : (pair + 1) * 4 * rope].astype(jnp.float32))
        for half in range(2):
            head = 2 * pair + half
            first = both[half * 2 * rope : half * 2 * rope + rope]
            second = both[half * 2 * rope + rope : (half + 1) * 2 * rope]
            cosine, sine_part = cosine_ref[...], sine_ref[...]
            queries[head, nope : nope + 2 * rope] = jnp.concatenate(
                [first * cosine - second * sine_part, second * cosine + first * sine_part], axis=0
            ).astype(queries.dtype)
            queries[head, nope + 2 * rope :] = jnp.zeros(
                (queries.shape[1] - nope - 2 * rope, tokens), queries.dtype
            )
            queries[head, 0:nope] = jnp.transpose(
                nope_ref[:, head * nope : (head + 1) * nope].astype(jnp.float32)
            ).astype(queries.dtype)

    experts = meta_ref.shape[0] * inner
    ids = lax.broadcasted_iota(jnp.int32, (experts, tokens), 0)
    mine = [routes_ref[at : at + 1, :] == ids for at in range(routes_ref.shape[0])]
    named = functools.reduce(jnp.logical_or, mine)
    weight = sum(
        jnp.where(chosen, route_weight_ref[at : at + 1, :], 0.0) for at, chosen in enumerate(mine)
    )
    earlier = lax.broadcasted_iota(jnp.int32, (tokens, tokens), 0)
    upto = jnp.where(earlier < lax.broadcasted_iota(jnp.int32, (tokens, tokens), 1), 1.0, 0.0)
    place = jnp.dot(
        jnp.where(named, 1.0, 0.0).astype(jnp.bfloat16), upto.astype(jnp.bfloat16),
        preferred_element_type=jnp.float32,
    )
    slot = jnp.where(named, place, -1.0)
    meta_ref[...] = jnp.zeros_like(meta_ref)
    for at in range(meta_ref.shape[0]):
        meta_ref[at, 0:inner] = slot[at * inner : (at + 1) * inner]
        meta_ref[at, inner : 2 * inner] = weight[at * inner : (at + 1) * inner]

    for turn in range(1, outer):
        row.from_z(turn)
        piece.from_z(turn)
    block.start_y(0)
    for turn in range(1, outer - 1):
        block.from_z(turn)
    for index in range(outer, groups):
        row.from_y(index)
        piece.from_y(index)
    piece.settle()

    span = 2 * tokens if groups % 2 == 0 else tokens
    chunks = span // tokens
    ending = me // chunks
    key_ids = lax.broadcasted_iota(jnp.int32, (span, tokens), 0)
    query_ids = lax.broadcasted_iota(jnp.int32, (span, tokens), 1)
    allowed = key_ids <= query_ids + lax.rem(me, chunks) * tokens

    def attend_group(group):
        up = ups[:, group].reshape(channels, 2 * columns)
        up_keys = up[:, 0:columns]
        up_values = up[:, columns : 2 * columns]
        up_values_t = jnp.transpose(up_values.astype(jnp.float32)).astype(jnp.bfloat16)

        def scores_of(place):
            taken = shared[pl.ds(place * chunks, chunks)].reshape(span, shared.shape[2])
            latent = taken[:, 0:channels]
            turned = taken[:, channels:]
            keys = jnp.dot(latent, up_keys, preferred_element_type=jnp.float32).astype(jnp.bfloat16)
            values_t = lax.dot_general(
                up_values_t, latent, (((1,), (1,)), ((), ())), preferred_element_type=jnp.float32
            ).astype(jnp.bfloat16)
            scores = []
            for head in range(heads_here):
                full = jnp.concatenate([keys[:, head * nope : (head + 1) * nope], turned], axis=1)
                scores.append(
                    jnp.dot(
                        full, queries[group * heads_here + head], preferred_element_type=jnp.float32
                    )
                    * (scale * log2_e)
                )
            return scores, [values_t[h * nope : (h + 1) * nope, :] for h in range(heads_here)]

        scores, values = scores_of(ending)
        state = []
        for score, value in zip(scores, values):
            score = jnp.where(allowed, score, masked_score)
            largest = jnp.max(score, axis=0, keepdims=True)
            powers = jnp.exp2(score - largest)
            state.append(
                (
                    largest,
                    jnp.sum(powers, axis=0, keepdims=True),
                    jnp.dot(value, powers.astype(jnp.bfloat16), preferred_element_type=jnp.float32),
                )
            )

        def step(place, state):
            scores, values = scores_of(place)
            after = []
            for (largest, total, kept), score, value in zip(state, scores, values):
                now = jnp.maximum(largest, jnp.max(score, axis=0, keepdims=True))
                fade = jnp.exp2(largest - now)
                powers = jnp.exp2(score - now)
                after.append(
                    (
                        now,
                        total * fade + jnp.sum(powers, axis=0, keepdims=True),
                        kept * fade
                        + jnp.dot(
                            value, powers.astype(jnp.bfloat16), preferred_element_type=jnp.float32
                        ),
                    )
                )
            return tuple(after)

        state = lax.fori_loop(0, ending, step, tuple(state))
        for head, (_, total, kept) in enumerate(state):
            start = pl.multiple_of(group * columns + head * nope, nope)
            heads[:, pl.ds(start, nope)] = jnp.transpose(kept / total).astype(heads.dtype)

    def one_group(group, carry):
        attend_group(group)

        @pl.when(group == 0)
        def _():
            block.from_z(outer - 1)

        nearby = group + outer - 1

        @pl.when((group > 0) & (nearby < groups))
        def _():
            block.from_y(nearby)

        @pl.when(group >= 1)
        def _():
            for lane in range(1, lanes):
                block.from_x(lane, group - 1)

        return carry

    lax.fori_loop(0, groups, one_group, 0)
    for lane in range(1, lanes):
        block.from_x(lane, groups - 1)
    block.settle()

    parts, width = weights.shape[0], weights.shape[3]
    pieces, narrow = normed_ref.shape[0], normed_ref.shape[2]
    squares = jnp.zeros((tokens, 1), jnp.float32)
    for part in range(parts):
        projected = (
            jnp.dot(
                heads[...], weights[part].reshape(total, width), preferred_element_type=jnp.float32
            )
            .astype(jnp.bfloat16)
            .astype(jnp.float32)
        )
        cols = slice(part * width, (part + 1) * width)
        after = resid_ref[:, cols].astype(jnp.float32) + projected
        each = width // narrow
        for at in range(each):
            after_ref[part * each + at] = after[:, at * narrow : (at + 1) * narrow]
        squares += jnp.sum(after * after, axis=1, keepdims=True)
    factor = lax.rsqrt(squares / (parts * width) + epsilon)
    for part in range(pieces):
        cols = slice(part * narrow, (part + 1) * narrow)
        normed_ref[part] = (after_ref[part] * factor * gain_ref[:, cols]).astype(normed_ref.dtype)
    row.drain()
    piece.drain()
    block.drain()


def run_front(
    row, piece, block, query_nope, query_rope, cosine, sine_part, resid, gain, routes, route_weight,
    experts, sp_count, dp_count, cores, heads_here, nope, channels, scale, number,
):
    outer, inner = split_of(sp_count)
    lanes = dp_count // cores
    tokens, model = resid.shape
    width = min(model // dp_count, part_width)
    dma = pltpu.SemaphoreType.DMA
    narrow = [
        dma((2, outer)),
        dma((outer,)),
        dma((max(inner - 1, 1), outer)),
        dma((max(inner - 1, 1), outer)),
    ]
    beside = [dma((max(lanes - 1, 1), sp_count))] * 2

    def crossing(count):
        return [dma((max(cores - 1, 1), count, sp_count))] * 2

    vmem = pl.BlockSpec(memory_space=pltpu.VMEM)
    return pl.pallas_call(
        functools.partial(front_kernel, outer, inner, cores, heads_here, nope, channels, scale),
        out_shape=[
            jax.ShapeDtypeStruct((model // width, tokens, width), jnp.float32),
            jax.ShapeDtypeStruct((model // width, tokens, width), jnp.bfloat16),
            jax.ShapeDtypeStruct(
                (outer, 2 * experts // outer + -2 * experts // outer % 8, tokens), jnp.float32
            ),
        ],
        in_specs=[vmem] * 11,
        out_specs=[vmem] * 3,
        scratch_shapes=[
            pltpu.VMEM((sp_count,) + row.shape, row.dtype),
            pltpu.VMEM((cores, sp_count) + piece.shape, piece.dtype),
            pltpu.VMEM((dp_count, sp_count) + block.shape, block.dtype),
            pltpu.VMEM((tokens, model), jnp.bfloat16),
            pltpu.VMEM((sp_count * heads_here, nope + 128, tokens), jnp.bfloat16),
        ]
        + narrow
        + narrow
        + crossing(1)
        + narrow
        + beside
        + crossing(lanes),
        compiler_params=pltpu.CompilerParams(
            collective_id=number, has_side_effects=True, vmem_limit_bytes=40 * 2**20
        ),
        cost_estimate=pl.CostEstimate(flops=2 * 10**10, bytes_accessed=10**7, transcendentals=0),
    )(
        row, piece, block, query_nope, query_rope, cosine, sine_part, resid, gain, routes, route_weight
    )


def split_of(sp_count):
    inner = max(d for d in range(1, math.isqrt(sp_count) + 1) if sp_count % d == 0)
    return sp_count // inner, inner


def plan_tasks(outer, parts, across_z, across_y):
    def forward(at, source):
        return 1 if source < at < outer - 1 else (-1 if 0 < at < source else 0)

    spent = {"A": 0.5, "B": 4.5, "C": 0.6, "F": 0.05, "R": 0.3}
    todo = [
        [("B", s, 0) for s in range(outer)]
        + [(kind, s, p) for s in range(outer) for p in range(parts) for kind in "AC"]
        + [("F", s, p) for s in range(outer) for p in range(parts) if forward(at, s)]
        + [("R", s, p) for s in range(outer) for p in range(parts) if s != at and 0 < at < outer - 1]
        for at in range(outer)
    ]
    free, landed = {}, {}
    clock, done, order = [2.0] * outer, [set() for _ in range(outer)], [[] for _ in range(outer)]

    def send(at, link, target, key, time, length):
        free[at, link] = max(time, free.get((at, link), 0.0)) + length
        landed[target, key] = free[at, link] + link_delay

    def ready(at, task):
        kind, source, part = task
        needed, before = [], []
        wait = 0.0
        if kind in "AF" and source != at:
            needed.append(("block", source, part))
        if kind == "A":
            before += [("F", source, part)] if forward(at, source) else []
            before += [("A", source, part - 1)] if part else []
            wait = free.get((at, "y"), 0.0) - 3.0
        if kind == "F" and part:
            before.append(("F", source, part - 1))
        if kind == "B":
            before += [("A", source, p) for p in range(parts)]
            before += [("B", s, 0) for s in range(outer) if s != at and source == at]
            needed += [("row", source, p) for p in range(parts)]
            wait = free.get((at, "y"), 0.0) - 6.0
        if kind == "C":
            before.append(("B", source, 0))
            needed.append(("back", source, part))
        if kind == "R":
            before.append(("C", source, part))
            needed.append(("sum", source, part))
        if any(task not in done[at] for task in before) or any((at, key) not in landed for key in needed):
            return None
        return max([clock[at], wait] + [landed[at, key] for key in needed])

    def rank(at, task):
        kind, source, part = task
        own = source == at
        return (8 if own and kind == "C" else "FRBCA".index(kind), abs(source - at), part)

    for at in range(outer):
        for part in range(parts):
            for way in (1, -1):
                if 0 <= at + way < outer:
                    send(at, way, at + way, ("block", at, part), 2.0, across_z)
    while any(todo):
        chosen = None
        for at in range(outer):
            times = [(ready(at, task), task) for task in todo[at]]
            times = [(time, task) for time, task in times if time is not None]
            if times:
                first = min(time for time, _ in times)
                task = min((t for time, t in times if time <= first), key=lambda t: rank(at, t))
                if chosen is None or first < chosen[0]:
                    chosen = (first, at, task)
        time, at, task = chosen
        kind, source, part = task
        todo[at].remove(task)
        order[at].append(task)
        done[at].add(task)
        clock[at] = end = time + spent[kind]
        way = -1 if source < at else 1
        if kind == "F":
            send(at, forward(at, source), at + forward(at, source), ("block", source, part), end, across_z)
        if kind == "A":
            send(at, "y", at, ("row", source, part), end, across_y)
        if kind == "B":
            for p in range(parts):
                begun = end - spent["B"] * 0.5 * (parts - 1 - p) / parts
                send(at, "y", at, ("back", source, p), begun, across_y)
        last = at == (outer - 1 if way < 0 else 0)
        if source != at and (kind == "R" or (kind == "C" and last)):
            key = ("last", at + way, part) if way > 0 and source == at + way else ("sum", source, part)
            send(at, way, at + way, key, end, across_z)
    return order


def experts_kernel(
    outer, inner, capacity, order,
    normed_ref, meta_ref, after_ref, gate_hbm, up_hbm, down_hbm, out_ref,
    gate_w, up_w, down_w, blocks, metas, picked, rows, made, back, partial, coming, total, gate_acc, up_acc,
    select, columns, spread,
    weight_sems, meta_send, meta_recv, block_send, block_recv, row_send, row_recv,
    back_send, back_recv, sum_send, sum_recv,
):
    me = lax.axis_index("sp")
    z, y = me // inner, lax.rem(me, inner)
    parts, tokens, width = normed_ref.shape
    loads = [
        pltpu.make_async_copy(hbm.at[0], ref, weight_sems.at[at])
        for at, (hbm, ref) in enumerate([(gate_hbm, gate_w), (up_hbm, up_w), (down_hbm, down_w)])
    ]
    for load in loads:
        load.start()

    barrier = pltpu.get_barrier_semaphore()
    steps_z = [lax.rem(z + step, outer) for step in range(1, outer)]
    steps_y = [lax.rem(y + step, inner) for step in range(1, inner)]
    greeted = [{"sp": at * inner + y} for at in steps_z] + [{"sp": z * inner + at} for at in steps_y]
    for peer in greeted:
        pl.semaphore_signal(barrier, inc=1, device_id=peer, device_id_type=pl.DeviceIdType.MESH)
    pl.semaphore_wait(barrier, len(greeted))

    def remote(source, target, send, recv, at_z, at_y):
        return pltpu.make_async_remote_copy(
            src_ref=source, dst_ref=target, send_sem=send, recv_sem=recv,
            device_id={"sp": at_z * inner + at_y}, device_id_type=pl.DeviceIdType.MESH,
        )

    def block_copy(source, part, own, way):
        ref = normed_ref.at[part] if own else blocks.at[source, part]
        return remote(
            ref, blocks.at[source, part],
            block_send.at[(way + 1) // 2, source, part], block_recv.at[source, part], z + way, y,
        )

    def meta_copy(step):
        at = lax.rem(z + step, outer)
        return remote(meta_ref.at[at], metas.at[z], meta_send.at[step - 1], meta_recv.at[z], at, y)

    def row_copy(source, step, part):
        at = lax.rem(y + step, inner)
        return remote(
            picked.at[source, at, part], rows.at[source, y, part],
            row_send.at[source, step - 1, part], row_recv.at[source, y, part], z, at,
        )

    def back_copy(source, step, part):
        at = lax.rem(y + step, inner)
        return remote(
            made.at[source, at, part], back.at[source, y, part],
            back_send.at[source, step - 1, part], back_recv.at[source, y, part], z, at,
        )

    def sum_copy(source, part, way):
        slot = source if way < 0 else jnp.where(source == z + 1, outer, source)
        return remote(
            partial.at[source, part], coming.at[slot, part],
            sum_send.at[source, part], sum_recv.at[slot, part], z + way, y,
        )

    def wait_recv(ref, sem):
        remote(ref, ref, block_send.at[0, 0, 0], sem, z, y).wait_recv()

    for step in range(1, outer):
        meta_copy(step).start()
    for part in range(parts):
        for way in (1, -1):

            @pl.when((z + way >= 0) & (z + way < outer))
            def _():
                block_copy(z, part, True, way).start()

    blocks[z] = normed_ref[...]
    metas[z] = meta_ref[z]

    kinds = "ABCFRW"
    steps = max(len(row) for row in order) + 1

    def coded(row):
        first = [kind for kind, _, _ in row].index("B")
        row = row[:first] + [("W", 0, 0)] + row[first:]
        codes = [(kinds.index(kind) * outer + source) * parts + part for kind, source, part in row]
        return codes + [len(kinds) * outer * parts] * (steps - len(codes))

    base = (len(kinds) + 1) * outer * parts
    rows_coded = [coded(row) for row in order]
    words = []
    for start in range(0, steps, 3):
        value = None
        for at in range(outer):
            word = sum(code * base**index for index, code in enumerate(rows_coded[at][start : start + 3]))
            value = jnp.int32(word) if value is None else jnp.where(z == at, word, value)
        words.append(value)

    def task_of(step):
        index, digit = step // 3, lax.rem(step, 3)
        level = words
        while len(level) > 1:
            even = lax.rem(index, 2) == 0
            level = [
                jnp.where(even, level[at], level[at + 1]) if at + 1 < len(level) else level[at]
                for at in range(0, len(level), 2)
            ]
            index = index // 2
        word = level[0]
        code = jnp.where(digit == 0, word, jnp.where(digit == 1, word // base, word // base**2))
        code = lax.rem(code, base)
        return code // (outer * parts), lax.rem(code // parts, outer), lax.rem(code, parts)

    def forwards(source):
        return [
            (1, (source < z) & (z < outer - 1)),
            (-1, (source > z) & (z > 0)),
        ]

    def ends(source):
        return [
            (-1, (source < z) & (z == outer - 1)),
            (1, (source > z) & (z == 0)),
        ]

    def needs(source):
        return functools.reduce(jnp.logical_or, [needed for _, needed in forwards(source)])

    def arrive(source, part):
        wait_recv(blocks.at[source, part], block_recv.at[source, part])

    def pick(source, part):
        @pl.when((source != z) & (part == 0))
        def _():
            wait_recv(metas.at[source], meta_recv.at[source])

        @pl.when(part == 0)
        def _():
            slot_ids = lax.broadcasted_iota(jnp.int32, (capacity, tokens), 0).astype(jnp.float32)
            for at in range(inner):
                select[source, at * capacity : (at + 1) * capacity] = jnp.where(
                    metas[source, at : at + 1, :] == slot_ids, 1.0, 0.0
                ).astype(jnp.bfloat16)

        @pl.when((source != z) & ~needs(source))
        def _():
            arrive(source, part)

        found = jnp.dot(
            select[source], blocks[source, part], preferred_element_type=jnp.float32
        ).astype(jnp.bfloat16)
        for at in range(inner):
            picked[source, at, part] = found[at * capacity : (at + 1) * capacity]
        rows[source, y, part] = picked[source, y, part]
        for step in range(1, inner):
            row_copy(source, step, part).start()

    def apply_experts(source):
        gate_acc[...] = jnp.zeros_like(gate_acc)
        up_acc[...] = jnp.zeros_like(up_acc)

        def widen(pair, carry):
            for part in (2 * pair, 2 * pair + 1):
                for step in range(1, inner):
                    at = lax.rem(y + step, inner)
                    wait_recv(rows.at[source, at, part], row_recv.at[source, at, part])
            taken = jnp.concatenate(
                [
                    jnp.concatenate([rows[source, at, 2 * pair + half] for half in range(2)], axis=1)
                    for at in range(inner)
                ],
                axis=0,
            )
            depth = pl.ds(pl.multiple_of(pair * 2 * width, 2 * width), 2 * width)
            gate_acc[...] += jnp.dot(taken, gate_w[depth, :], preferred_element_type=jnp.float32)
            up_acc[...] += jnp.dot(taken, up_w[depth, :], preferred_element_type=jnp.float32)
            return carry

        lax.fori_loop(0, parts // 2, widen, 0)
        gate = gate_acc[...]
        hidden = (gate / (1.0 + jnp.exp(-gate)) * up_acc[...]).astype(jnp.bfloat16)

        for part in range(parts):
            cols = slice(part * width, (part + 1) * width)
            result = jnp.dot(hidden, down_w[:, cols], preferred_element_type=jnp.float32).astype(
                jnp.bfloat16
            )
            for at in range(inner):
                made[source, at, part] = result[at * capacity : (at + 1) * capacity]
            back[source, y, part] = made[source, y, part]
            for step in range(1, inner):
                back_copy(source, step, part).start()

        columns[source] = jnp.transpose(metas[source])
        slot_lanes = lax.broadcasted_iota(jnp.int32, (tokens, capacity), 1).astype(jnp.float32)
        for at in range(inner):
            spread[source, at] = jnp.where(
                columns[source, :, at : at + 1] == slot_lanes, 1.0, 0.0
            ).astype(jnp.bfloat16)

    def combine(source, part):
        for step in range(1, inner):
            at = lax.rem(y + step, inner)
            wait_recv(back.at[source, at, part], back_recv.at[source, at, part])
        summed = sum(
            jnp.dot(spread[source, at], back[source, at, part], preferred_element_type=jnp.float32)
            * columns[source, :, inner + at : inner + at + 1]
            for at in range(inner)
        )

        @pl.when(source == z)
        def _():
            total[part] = after_ref[part] + summed

        @pl.when(source != z)
        def _():
            partial[source, part] = summed.astype(jnp.bfloat16)

        for way, needed in ends(source):

            @pl.when(needed)
            def _():
                sum_copy(source, part, way).start()

    def relay(source, part):
        wait_recv(coming.at[source, part], sum_recv.at[source, part])
        partial[source, part] = (
            partial[source, part].astype(jnp.float32) + coming[source, part].astype(jnp.float32)
        ).astype(jnp.bfloat16)
        for way in (1, -1):

            @pl.when((source > z) if way > 0 else (source < z))
            def _():
                sum_copy(source, part, way).start()

    def run_task(step, carry):
        kind, source, part = task_of(step)

        @pl.when(kind == 0)
        def _():
            pick(source, part)

        @pl.when(kind == 1)
        def _():
            apply_experts(source)

        @pl.when(kind == 2)
        def _():
            combine(source, part)

        @pl.when(kind == 3)
        def _():
            arrive(source, part)
            for way, needed in forwards(source):

                @pl.when(needed)
                def _():
                    block_copy(source, part, False, way).start()

        @pl.when(kind == 4)
        def _():
            relay(source, part)

        @pl.when(kind == 5)
        def _():
            for load in loads:
                load.wait()

        return carry

    lax.fori_loop(0, steps, run_task, 0)

    for part in range(parts):
        for slot, valid in ((z, z < outer - 1), (outer, z > 0)):

            @pl.when(valid)
            def _():
                wait_recv(coming.at[slot, part], sum_recv.at[slot, part])
                total[part] += coming[slot, part].astype(jnp.float32)

        out_ref[:, part * width : (part + 1) * width] = total[part].astype(out_ref.dtype)

    for step in range(1, outer):
        meta_copy(step).wait_send()
    def drain(source, carry):
        for part in range(parts):
            for way in (1, -1):
                onward = (z + way >= 0) & (z + way < outer)
                passing = (source == z) | ((source < z) if way > 0 else (source > z))

                @pl.when(onward & passing)
                def _():
                    block_copy(source, part, False, way).wait_send()

                @pl.when(onward & ((source > z) if way > 0 else (source < z)))
                def _():
                    sum_copy(source, part, way).wait_send()

            for step in range(1, inner):
                row_copy(source, step, part).wait_send()
                back_copy(source, step, part).wait_send()
        return carry

    lax.fori_loop(0, outer, drain, 0)


def run_experts(normed, meta, after, gate, up, down, sp_count, capacity, number):
    outer, inner = split_of(sp_count)
    parts, tokens, width = normed.shape
    model, hidden = gate.shape[1:]
    across_z = tokens * width * 2 / link_rate
    order = plan_tasks(outer, parts, across_z, across_z * capacity / tokens)
    dma = pltpu.SemaphoreType.DMA
    bf16, f32 = jnp.bfloat16, jnp.float32
    steps_y = max(inner - 1, 1)
    vmem = pl.BlockSpec(memory_space=pltpu.VMEM)
    anywhere = pl.BlockSpec(memory_space=pl.ANY)
    held = [
        pltpu.VMEM((model, hidden), bf16),
        pltpu.VMEM((model, hidden), bf16),
        pltpu.VMEM((hidden, model), bf16),
        pltpu.VMEM((outer, parts, tokens, width), bf16),
        pltpu.VMEM((outer,) + meta.shape[1:], f32),
        pltpu.VMEM((outer, inner, parts, capacity, width), bf16),
        pltpu.VMEM((outer, inner, parts, capacity, width), bf16),
        pltpu.VMEM((outer, inner, parts, capacity, width), bf16),
        pltpu.VMEM((outer, inner, parts, capacity, width), bf16),
        pltpu.VMEM((outer, parts, tokens, width), bf16),
        pltpu.VMEM((outer + 1, parts, tokens, width), bf16),
        pltpu.VMEM((parts, tokens, width), f32),
        pltpu.VMEM((inner * capacity, hidden), f32),
        pltpu.VMEM((inner * capacity, hidden), f32),
        pltpu.VMEM((outer, inner * capacity, tokens), bf16),
        pltpu.VMEM((outer, tokens, meta.shape[1]), f32),
        pltpu.VMEM((outer, inner, tokens, capacity), bf16),
    ]
    grant = sum(
        math.prod(s.shape[:-1]) * -(-s.shape[-1] // 128) * 128 * s.dtype.itemsize for s in held
    )
    return pl.pallas_call(
        functools.partial(experts_kernel, outer, inner, capacity, order),
        out_shape=jax.ShapeDtypeStruct((tokens, parts * width), bf16),
        in_specs=[vmem, vmem, vmem, anywhere, anywhere, anywhere],
        out_specs=vmem,
        scratch_shapes=held
        + [
            dma((3,)),
            dma((outer,)),
            dma((outer,)),
            dma((2, outer, parts)),
            dma((outer, parts)),
            dma((outer, steps_y, parts)),
            dma((outer, inner, parts)),
            dma((outer, steps_y, parts)),
            dma((outer, inner, parts)),
            dma((outer, parts)),
            dma((outer + 1, parts)),
        ],
        compiler_params=pltpu.CompilerParams(
            collective_id=number, has_side_effects=True, vmem_limit_bytes=grant + extra_vmem
        ),
        cost_estimate=pl.CostEstimate(
            flops=6 * sp_count * capacity * model * hidden, bytes_accessed=10**7, transcendentals=0
        ),
    )(normed, meta, after, gate, up, down)


def shards(
    query_nope,
    query_rope,
    latent,
    key_rope,
    resid,
    latent_gain,
    key_up,
    value_up,
    out_proj,
    norm_gain,
    expert_gate,
    expert_up,
    expert_down,
    routes,
    route_weight,
):
    tokens, channels = latent.shape[1:]
    sp_count = lax.axis_size("sp")
    dp_count = lax.axis_size("dp")
    me = lax.axis_index("sp")
    nope, rope = query_nope.shape[-1], query_rope.shape[-1]
    heads_here = key_up.shape[1] // nope
    scale = (nope + rope) ** (-0.5)
    local_pos = me * tokens + jnp.arange(tokens, dtype=jnp.int32)
    latent_normed = rms_scaled(latent[0], latent_gain).astype(jnp.bfloat16)
    key_turned = rotate(key_rope[0], local_pos)
    spare = 128 - rope
    row = jnp.concatenate(
        [latent_normed, key_turned, jnp.zeros((tokens, spare), jnp.bfloat16)], axis=1
    )
    cores = 2 if dp_count % 2 == 0 else 1
    piece = channels // cores
    ups = lax.dynamic_slice_in_dim(
        jnp.concatenate([key_up, value_up], axis=1),
        lax.rem(lax.axis_index("dp"), cores) * piece, piece, axis=0,
    )
    frequency = rope_base ** (-jnp.arange(rope // 2, dtype=jnp.float32) / (rope // 2))
    angles = frequency[:, None] * local_pos.astype(jnp.float32)[None, :]
    experts_all = sp_count * expert_gate.shape[0]
    capacity = 4 * tokens // experts_all
    after, normed, meta = run_front(
        row, ups, out_proj, query_nope[0].reshape(tokens, -1), query_rope[0].reshape(tokens, -1),
        jnp.cos(angles), jnp.sin(angles), resid[0], norm_gain[None], routes[0].T, route_weight[0].T,
        experts_all, sp_count, dp_count, cores, heads_here, nope, channels, scale, 0,
    )
    mixed = run_experts(
        normed, meta, after, expert_gate, expert_up, expert_down, sp_count, capacity, 1
    )
    return mixed[None]


def solution(mesh):
    return jax.shard_map(
        shards,
        mesh=mesh,
        in_specs=(
            P("dp", "sp", None, None),
            P("dp", "sp", None, None),
            P("dp", "sp", None),
            P("dp", "sp", None),
            P("dp", "sp", None),
            P(),
            P(None, "sp"),
            P(None, "sp"),
            P("sp", "dp"),
            P(),
            P("sp", None, None),
            P("sp", None, None),
            P("sp", None, None),
            P("dp", "sp", None),
            P("dp", "sp", None),
        ),
        out_specs=P("dp", "sp", None),
        check_vma=False,
    )
```

```python
import functools
import math

import jax
import jax.numpy as jnp
from jax import lax
from jax.experimental import pallas as pl
from jax.experimental.pallas import tpu as pltpu
from jax.sharding import PartitionSpec as P

epsilon = 1e-06
rope_base = 10000.0
masked_score = -1e30
log2_e = 1.4426950408889634
part_width = 256
extra_vmem = 3 * 2**19
link_rate = 46.6e3
link_delay = 2.2


def rotate(values, positions):
    half_width = values.shape[-1] // 2
    frequency = rope_base ** (-jnp.arange(half_width, dtype=jnp.float32) / half_width)
    angles = positions.astype(jnp.float32)[:, None] * frequency[None, :]
    cosine = jnp.cos(angles)
    sine_part = jnp.sin(angles)
    if values.ndim == 3:
        cosine = cosine[:, None, :]
        sine_part = sine_part[:, None, :]
    floats = values.astype(jnp.float32)
    first_half = floats[..., :half_width]
    second_half = floats[..., half_width:]
    turned = jnp.concatenate(
        [
            first_half * cosine - second_half * sine_part,
            second_half * cosine + first_half * sine_part,
        ],
        axis=-1,
    )
    return turned.astype(jnp.bfloat16)


def rms_scaled(values, gain):
    floats = values.astype(jnp.float32)
    return floats * lax.rsqrt(jnp.mean(floats * floats, axis=-1, keepdims=True) + epsilon) * gain


def front_kernel(
    outer, inner, cores, heads_here, nope, channels, scale,
    row_ref, piece_ref, block_ref, nope_ref, rope_ref, cosine_ref, sine_ref, resid_ref, gain_ref,
    routes_ref, route_weight_ref, after_ref, normed_ref, meta_ref, shared, ups, weights, heads, queries, *sems,
):
    me, dp = lax.axis_index("sp"), lax.axis_index("dp")
    z, y = me // inner, lax.rem(me, inner)
    lanes = weights.shape[0] // cores
    x, core = dp // cores, lax.rem(dp, cores)
    groups, tokens = shared.shape[0], shared.shape[1]
    columns = heads_here * nope
    total = groups * columns
    row_sems, piece_sems, block_sems = sems[0:4], sems[4:10], sems[10:18]

    def remote(source, target, send, recv, peer):
        return pltpu.make_async_remote_copy(
            src_ref=source, dst_ref=target, send_sem=send, recv_sem=recv,
            device_id=peer, device_id_type=pl.DeviceIdType.MESH,
        )

    def at_z(step):
        return {"sp": lax.rem(z + step, outer) * inner + y}

    def at_y(step):
        return {"sp": z * inner + lax.rem(y + step, inner)}

    def at_x(step):
        return {"dp": lax.rem(x + step, lanes) * cores + core}

    def at_core(step):
        return {"dp": x * cores + lax.rem(core + step, cores)}

    barrier = pltpu.get_barrier_semaphore()
    greeted = (
        [at_y(step) for step in range(1, inner)]
        + [at_x(step) for step in range(1, lanes)]
        + [at_core(step) for step in range(1, cores)]
    )
    below, above = z > 0, z < outer - 1
    for peer in greeted:
        pl.semaphore_signal(barrier, inc=1, device_id=peer, device_id_type=pl.DeviceIdType.MESH)
    for way, there in ((-1, below), (1, above)):

        @pl.when(there)
        def _():
            pl.semaphore_signal(
                barrier, inc=1, device_id=at_z(way), device_id_type=pl.DeviceIdType.MESH
            )

    pl.semaphore_wait(barrier, len(greeted) + jnp.where(below & above, 2, 1 if outer > 1 else 0))

    orders = [sorted(range(outer), key=lambda s: (abs(s - at), s)) for at in range(outer)]

    def source_of(turn):
        found = z
        for index in range(1, outer):
            value = jnp.int32(orders[0][index])
            for at in range(1, outer):
                value = jnp.where(z == at, orders[at][index], value)
            found = jnp.where(turn == index, value, found)
        return found

    def member(index):
        return source_of(lax.rem(index, outer)) * inner + lax.rem(y + index // outer, inner)

    class Spread:
        def __init__(self, own, held, sems, lanes, row):
            self.own, self.held, self.sems, self.lanes, self.row = own, held, sems, lanes, row

        def place(self, block, lane=0, at_core=None):
            if self.row is None:
                return self.held.at[block]
            return self.held.at[self.row(lane, core if at_core is None else at_core), block]

        def source(self, index, lane=0):
            own = isinstance(index, int) and index == 0 and isinstance(lane, int) and lane == 0
            return self.own if own else self.place(member(index), lane)

        def along_z(self, turn, way):
            block, at = member(turn), source_of(turn)
            return remote(
                self.source(turn), self.place(block),
                self.sems[0].at[(way + 1) // 2, at], self.sems[1].at[at], at_z(way),
            )

        def along_y(self, step, turn):
            return remote(
                self.source(turn), self.place(member(turn)),
                self.sems[2].at[step - 1, turn], self.sems[3].at[step - 1, turn], at_y(step),
            )

        def along_x(self, step, index):
            return remote(
                self.source(index), self.place(member(index)),
                self.sems[4].at[step - 1, index], self.sems[5].at[step - 1, index], at_x(step),
            )

        def across(self, step, lane, index):
            return remote(
                self.source(index, lane), self.place(member(index), lane),
                self.sems[-2].at[step - 1, lane, index], self.sems[-1].at[step - 1, lane, index], at_core(step),
            )

        def wait(self, ref, sem):
            remote(ref, ref, self.sems[0].at[0, 0], sem, at_core(0)).wait_recv()

        def start_z(self, turn):
            at = source_of(turn)
            for way, there in ((-1, below & (at >= z)), (1, above & (at <= z))):

                @pl.when(there)
                def _():
                    self.along_z(turn, way).start()

        def start_y(self, turn):
            for step in range(1, inner):
                self.along_y(step, turn).start()

        def start_wide(self, index):
            if self.row is None:
                return
            for step in range(1, self.lanes):
                self.along_x(step, index).start()
            for step in range(1, cores):
                self.across(step, 0, index).start()

        def reach_z(self, turn):
            self.wait(self.place(member(turn)), self.sems[1].at[source_of(turn)])
            self.start_z(turn)
            self.start_wide(turn)

        def from_z(self, turn):
            self.reach_z(turn)
            self.start_y(turn)

        def from_y(self, index):
            step = inner - index // outer
            self.wait(self.place(member(index)), self.sems[3].at[step - 1, lax.rem(index, outer)])
            self.start_wide(index)

        def from_x(self, lane, index):
            self.wait(self.place(member(index), lane), self.sems[5].at[self.lanes - lane - 1, index])
            for step in range(1, cores):
                self.across(step, lane, index).start()

        def settle(self):
            def one(index, carry):
                for lane in range(self.lanes):
                    for step in range(1, cores):
                        self.wait(
                            self.place(member(index), lane, lax.rem(core + step, cores)),
                            self.sems[-1].at[cores - step - 1, lane, index],
                        )
                return carry

            lax.fori_loop(0, groups, one, 0)

        def drain(self):
            for turn in range(outer):
                at = source_of(turn)
                for way, there in ((-1, below & (at >= z)), (1, above & (at <= z))):

                    @pl.when(there)
                    def _():
                        self.along_z(turn, way).wait_send()

                for step in range(1, inner):
                    self.along_y(step, turn).wait_send()
            if self.row is None:
                return

            def one(index, carry):
                for step in range(1, self.lanes):
                    self.along_x(step, index).wait_send()
                for step in range(1, cores):
                    for lane in range(self.lanes):
                        self.across(step, lane, index).wait_send()
                return carry

            lax.fori_loop(0, groups, one, 0)

    row = Spread(row_ref, shared, row_sems, 1, None)
    piece = Spread(piece_ref, ups, piece_sems, 1, lambda lane, at: at)
    block = Spread(
        block_ref, weights, block_sems, lanes, lambda lane, at: lax.rem(x + lane, lanes) * cores + at
    )
    for spread in (row, piece):
        spread.start_z(0)
        spread.start_y(0)
        spread.start_wide(0)
    block.start_z(0)
    block.start_y(0)
    block.start_wide(0)
    shared[me] = row_ref[...]
    ups[core, me] = piece_ref[...]
    weights[dp, me] = block_ref[...]

    rope = cosine_ref.shape[0]
    for pair in range(queries.shape[0] // 2):
        both = jnp.transpose(rope_ref[:, pair * 4 * rope : (pair + 1) * 4 * rope].astype(jnp.float32))
        for half in range(2):
            head = 2 * pair + half
            first = both[half * 2 * rope : half * 2 * rope + rope]
            second = both[half * 2 * rope + rope : (half + 1) * 2 * rope]
            cosine, sine_part = cosine_ref[...], sine_ref[...]
            queries[head, nope : nope + 2 * rope] = jnp.concatenate(
                [first * cosine - second * sine_part, second * cosine + first * sine_part], axis=0
            ).astype(queries.dtype)
            queries[head, nope + 2 * rope :] = jnp.zeros(
                (queries.shape[1] - nope - 2 * rope, tokens), queries.dtype
            )
            queries[head, 0:nope] = jnp.transpose(
                nope_ref[:, head * nope : (head + 1) * nope].astype(jnp.float32)
            ).astype(queries.dtype)

    experts = meta_ref.shape[0] * inner
    ids = lax.broadcasted_iota(jnp.int32, (experts, tokens), 0)
    mine = [routes_ref[at : at + 1, :] == ids for at in range(routes_ref.shape[0])]
    named = functools.reduce(jnp.logical_or, mine)
    weight = sum(
        jnp.where(chosen, route_weight_ref[at : at + 1, :], 0.0) for at, chosen in enumerate(mine)
    )
    earlier = lax.broadcasted_iota(jnp.int32, (tokens, tokens), 0)
    upto = jnp.where(earlier < lax.broadcasted_iota(jnp.int32, (tokens, tokens), 1), 1.0, 0.0)
    place = jnp.dot(
        jnp.where(named, 1.0, 0.0).astype(jnp.bfloat16), upto.astype(jnp.bfloat16),
        preferred_element_type=jnp.float32,
    )
    slot = jnp.where(named, place, -1.0)
    meta_ref[...] = jnp.zeros_like(meta_ref)
    for at in range(meta_ref.shape[0]):
        meta_ref[at, 0:inner] = slot[at * inner : (at + 1) * inner]
        meta_ref[at, inner : 2 * inner] = weight[at * inner : (at + 1) * inner]

    for turn in range(1, outer - 1):
        row.from_z(turn)
        piece.from_z(turn)
    block.reach_z(1)
    block.from_y(outer)
    row.from_z(outer - 1)
    piece.from_z(outer - 1)
    block.start_y(1)
    for turn in range(2, outer - 1):
        block.from_z(turn)
    for index in range(outer, groups):
        row.from_y(index)
        piece.from_y(index)
    piece.settle()

    span = 2 * tokens if groups % 2 == 0 else tokens
    chunks = span // tokens
    ending = me // chunks
    key_ids = lax.broadcasted_iota(jnp.int32, (span, tokens), 0)
    query_ids = lax.broadcasted_iota(jnp.int32, (span, tokens), 1)
    allowed = key_ids <= query_ids + lax.rem(me, chunks) * tokens

    def attend_group(group):
        up = ups[:, group].reshape(channels, 2 * columns)
        up_keys = up[:, 0:columns]
        up_values = up[:, columns : 2 * columns]
        up_values_t = jnp.transpose(up_values.astype(jnp.float32)).astype(jnp.bfloat16)

        def scores_of(place):
            taken = shared[pl.ds(place * chunks, chunks)].reshape(span, shared.shape[2])
            latent = taken[:, 0:channels]
            turned = taken[:, channels:]
            keys = jnp.dot(latent, up_keys, preferred_element_type=jnp.float32).astype(jnp.bfloat16)
            values_t = lax.dot_general(
                up_values_t, latent, (((1,), (1,)), ((), ())), preferred_element_type=jnp.float32
            ).astype(jnp.bfloat16)
            scores = []
            for head in range(heads_here):
                full = jnp.concatenate([keys[:, head * nope : (head + 1) * nope], turned], axis=1)
                scores.append(
                    jnp.dot(
                        full, queries[group * heads_here + head], preferred_element_type=jnp.float32
                    )
                    * (scale * log2_e)
                )
            return scores, [values_t[h * nope : (h + 1) * nope, :] for h in range(heads_here)]

        scores, values = scores_of(ending)
        state = []
        for score, value in zip(scores, values):
            score = jnp.where(allowed, score, masked_score)
            largest = jnp.max(score, axis=0, keepdims=True)
            powers = jnp.exp2(score - largest)
            state.append(
                (
                    largest,
                    jnp.sum(powers, axis=0, keepdims=True),
                    jnp.dot(value, powers.astype(jnp.bfloat16), preferred_element_type=jnp.float32),
                )
            )

        def step(place, state):
            scores, values = scores_of(place)
            after = []
            for (largest, total, kept), score, value in zip(state, scores, values):
                now = jnp.maximum(largest, jnp.max(score, axis=0, keepdims=True))
                fade = jnp.exp2(largest - now)
                powers = jnp.exp2(score - now)
                after.append(
                    (
                        now,
                        total * fade + jnp.sum(powers, axis=0, keepdims=True),
                        kept * fade
                        + jnp.dot(
                            value, powers.astype(jnp.bfloat16), preferred_element_type=jnp.float32
                        ),
                    )
                )
            return tuple(after)

        state = lax.fori_loop(0, ending, step, tuple(state))
        for head, (_, total, kept) in enumerate(state):
            start = pl.multiple_of(group * columns + head * nope, nope)
            heads[:, pl.ds(start, nope)] = jnp.transpose(kept / total).astype(heads.dtype)

    def one_group(group, carry):
        attend_group(group)

        @pl.when(group == 0)
        def _():
            block.from_z(outer - 1)

        nearby = group + outer

        @pl.when((group > 0) & (nearby < groups))
        def _():
            block.from_y(nearby)

        @pl.when(group >= 1)
        def _():
            for lane in range(1, lanes):
                block.from_x(lane, group - 1)

        return carry

    lax.fori_loop(0, groups, one_group, 0)
    for lane in range(1, lanes):
        block.from_x(lane, groups - 1)
    block.settle()

    parts, width = weights.shape[0], weights.shape[3]
    pieces, narrow = normed_ref.shape[0], normed_ref.shape[2]
    squares = jnp.zeros((tokens, 1), jnp.float32)
    for part in range(parts):
        projected = (
            jnp.dot(
                heads[...], weights[part].reshape(total, width), preferred_element_type=jnp.float32
            )
            .astype(jnp.bfloat16)
            .astype(jnp.float32)
        )
        cols = slice(part * width, (part + 1) * width)
        after = resid_ref[:, cols].astype(jnp.float32) + projected
        each = width // narrow
        for at in range(each):
            after_ref[part * each + at] = after[:, at * narrow : (at + 1) * narrow]
        squares += jnp.sum(after * after, axis=1, keepdims=True)
    factor = lax.rsqrt(squares / (parts * width) + epsilon)
    for part in range(pieces):
        cols = slice(part * narrow, (part + 1) * narrow)
        normed_ref[part] = (after_ref[part] * factor * gain_ref[:, cols]).astype(normed_ref.dtype)
    row.drain()
    piece.drain()
    block.drain()


def run_front(
    row, piece, block, query_nope, query_rope, cosine, sine_part, resid, gain, routes, route_weight,
    experts, sp_count, dp_count, cores, heads_here, nope, channels, scale, number,
):
    outer, inner = split_of(sp_count)
    lanes = dp_count // cores
    tokens, model = resid.shape
    width = min(model // dp_count, part_width)
    dma = pltpu.SemaphoreType.DMA
    narrow = [
        dma((2, outer)),
        dma((outer,)),
        dma((max(inner - 1, 1), outer)),
        dma((max(inner - 1, 1), outer)),
    ]
    beside = [dma((max(lanes - 1, 1), sp_count))] * 2

    def crossing(count):
        return [dma((max(cores - 1, 1), count, sp_count))] * 2

    vmem = pl.BlockSpec(memory_space=pltpu.VMEM)
    return pl.pallas_call(
        functools.partial(front_kernel, outer, inner, cores, heads_here, nope, channels, scale),
        out_shape=[
            jax.ShapeDtypeStruct((model // width, tokens, width), jnp.float32),
            jax.ShapeDtypeStruct((model // width, tokens, width), jnp.bfloat16),
            jax.ShapeDtypeStruct(
                (outer, 2 * experts // outer + -2 * experts // outer % 8, tokens), jnp.float32
            ),
        ],
        in_specs=[vmem] * 11,
        out_specs=[vmem] * 3,
        scratch_shapes=[
            pltpu.VMEM((sp_count,) + row.shape, row.dtype),
            pltpu.VMEM((cores, sp_count) + piece.shape, piece.dtype),
            pltpu.VMEM((dp_count, sp_count) + block.shape, block.dtype),
            pltpu.VMEM((tokens, model), jnp.bfloat16),
            pltpu.VMEM((sp_count * heads_here, nope + 128, tokens), jnp.bfloat16),
        ]
        + narrow
        + narrow
        + crossing(1)
        + narrow
        + beside
        + crossing(lanes),
        compiler_params=pltpu.CompilerParams(
            collective_id=number, has_side_effects=True, vmem_limit_bytes=40 * 2**20
        ),
        cost_estimate=pl.CostEstimate(flops=2 * 10**10, bytes_accessed=10**7, transcendentals=0),
    )(
        row, piece, block, query_nope, query_rope, cosine, sine_part, resid, gain, routes, route_weight
    )


def split_of(sp_count):
    inner = max(d for d in range(1, math.isqrt(sp_count) + 1) if sp_count % d == 0)
    return sp_count // inner, inner


def plan_tasks(outer, parts, across_z, across_y):
    def forward(at, source):
        return 1 if source < at < outer - 1 else (-1 if 0 < at < source else 0)

    spent = {"A": 0.5, "B": 4.5, "C": 0.6, "F": 0.05, "R": 0.3}
    todo = [
        [("B", s, 0) for s in range(outer)]
        + [(kind, s, p) for s in range(outer) for p in range(parts) for kind in "AC"]
        + [("F", s, p) for s in range(outer) for p in range(parts) if forward(at, s)]
        + [("R", s, p) for s in range(outer) for p in range(parts) if s != at and 0 < at < outer - 1]
        for at in range(outer)
    ]
    free, landed = {}, {}
    clock, done, order = [2.0] * outer, [set() for _ in range(outer)], [[] for _ in range(outer)]

    def send(at, link, target, key, time, length):
        free[at, link] = max(time, free.get((at, link), 0.0)) + length
        landed[target, key] = free[at, link] + link_delay

    def ready(at, task):
        kind, source, part = task
        needed, before = [], []
        wait = 0.0
        if kind in "AF" and source != at:
            needed.append(("block", source, part))
        if kind == "A":
            before += [("F", source, part)] if forward(at, source) else []
            before += [("A", source, part - 1)] if part else []
            wait = free.get((at, "y"), 0.0) - 3.0
        if kind == "F" and part:
            before.append(("F", source, part - 1))
        if kind == "B":
            before += [("A", source, p) for p in range(parts)]
            before += [("B", s, 0) for s in range(outer) if s != at and source == at]
            needed += [("row", source, p) for p in range(parts)]
            wait = free.get((at, "y"), 0.0) - 6.0
        if kind == "C":
            before.append(("B", source, 0))
            needed.append(("back", source, part))
        if kind == "R":
            before.append(("C", source, part))
            needed.append(("sum", source, part))
        if any(task not in done[at] for task in before) or any((at, key) not in landed for key in needed):
            return None
        return max([clock[at], wait] + [landed[at, key] for key in needed])

    def rank(at, task):
        kind, source, part = task
        own = source == at
        return (8 if own and kind == "C" else "FRBCA".index(kind), abs(source - at), part)

    for at in range(outer):
        for part in range(parts):
            for way in (1, -1):
                if 0 <= at + way < outer:
                    send(at, way, at + way, ("block", at, part), 2.0, across_z)
    while any(todo):
        chosen = None
        for at in range(outer):
            times = [(ready(at, task), task) for task in todo[at]]
            times = [(time, task) for time, task in times if time is not None]
            if times:
                first = min(time for time, _ in times)
                task = min((t for time, t in times if time <= first), key=lambda t: rank(at, t))
                if chosen is None or first < chosen[0]:
                    chosen = (first, at, task)
        time, at, task = chosen
        kind, source, part = task
        todo[at].remove(task)
        order[at].append(task)
        done[at].add(task)
        clock[at] = end = time + spent[kind]
        way = -1 if source < at else 1
        if kind == "F":
            send(at, forward(at, source), at + forward(at, source), ("block", source, part), end, across_z)
        if kind == "A":
            send(at, "y", at, ("row", source, part), end, across_y)
        if kind == "B":
            for p in range(parts):
                begun = end - spent["B"] * 0.5 * (parts - 1 - p) / parts
                send(at, "y", at, ("back", source, p), begun, across_y)
        last = at == (outer - 1 if way < 0 else 0)
        if source != at and (kind == "R" or (kind == "C" and last)):
            key = ("last", at + way, part) if way > 0 and source == at + way else ("sum", source, part)
            send(at, way, at + way, key, end, across_z)
    return order


def experts_kernel(
    outer, inner, capacity, order,
    normed_ref, meta_ref, after_ref, gate_hbm, up_hbm, down_hbm, out_ref,
    gate_w, up_w, down_w, blocks, metas, picked, rows, made, back, partial, coming, total, gate_acc, up_acc,
    select, columns, spread,
    weight_sems, meta_send, meta_recv, block_send, block_recv, row_send, row_recv,
    back_send, back_recv, sum_send, sum_recv,
):
    me = lax.axis_index("sp")
    z, y = me // inner, lax.rem(me, inner)
    parts, tokens, width = normed_ref.shape
    loads = [
        pltpu.make_async_copy(hbm.at[0], ref, weight_sems.at[at])
        for at, (hbm, ref) in enumerate([(gate_hbm, gate_w), (up_hbm, up_w), (down_hbm, down_w)])
    ]
    for load in loads:
        load.start()

    barrier = pltpu.get_barrier_semaphore()
    steps_z = [lax.rem(z + step, outer) for step in range(1, outer)]
    steps_y = [lax.rem(y + step, inner) for step in range(1, inner)]
    greeted = [{"sp": at * inner + y} for at in steps_z] + [{"sp": z * inner + at} for at in steps_y]
    for peer in greeted:
        pl.semaphore_signal(barrier, inc=1, device_id=peer, device_id_type=pl.DeviceIdType.MESH)
    pl.semaphore_wait(barrier, len(greeted))

    def remote(source, target, send, recv, at_z, at_y):
        return pltpu.make_async_remote_copy(
            src_ref=source, dst_ref=target, send_sem=send, recv_sem=recv,
            device_id={"sp": at_z * inner + at_y}, device_id_type=pl.DeviceIdType.MESH,
        )

    def block_copy(source, part, own, way):
        ref = normed_ref.at[part] if own else blocks.at[source, part]
        return remote(
            ref, blocks.at[source, part],
            block_send.at[(way + 1) // 2, source, part], block_recv.at[source, part], z + way, y,
        )

    def meta_copy(step):
        at = lax.rem(z + step, outer)
        return remote(meta_ref.at[at], metas.at[z], meta_send.at[step - 1], meta_recv.at[z], at, y)

    def row_copy(source, step, part):
        at = lax.rem(y + step, inner)
        return remote(
            picked.at[source, at, part], rows.at[source, y, part],
            row_send.at[source, step - 1, part], row_recv.at[source, y, part], z, at,
        )

    def back_copy(source, step, part):
        at = lax.rem(y + step, inner)
        return remote(
            made.at[source, at, part], back.at[source, y, part],
            back_send.at[source, step - 1, part], back_recv.at[source, y, part], z, at,
        )

    def sum_copy(source, part, way):
        slot = source if way < 0 else jnp.where(source == z + 1, outer, source)
        return remote(
            partial.at[source, part], coming.at[slot, part],
            sum_send.at[source, part], sum_recv.at[slot, part], z + way, y,
        )

    def wait_recv(ref, sem):
        remote(ref, ref, block_send.at[0, 0, 0], sem, z, y).wait_recv()

    for step in range(1, outer):
        meta_copy(step).start()
    for part in range(parts):
        for way in (1, -1):

            @pl.when((z + way >= 0) & (z + way < outer))
            def _():
                block_copy(z, part, True, way).start()

    blocks[z] = normed_ref[...]
    metas[z] = meta_ref[z]

    kinds = "ABCFRW"
    steps = max(len(row) for row in order) + 1

    def coded(row):
        first = [kind for kind, _, _ in row].index("B")
        row = row[:first] + [("W", 0, 0)] + row[first:]
        codes = [(kinds.index(kind) * outer + source) * parts + part for kind, source, part in row]
        return codes + [len(kinds) * outer * parts] * (steps - len(codes))

    base = (len(kinds) + 1) * outer * parts
    rows_coded = [coded(row) for row in order]
    words = []
    for start in range(0, steps, 3):
        value = None
        for at in range(outer):
            word = sum(code * base**index for index, code in enumerate(rows_coded[at][start : start + 3]))
            value = jnp.int32(word) if value is None else jnp.where(z == at, word, value)
        words.append(value)

    def task_of(step):
        index, digit = step // 3, lax.rem(step, 3)
        level = words
        while len(level) > 1:
            even = lax.rem(index, 2) == 0
            level = [
                jnp.where(even, level[at], level[at + 1]) if at + 1 < len(level) else level[at]
                for at in range(0, len(level), 2)
            ]
            index = index // 2
        word = level[0]
        code = jnp.where(digit == 0, word, jnp.where(digit == 1, word // base, word // base**2))
        code = lax.rem(code, base)
        return code // (outer * parts), lax.rem(code // parts, outer), lax.rem(code, parts)

    def forwards(source):
        return [
            (1, (source < z) & (z < outer - 1)),
            (-1, (source > z) & (z > 0)),
        ]

    def ends(source):
        return [
            (-1, (source < z) & (z == outer - 1)),
            (1, (source > z) & (z == 0)),
        ]

    def needs(source):
        return functools.reduce(jnp.logical_or, [needed for _, needed in forwards(source)])

    def arrive(source, part):
        wait_recv(blocks.at[source, part], block_recv.at[source, part])

    def pick(source, part):
        @pl.when((source != z) & (part == 0))
        def _():
            wait_recv(metas.at[source], meta_recv.at[source])

        @pl.when(part == 0)
        def _():
            slot_ids = lax.broadcasted_iota(jnp.int32, (capacity, tokens), 0).astype(jnp.float32)
            for at in range(inner):
                select[source, at * capacity : (at + 1) * capacity] = jnp.where(
                    metas[source, at : at + 1, :] == slot_ids, 1.0, 0.0
                ).astype(jnp.bfloat16)

        @pl.when((source != z) & ~needs(source))
        def _():
            arrive(source, part)

        found = jnp.dot(
            select[source], blocks[source, part], preferred_element_type=jnp.float32
        ).astype(jnp.bfloat16)
        for at in range(inner):
            picked[source, at, part] = found[at * capacity : (at + 1) * capacity]
        rows[source, y, part] = picked[source, y, part]
        for step in range(1, inner):
            row_copy(source, step, part).start()

    def apply_experts(source):
        gate_acc[...] = jnp.zeros_like(gate_acc)
        up_acc[...] = jnp.zeros_like(up_acc)

        def widen(pair, carry):
            for part in (2 * pair, 2 * pair + 1):
                for step in range(1, inner):
                    at = lax.rem(y + step, inner)
                    wait_recv(rows.at[source, at, part], row_recv.at[source, at, part])
            taken = jnp.concatenate(
                [
                    jnp.concatenate([rows[source, at, 2 * pair + half] for half in range(2)], axis=1)
                    for at in range(inner)
                ],
                axis=0,
            )
            depth = pl.ds(pl.multiple_of(pair * 2 * width, 2 * width), 2 * width)
            gate_acc[...] += jnp.dot(taken, gate_w[depth, :], preferred_element_type=jnp.float32)
            up_acc[...] += jnp.dot(taken, up_w[depth, :], preferred_element_type=jnp.float32)
            return carry

        lax.fori_loop(0, parts // 2, widen, 0)
        gate = gate_acc[...]
        hidden = (gate / (1.0 + jnp.exp(-gate)) * up_acc[...]).astype(jnp.bfloat16)

        for part in range(parts):
            cols = slice(part * width, (part + 1) * width)
            result = jnp.dot(hidden, down_w[:, cols], preferred_element_type=jnp.float32).astype(
                jnp.bfloat16
            )
            for at in range(inner):
                made[source, at, part] = result[at * capacity : (at + 1) * capacity]
            back[source, y, part] = made[source, y, part]
            for step in range(1, inner):
                back_copy(source, step, part).start()

        columns[source] = jnp.transpose(metas[source])
        slot_lanes = lax.broadcasted_iota(jnp.int32, (tokens, capacity), 1).astype(jnp.float32)
        for at in range(inner):
            spread[source, at] = jnp.where(
                columns[source, :, at : at + 1] == slot_lanes, 1.0, 0.0
            ).astype(jnp.bfloat16)

    def combine(source, part):
        for step in range(1, inner):
            at = lax.rem(y + step, inner)
            wait_recv(back.at[source, at, part], back_recv.at[source, at, part])
        summed = sum(
            jnp.dot(spread[source, at], back[source, at, part], preferred_element_type=jnp.float32)
            * columns[source, :, inner + at : inner + at + 1]
            for at in range(inner)
        )

        @pl.when(source == z)
        def _():
            total[part] = after_ref[part] + summed

        @pl.when(source != z)
        def _():
            partial[source, part] = summed.astype(jnp.bfloat16)

        for way, needed in ends(source):

            @pl.when(needed)
            def _():
                sum_copy(source, part, way).start()

    def relay(source, part):
        wait_recv(coming.at[source, part], sum_recv.at[source, part])
        partial[source, part] = (
            partial[source, part].astype(jnp.float32) + coming[source, part].astype(jnp.float32)
        ).astype(jnp.bfloat16)
        for way in (1, -1):

            @pl.when((source > z) if way > 0 else (source < z))
            def _():
                sum_copy(source, part, way).start()

    def run_task(step, carry):
        kind, source, part = task_of(step)

        @pl.when(kind == 0)
        def _():
            pick(source, part)

        @pl.when(kind == 1)
        def _():
            apply_experts(source)

        @pl.when(kind == 2)
        def _():
            combine(source, part)

        @pl.when(kind == 3)
        def _():
            arrive(source, part)
            for way, needed in forwards(source):

                @pl.when(needed)
                def _():
                    block_copy(source, part, False, way).start()

        @pl.when(kind == 4)
        def _():
            relay(source, part)

        @pl.when(kind == 5)
        def _():
            for load in loads:
                load.wait()

        return carry

    lax.fori_loop(0, steps, run_task, 0)

    for part in range(parts):
        for slot, valid in ((z, z < outer - 1), (outer, z > 0)):

            @pl.when(valid)
            def _():
                wait_recv(coming.at[slot, part], sum_recv.at[slot, part])
                total[part] += coming[slot, part].astype(jnp.float32)

        out_ref[:, part * width : (part + 1) * width] = total[part].astype(out_ref.dtype)

    for step in range(1, outer):
        meta_copy(step).wait_send()
    def drain(source, carry):
        for part in range(parts):
            for way in (1, -1):
                onward = (z + way >= 0) & (z + way < outer)
                passing = (source == z) | ((source < z) if way > 0 else (source > z))

                @pl.when(onward & passing)
                def _():
                    block_copy(source, part, False, way).wait_send()

                @pl.when(onward & ((source > z) if way > 0 else (source < z)))
                def _():
                    sum_copy(source, part, way).wait_send()

            for step in range(1, inner):
                row_copy(source, step, part).wait_send()
                back_copy(source, step, part).wait_send()
        return carry

    lax.fori_loop(0, outer, drain, 0)


def run_experts(normed, meta, after, gate, up, down, sp_count, capacity, number):
    outer, inner = split_of(sp_count)
    parts, tokens, width = normed.shape
    model, hidden = gate.shape[1:]
    across_z = tokens * width * 2 / link_rate
    order = plan_tasks(outer, parts, across_z, across_z * capacity / tokens)
    dma = pltpu.SemaphoreType.DMA
    bf16, f32 = jnp.bfloat16, jnp.float32
    steps_y = max(inner - 1, 1)
    vmem = pl.BlockSpec(memory_space=pltpu.VMEM)
    anywhere = pl.BlockSpec(memory_space=pl.ANY)
    held = [
        pltpu.VMEM((model, hidden), bf16),
        pltpu.VMEM((model, hidden), bf16),
        pltpu.VMEM((hidden, model), bf16),
        pltpu.VMEM((outer, parts, tokens, width), bf16),
        pltpu.VMEM((outer,) + meta.shape[1:], f32),
        pltpu.VMEM((outer, inner, parts, capacity, width), bf16),
        pltpu.VMEM((outer, inner, parts, capacity, width), bf16),
        pltpu.VMEM((outer, inner, parts, capacity, width), bf16),
        pltpu.VMEM((outer, inner, parts, capacity, width), bf16),
        pltpu.VMEM((outer, parts, tokens, width), bf16),
        pltpu.VMEM((outer + 1, parts, tokens, width), bf16),
        pltpu.VMEM((parts, tokens, width), f32),
        pltpu.VMEM((inner * capacity, hidden), f32),
        pltpu.VMEM((inner * capacity, hidden), f32),
        pltpu.VMEM((outer, inner * capacity, tokens), bf16),
        pltpu.VMEM((outer, tokens, meta.shape[1]), f32),
        pltpu.VMEM((outer, inner, tokens, capacity), bf16),
    ]
    grant = sum(
        math.prod(s.shape[:-1]) * -(-s.shape[-1] // 128) * 128 * s.dtype.itemsize for s in held
    )
    return pl.pallas_call(
        functools.partial(experts_kernel, outer, inner, capacity, order),
        out_shape=jax.ShapeDtypeStruct((tokens, parts * width), bf16),
        in_specs=[vmem, vmem, vmem, anywhere, anywhere, anywhere],
        out_specs=vmem,
        scratch_shapes=held
        + [
            dma((3,)),
            dma((outer,)),
            dma((outer,)),
            dma((2, outer, parts)),
            dma((outer, parts)),
            dma((outer, steps_y, parts)),
            dma((outer, inner, parts)),
            dma((outer, steps_y, parts)),
            dma((outer, inner, parts)),
            dma((outer, parts)),
            dma((outer + 1, parts)),
        ],
        compiler_params=pltpu.CompilerParams(
            collective_id=number, has_side_effects=True, vmem_limit_bytes=grant + extra_vmem
        ),
        cost_estimate=pl.CostEstimate(
            flops=6 * sp_count * capacity * model * hidden, bytes_accessed=10**7, transcendentals=0
        ),
    )(normed, meta, after, gate, up, down)


def shards(
    query_nope,
    query_rope,
    latent,
    key_rope,
    resid,
    latent_gain,
    key_up,
    value_up,
    out_proj,
    norm_gain,
    expert_gate,
    expert_up,
    expert_down,
    routes,
    route_weight,
):
    tokens, channels = latent.shape[1:]
    sp_count = lax.axis_size("sp")
    dp_count = lax.axis_size("dp")
    me = lax.axis_index("sp")
    nope, rope = query_nope.shape[-1], query_rope.shape[-1]
    heads_here = key_up.shape[1] // nope
    scale = (nope + rope) ** (-0.5)
    local_pos = me * tokens + jnp.arange(tokens, dtype=jnp.int32)
    latent_normed = rms_scaled(latent[0], latent_gain).astype(jnp.bfloat16)
    key_turned = rotate(key_rope[0], local_pos)
    spare = 128 - rope
    row = jnp.concatenate(
        [latent_normed, key_turned, jnp.zeros((tokens, spare), jnp.bfloat16)], axis=1
    )
    cores = 2 if dp_count % 2 == 0 else 1
    piece = channels // cores
    ups = lax.dynamic_slice_in_dim(
        jnp.concatenate([key_up, value_up], axis=1),
        lax.rem(lax.axis_index("dp"), cores) * piece, piece, axis=0,
    )
    frequency = rope_base ** (-jnp.arange(rope // 2, dtype=jnp.float32) / (rope // 2))
    angles = frequency[:, None] * local_pos.astype(jnp.float32)[None, :]
    experts_all = sp_count * expert_gate.shape[0]
    capacity = 4 * tokens // experts_all
    after, normed, meta = run_front(
        row, ups, out_proj, query_nope[0].reshape(tokens, -1), query_rope[0].reshape(tokens, -1),
        jnp.cos(angles), jnp.sin(angles), resid[0], norm_gain[None], routes[0].T, route_weight[0].T,
        experts_all, sp_count, dp_count, cores, heads_here, nope, channels, scale, 0,
    )
    mixed = run_experts(
        normed, meta, after, expert_gate, expert_up, expert_down, sp_count, capacity, 1
    )
    return mixed[None]


def solution(mesh):
    return jax.shard_map(
        shards,
        mesh=mesh,
        in_specs=(
            P("dp", "sp", None, None),
            P("dp", "sp", None, None),
            P("dp", "sp", None),
            P("dp", "sp", None),
            P("dp", "sp", None),
            P(),
            P(None, "sp"),
            P(None, "sp"),
            P("sp", "dp"),
            P(),
            P("sp", None, None),
            P("sp", None, None),
            P("sp", None, None),
            P("dp", "sp", None),
            P("dp", "sp", None),
        ),
        out_specs=P("dp", "sp", None),
        check_vma=False,
    )
```
